32 devices in a mesh: dp: 4 (over y, x), kv: 4 (over z), tp: 2 (over core).
Axes of the slice: x: 2, y: 2, z: 4, core: 2. Of those that a mesh axis runs over, the one named last changes fastest.
Arguments:
- tokens: bfloat16 [1024, 2048], P(('dp', 'kv', 'tp')), may hold values from -6 to 6
- norm_gain: float32 [2048], replicated, may hold values from 0.1 to 1.9
- gate_proj: bfloat16 [2048, 4096], P(None, ('kv', 'tp')), may hold values from -0.125 to 0.125
- inner_proj: bfloat16 [2048, 4096], P(None, ('kv', 'tp')), may hold values from -0.125 to 0.125
- write_proj: bfloat16 [2048, 1024], P(None, ('kv', 'tp')), may hold values from -0.125 to 0.125
- read_proj: bfloat16 [2048, 1024], P(None, ('kv', 'tp')), may hold values from -0.125 to 0.125
- step_proj: bfloat16 [2048, 64], replicated, may hold values from -0.125 to 0.125
- step_bias: float32 [64], replicated, may hold values from -3 to 0
- decay_log: float32 [64], replicated, may hold values from -5 to 0.7
- skip_gain: float32 [64], replicated, may hold values from 0.25 to 4
- conv_inner: bfloat16 [4, 4096], replicated, may hold values from -3 to 3
- conv_write: bfloat16 [4, 1024], replicated, may hold values from -3 to 3
- conv_read: bfloat16 [4, 1024], replicated, may hold values from -3 to 3
- out_gain: float32 [4096], replicated, may hold values from 0.1 to 1.9
- out_proj: bfloat16 [4096, 2048], P(('kv', 'tp')), may hold values from -0.09375 to 0.09375
- saved_state: float32 [256, 64, 64, 128], P('dp', ('kv', 'tp')), may hold values from -1.75 to 1.75
- inner_history: bfloat16 [256, 7, 4096], P('dp', None, ('kv', 'tp')), may hold values from -6 to 6
- write_history: bfloat16 [256, 7, 1024], P('dp', None, ('kv', 'tp')), may hold values from -6 to 6
- read_history: bfloat16 [256, 7, 1024], P('dp', None, ('kv', 'tp')), may hold values from -6 to 6
- last_steps: float32 [256, 4, 64], P('dp', None, ('kv', 'tp')), may hold values from 0.02 to 1
- accepted: int32 [256], P('dp'), may hold values from 0 to 4
Outputs:
- mixed: bfloat16 [1024, 2048], P(('dp', 'kv', 'tp'))
- base_state: float32 [256, 64, 64, 128], P('dp', ('kv', 'tp'))
The draws below stay inside these ranges and needn't reach their ends.
All inputs are finite; a program needn't handle non-finite values.
Results may differ from the reference program's by a relative error of at most 0.014.
Values may be sent and summed in bfloat16 or wider, within the bound.
A program may use at most 128 MiB of HBM per device.

```python
import math
import jax
import jax.numpy as jnp
from jax import lax

D = 2048
HEADS = 64
HEAD_DIM = 64
STATE = 128
GROUPS = 8
WIDTH = 4
PROP = 4
INNER = 4096
SEQS = 256
TOKENS = 1024
HIST = 7


def draw_decay_log(key, part):
    spread_draw = jax.random.uniform(key, (HEADS,), jnp.float32)
    return -3.9 + 4.6 * spread_draw


def touch_ends(array, rng, least, largest):
    longest = array.shape.index(max(array.shape))
    spots = []
    for shift in (0, 1):
        where = [jax.random.randint(jax.random.fold_in(rng, axis), (), 0, length) for axis, length in enumerate(array.shape)]
        where[longest] = (where[longest] + shift) % array.shape[longest]
        spots.append(tuple(where))
    return array.at[spots[0]].set(least).at[spots[1]].set(largest)


def steps_of(rng, dims, pieces, low, high):
    factor_of = 1.0
    for axis_at, shards_of in pieces:
        draws = jax.random.uniform(jax.random.fold_in(jax.random.fold_in(rng, 6), axis_at), (shards_of,), jnp.float32, low / len(pieces), high / len(pieces))
        factor_of = factor_of * jnp.repeat(jnp.exp(draws), dims[axis_at] // shards_of).reshape((-1,) + (1,) * (len(dims) - 1 - axis_at))
    return factor_of


def normal_values(stream_key, extent, width, reach, shards=(), kind=jnp.bfloat16):
    factor_of = steps_of(stream_key, extent, shards, -0.22, 0.18) if shards else 1.0
    array = jax.random.normal(stream_key, extent, jnp.float32) * width * factor_of
    return jnp.minimum(jnp.maximum(array, -reach), reach).astype(kind)


def setup_inputs(seed: int = 0) -> dict:
    key_list = jax.random.split(jax.random.key(seed), 22)
    tokens = normal_values(key_list[0], (TOKENS, D), 1.0, 6.0, ((0, 32),))
    norm_gain = jnp.clip(1.0 + 0.18 * jax.random.normal(key_list[1], (D,), jnp.float32), 0.1, 1.9)
    gate_proj = normal_values(key_list[2], (D, INNER), D ** -0.5, 0.125, ((1, 8),))
    inner_proj = normal_values(key_list[3], (D, INNER), D ** -0.5, 0.125, ((1, 8),))
    write_proj = normal_values(key_list[4], (D, GROUPS * STATE), D ** -0.5, 0.125, ((1, 8),))
    read_proj = normal_values(key_list[5], (D, GROUPS * STATE), D ** -0.5, 0.125, ((1, 8),))
    step_proj = normal_values(key_list[6], (D, HEADS), D ** -0.5, 0.125)
    step_bias = jnp.clip(jax.random.uniform(key_list[7], (HEADS,), jnp.float32, -3.0, 0.0), -3.0, 0.0)
    decay_log = draw_decay_log(jax.random.fold_in(key_list[21], 71), 0)
    skip_gain = jnp.clip(jnp.exp(jax.random.uniform(key_list[9], (HEADS,), jnp.float32, math.log(0.25), math.log(4.0))), 0.25, 4.0)
    conv_inner = normal_values(key_list[10], (WIDTH, INNER), WIDTH ** -0.5, 3.0)
    conv_write = normal_values(key_list[11], (WIDTH, GROUPS * STATE), WIDTH ** -0.5, 3.0)
    conv_read = normal_values(key_list[12], (WIDTH, GROUPS * STATE), WIDTH ** -0.5, 3.0)
    out_gain = jnp.clip(1.0 + 0.18 * jax.random.normal(key_list[13], (INNER,), jnp.float32), 0.1, 1.9)
    out_proj = normal_values(key_list[14], (INNER, D), INNER ** -0.5, 0.09375, ((0, 8),))
    saved_state = normal_values(key_list[15], (SEQS, HEADS, HEAD_DIM, STATE), 0.3, 1.75, ((0, 4), (1, 8)), jnp.float32)
    inner_history = normal_values(key_list[16], (SEQS, HIST, INNER), 1.0, 6.0, ((0, 4), (2, 8)))
    write_history = normal_values(key_list[17], (SEQS, HIST, GROUPS * STATE), 1.0, 6.0, ((0, 4), (2, 8)))
    read_history = normal_values(key_list[18], (SEQS, HIST, GROUPS * STATE), 1.0, 6.0, ((0, 4), (2, 8)))
    last_steps = jnp.clip(jnp.exp(math.log(1.0) - 3.912023 * jax.random.uniform(key_list[19], (SEQS, PROP, HEADS), jnp.float32) ** steps_of(key_list[19], (SEQS, PROP, HEADS), ((0, 4), (2, 8)), -0.2, 0.2)), 0.02, 1.0)
    accepted = touch_ends(jax.random.randint(key_list[20], (SEQS,), 0, PROP + 1), jax.random.fold_in(key_list[20], 1), 0, PROP).astype(jnp.int32)
    return {"tokens": tokens, "norm_gain": norm_gain, "gate_proj": gate_proj, "inner_proj": inner_proj, "write_proj": write_proj, "read_proj": read_proj, "step_proj": step_proj, "step_bias": step_bias, "decay_log": decay_log, "skip_gain": skip_gain, "conv_inner": conv_inner, "conv_write": conv_write, "conv_read": conv_read, "out_gain": out_gain, "out_proj": out_proj, "saved_state": saved_state, "inner_history": inner_history, "write_history": write_history, "read_history": read_history, "last_steps": last_steps, "accepted": accepted}


EPSILON = 0.1
highest = lax.Precision.HIGHEST

def conv_rows(row_block, weight):
    out_len = row_block.shape[1] - weight.shape[0] + 1
    result = weight[0] * row_block[:, 0:out_len]
    for offset in range(1, weight.shape[0]):
        result = result + weight[offset] * row_block[:, offset:offset + out_len]
    return result

def rounded(values):
    return lax.optimization_barrier(values.astype(jnp.bfloat16)).astype(jnp.float32)

def reference(tokens, norm_gain, gate_proj, inner_proj, write_proj, read_proj, step_proj, step_bias, decay_log, skip_gain, conv_inner, conv_write, conv_read, out_gain, out_proj, saved_state, inner_history, write_history, read_history, last_steps, accepted):
    seq_count = saved_state.shape[0]
    own_rows = tokens.astype(jnp.float32)
    normed = (own_rows * lax.rsqrt(lax.optimization_barrier(jnp.mean(own_rows * own_rows, axis=-1, keepdims=True)) + EPSILON) * norm_gain).astype(jnp.bfloat16)
    gate_rows = jnp.dot(normed, gate_proj, preferred_element_type=jnp.float32).astype(jnp.bfloat16)
    inner_rows = jnp.dot(normed, inner_proj, preferred_element_type=jnp.float32).astype(jnp.bfloat16)
    write_rows = jnp.dot(normed, write_proj, preferred_element_type=jnp.float32).astype(jnp.bfloat16)
    read_rows = jnp.dot(normed, read_proj, preferred_element_type=jnp.float32).astype(jnp.bfloat16)
    step_rows = jnp.dot(normed, step_proj, preferred_element_type=jnp.float32)
    conv_width = conv_inner.shape[0]
    window_rows = (accepted[:, None] + jnp.arange(conv_width - 1, dtype=jnp.int32)[None, :]).astype(jnp.int32)

    def current(history, new_rows, weight):
        window = jnp.take_along_axis(history, window_rows[:, :, None], axis=1)
        joined = jnp.concatenate([window, new_rows.reshape(seq_count, PROP, -1)], axis=1)
        return jax.nn.silu(conv_rows(joined.astype(jnp.float32), weight.astype(jnp.float32)))
    inner_old = jax.nn.silu(conv_rows(inner_history.astype(jnp.float32), conv_inner.astype(jnp.float32)))
    write_old = rounded(jax.nn.silu(conv_rows(write_history.astype(jnp.float32), conv_write.astype(jnp.float32))))
    inner_new = current(inner_history, inner_rows, conv_inner)
    write_new = rounded(current(write_history, write_rows, conv_write))
    read_new = rounded(current(read_history, read_rows, conv_read))
    step_size = jax.nn.softplus(step_rows + step_bias[None, :]).reshape(seq_count, PROP, HEADS)
    decay_rate = -jnp.exp(decay_log)
    per_group = HEADS // GROUPS
    accepted_mask = (jnp.arange(PROP, dtype=jnp.int32)[None, :] < accepted[:, None]).astype(jnp.float32)
    step_logs = decay_rate[None, None, :] * last_steps * accepted_mask[:, :, None]
    total_log = lax.optimization_barrier(jnp.sum(step_logs, axis=1))
    tail_log = total_log[:, None, :] - jnp.cumsum(step_logs, axis=1)
    old_weights = accepted_mask[:, :, None] * jnp.exp(tail_log) * last_steps
    inner_old_heads = inner_old.reshape(seq_count, PROP, HEADS, HEAD_DIM)
    write_old_heads = jnp.repeat(write_old.reshape(seq_count, PROP, GROUPS, STATE), per_group, axis=2)
    base_state = jnp.exp(total_log)[:, :, None, None] * saved_state + jnp.einsum('sth,sthp,sthn->shpn', old_weights, inner_old_heads, write_old_heads, precision=highest)
    cumulative = jnp.cumsum(decay_rate[None, None, :] * step_size, axis=1)
    log_gap = cumulative[:, :, None, :] - cumulative[:, None, :, :]
    causal = (jnp.arange(PROP)[:, None] >= jnp.arange(PROP)[None, :])[None, :, :, None]
    kernel = jnp.where(causal, jnp.exp(jnp.where(causal, log_gap, 0.0)), 0.0)
    write_heads = jnp.repeat(write_new.reshape(seq_count, PROP, GROUPS, STATE), per_group, axis=2)
    read_heads = jnp.repeat(read_new.reshape(seq_count, PROP, GROUPS, STATE), per_group, axis=2)
    scores = jnp.einsum('sihn,sjhn->sijh', read_heads, write_heads, precision=highest)
    inner_heads = inner_new.reshape(seq_count, PROP, HEADS, HEAD_DIM)
    within = jnp.einsum('sijh,sjh,sjhp->sihp', kernel * scores, step_size, inner_heads, precision=highest)
    carried = jnp.exp(cumulative)[..., None] * jnp.einsum('sihn,shpn->sihp', read_heads, base_state, precision=highest)
    mixed_heads = within + carried + skip_gain[None, None, :, None] * inner_heads
    gated_rows = mixed_heads.reshape(seq_count * PROP, INNER) * jax.nn.silu(gate_rows.astype(jnp.float32))
    squares = lax.optimization_barrier(jnp.mean(gated_rows * gated_rows, axis=-1, keepdims=True))
    unscaled = (gated_rows * out_gain).astype(jnp.bfloat16)
    mixed = (jnp.dot(unscaled, out_proj, preferred_element_type=jnp.float32) * lax.rsqrt(squares + EPSILON)).astype(jnp.bfloat16)
    return (mixed, base_state)
```

```python
import functools

import jax
import jax.numpy as jnp
from jax import lax
from jax.experimental import pallas as pl
from jax.experimental.pallas import tpu as pltpu
from jax.sharding import PartitionSpec as P

GROUPS = 8
EPSILON = 0.1
BLOCK = 8
highest = lax.Precision.HIGHEST


def swapped(value, axis, stride):
    mask = 2**stride
    pairs = [(source, source ^ mask) for source in range(lax.axis_size(axis))]
    return lax.ppermute(value, axis, pairs)


def mix_kernel(
    rank_ref,
    acc_ref,
    steps_ref,
    last_ref,
    par_ref,
    gate_ref,
    inner_ref,
    write_ref,
    read_ref,
    hist_inner_ref,
    hist_write_ref,
    hist_read_ref,
    taps_inner_ref,
    taps_write_ref,
    taps_read_ref,
    gain_ref,
    expand_ref,
    state_ref,
    un_ref,
    sq_ref,
    base_ref,
):
    f32 = jnp.float32
    props = steps_ref.shape[0]
    heads = last_ref.shape[2]
    cols = inner_ref.shape[2]
    states = write_ref.shape[2]
    head_dim = cols // heads
    hist = hist_inner_ref.shape[0]
    width = taps_inner_ref.shape[0]
    acc = acc_ref[...]

    def silu(x):
        return x / (1.0 + jnp.exp(-x))

    def slabs(ref):
        return [ref[k].astype(f32) for k in range(ref.shape[0])]

    round_bf = lambda x: x.astype(jnp.bfloat16).astype(f32)

    def conv(rows, taps_ref):
        taps = taps_ref[...].astype(f32)
        res = []
        for r in range(len(rows) - width + 1):
            v = taps[0:1] * rows[r]
            for k in range(1, width):
                v = v + taps[k : k + 1] * rows[r + k]
            res.append(silu(v))
        return res

    def current(h, new_ref):
        where_at = jnp.broadcast_to(acc, h[0].shape)
        rows = []
        for k in range(width - 1):
            r = h[k]
            for v in range(1, hist - width + 2):
                r = jnp.where(where_at == v, h[k + v], r)
            rows.append(r)
        return rows + [round_bf(x) for x in slabs(new_ref)]

    h_inner = slabs(hist_inner_ref)
    inner_old = conv(h_inner, taps_inner_ref)
    inner_new = conv(current(h_inner, inner_ref), taps_inner_ref)
    h_write = slabs(hist_write_ref)
    write_old = [round_bf(x) for x in conv(h_write, taps_write_ref)]
    write_new = [round_bf(x) for x in conv(current(h_write, write_ref), taps_write_ref)]
    read_new = [round_bf(x) for x in conv(current(slabs(hist_read_ref), read_ref), taps_read_ref)]

    bias = par_ref[0:1]
    rate = -jnp.exp(par_ref[1:2])
    skip = par_ref[2:3]
    acc_h = jnp.broadcast_to(acc, (BLOCK, heads))
    masks = [jnp.where(acc_h > t, 1.0, 0.0) for t in range(props)]
    logs = [rate * last_ref[t] * masks[t] for t in range(props)]
    coefs = [None] * props
    tail = jnp.zeros((BLOCK, heads), f32)
    for t in reversed(range(props)):
        coefs[t] = masks[t] * jnp.exp(tail) * last_ref[t]
        tail = tail + logs[t]
    decay = jnp.exp(tail)
    step = []
    for t in range(props):
        x = steps_ref[t][:, :heads] + bias
        step.append(jnp.maximum(x, 0.0) + jnp.log1p(jnp.exp(-jnp.abs(x))))
    cums = []
    for t in range(props):
        cums.append(rate * step[t] + (cums[-1] if cums else 0.0))
    where_of = {}
    for i in range(props):
        for j in range(i + 1):
            score = jnp.sum(read_new[i] * write_new[j], axis=-1, keepdims=True)
            c = jnp.exp(cums[i] - cums[j]) * step[j] * score
            if i == j:
                c = c + skip
            where_of[(i, j)] = len(coefs)
            coefs.append(c)
    first_cum = len(coefs)
    for i in range(props):
        coefs.append(jnp.exp(cums[i]))
    wide = jnp.dot(
        jnp.concatenate(coefs, axis=0),
        expand_ref[...],
        precision=highest,
        preferred_element_type=f32,
    )

    def at(k):
        return wide[k * BLOCK : (k + 1) * BLOCK]

    left = jnp.concatenate([at(t) * inner_old[t] for t in range(props)], axis=0)
    high = round_bf(left)
    both = jnp.concatenate([high, left - high], axis=0)
    turned = jnp.transpose(both).astype(jnp.bfloat16)
    write_all = jnp.concatenate(write_old + write_old, axis=0)
    read_all = jnp.concatenate(read_new, axis=0)
    seq_w = lax.broadcasted_iota(jnp.int32, write_all.shape, 0) % BLOCK
    seq_r = lax.broadcasted_iota(jnp.int32, read_all.shape, 0) % BLOCK
    carried = jnp.zeros((props * BLOCK, cols), f32)
    for s in range(BLOCK):
        right = jnp.where(seq_w == s, write_all, 0.0).astype(jnp.bfloat16)
        update = jnp.dot(turned, right, preferred_element_type=f32)
        parts = []
        for h in range(heads):
            lo, hi = h * head_dim, (h + 1) * head_dim
            d = jnp.broadcast_to(decay[s : s + 1, h : h + 1], (head_dim, states))
            new = d * state_ref[s, lo:hi, :] + update[lo:hi]
            base_ref[s, lo:hi, :] = new
            parts.append(new.astype(jnp.bfloat16))
        asked = jnp.where(seq_r == s, read_all, 0.0).astype(jnp.bfloat16)
        carried = carried + lax.dot_general(
            asked,
            jnp.concatenate(parts, axis=0),
            (((1,), (1,)), ((), ())),
            preferred_element_type=f32,
        )
    for i in range(props):
        y = at(first_cum + i) * carried[i * BLOCK : (i + 1) * BLOCK]
        for j in range(i + 1):
            y = y + at(where_of[(i, j)]) * inner_new[j]
        g = y * silu(gate_ref[i].astype(f32))
        sq_ref[i] = jnp.broadcast_to(jnp.sum(g * g, axis=-1, keepdims=True), sq_ref.shape[1:])
        un_ref[i] = (g * gain_ref[...]).astype(un_ref.dtype)


def mix(rank, group, acc, last, par, gate, inner, small, hi, hw, hr, ci, cw, cr, gain, state):
    props, seqs, heads = last.shape
    cols, states = state.shape[1], state.shape[2]
    expand = (jnp.arange(cols)[None, :] // (cols // heads) == jnp.arange(heads)[:, None]).astype(
        jnp.float32
    )
    hist = hi.shape[0]
    width = ci.shape[0]

    def slab(lead, last_dim):
        return pl.BlockSpec((lead, BLOCK, last_dim), lambda g, r: (0, g, 0))

    def piece(which):
        return pl.BlockSpec((props, BLOCK, states), lambda g, r: (0, g, which))

    def own(rows, last_dim, which):
        return pl.BlockSpec((rows, last_dim), lambda g, r: (0, r[which]))

    state_spec = pl.BlockSpec((BLOCK, cols, states), lambda g, r: (g, 0, 0))
    return pl.pallas_call(
        mix_kernel,
        grid_spec=pltpu.PrefetchScalarGridSpec(
            num_scalar_prefetch=1,
            grid=(seqs // BLOCK,),
            in_specs=[
                pl.BlockSpec((BLOCK, 1), lambda g, r: (g, 0)),
                piece(2),
                slab(props, heads),
                pl.BlockSpec(par.shape, lambda g, r: (0, 0)),
                slab(props, cols),
                slab(props, cols),
                piece(0),
                piece(1),
                slab(hist, cols),
                slab(hist, states),
                slab(hist, states),
                own(width, cols, 0),
                own(width, states, 1),
                own(width, states, 1),
                own(1, cols, 0),
                pl.BlockSpec(expand.shape, lambda g, r: (0, 0)),
                state_spec,
            ],
            out_specs=[slab(props, cols), slab(props, 128), state_spec],
        ),
        out_shape=[
            jax.ShapeDtypeStruct((props, seqs, cols), jnp.bfloat16),
            jax.ShapeDtypeStruct((props, seqs, 128), jnp.float32),
            jax.ShapeDtypeStruct(state.shape, jnp.float32),
        ],
        compiler_params=pltpu.CompilerParams(
            dimension_semantics=("arbitrary",), vmem_limit_bytes=48 * 1024 * 1024
        ),
        name="mix",
    )(
        jnp.stack([rank, group]).astype(jnp.int32),
        acc, small, last, par, gate, inner, small, small, hi, hw, hr, ci, cw, cr, gain, expand, state,
    )


MESH = pl.DeviceIdType.MESH
CHUNKS = 2


def remote(src, dst, send, recv, where):
    return pltpu.make_async_remote_copy(
        src_ref=src, dst_ref=dst, send_sem=send, recv_sem=recv, device_id=where, device_id_type=MESH
    )


def gather_kernel(n, own_ref, out_ref, rs, rr, ls, lr, fs, fr, local_sem):
    k = lax.axis_index("kv")
    t = lax.axis_index("tp")
    right = {"kv": lax.rem(k + 1, n)}
    left = {"kv": lax.rem(k + n - 1, n)}
    partner = {"tp": 1 - t}
    span = own_ref.shape[1] // CHUNKS
    barrier = pltpu.get_barrier_semaphore()
    pl.semaphore_signal(barrier, inc=1, device_id=partner, device_id_type=MESH)

    @pl.when(k < n - 1)
    def _():
        pl.semaphore_signal(barrier, inc=1, device_id=right, device_id_type=MESH)

    @pl.when(k > 0)
    def _():
        pl.semaphore_signal(barrier, inc=1, device_id=left, device_id_type=MESH)

    inner = (k > 0) & (k < n - 1)

    @pl.when(inner)
    def _():
        pl.semaphore_wait(barrier, 3)

    @pl.when(jnp.logical_not(inner))
    def _():
        pl.semaphore_wait(barrier, 2)

    def view(j, c):
        return out_ref.at[j, t, :, pl.ds(c * span, span)]

    def own(c):
        return own_ref.at[:, pl.ds(c * span, span)]

    def to_right(s, c):
        j = jnp.maximum(k - s, 0)
        return remote(own(c) if s == 0 else view(j, c), view(j, c), rs.at[s, c], rr.at[s, c], right)

    def to_left(s, c):
        j = jnp.minimum(k + s, n - 1)
        return remote(own(c) if s == 0 else view(j, c), view(j, c), ls.at[s, c], lr.at[s, c], left)

    def across(j, c, mine=False):
        return remote(own(c) if mine else view(j, c), view(j, c), fs.at[j, c], fr.at[j, c], partner)

    for s in range(n - 1):
        for c in range(CHUNKS):
            if s > 0:
                @pl.when(k - s >= 0)
                def _():
                    to_right(s - 1, c).wait_recv()

                @pl.when(k + s < n)
                def _():
                    to_left(s - 1, c).wait_recv()

            @pl.when((k - s >= 0) & (k < n - 1))
            def _():
                to_right(s, c).start()

            @pl.when((k + s < n) & (k > 0))
            def _():
                to_left(s, c).start()

            if s == 0:
                across(k, c, True).start()
            else:
                @pl.when(k - s >= 0)
                def _():
                    across(k - s, c).start()

                @pl.when(k + s < n)
                def _():
                    across(k + s, c).start()
        if s == 0:
            local = pltpu.make_async_copy(own_ref, out_ref.at[k, t], local_sem)
            local.start()
            local.wait()
    s = n - 1
    for c in range(CHUNKS):
        @pl.when(k - s >= 0)
        def _():
            to_right(s - 1, c).wait_recv()
            across(k - s, c).start()

        @pl.when(k + s < n)
        def _():
            to_left(s - 1, c).wait_recv()
            across(k + s, c).start()
    for s in range(n - 1):
        for c in range(CHUNKS):
            @pl.when((k - s >= 0) & (k < n - 1))
            def _():
                to_right(s, c).wait_send()

            @pl.when((k + s < n) & (k > 0))
            def _():
                to_left(s, c).wait_send()
    for j in range(n):
        for c in range(CHUNKS):
            across(j, c).wait_send()
            remote(
                out_ref.at[j, 1 - t, :, pl.ds(c * span, span)],
                out_ref.at[j, 1 - t, :, pl.ds(c * span, span)],
                fs.at[j, c],
                fr.at[j, c],
                partner,
            ).wait_recv()


def gathered(own):
    n = lax.axis_size("kv")
    rows, cols = own.shape
    dma = pltpu.SemaphoreType.DMA
    out = pl.pallas_call(
        functools.partial(gather_kernel, n),
        out_shape=jax.ShapeDtypeStruct((n, 2, rows, cols), own.dtype),
        in_specs=[pl.BlockSpec(memory_space=pltpu.VMEM)],
        out_specs=pl.BlockSpec(memory_space=pltpu.VMEM),
        scratch_shapes=[dma((n - 1, CHUNKS))] * 4 + [dma((n, CHUNKS))] * 2 + [dma],
        compiler_params=pltpu.CompilerParams(
            collective_id=0, has_side_effects=True, vmem_limit_bytes=32 * 1024 * 1024
        ),
        name="gather",
    )(own)
    return out.reshape(n * 2 * rows, cols)


def scatter_kernel(
    n, part, sq, out, sqs, pbuf, rbuf, lbuf, rout, lout, ps, pr, rs, rr, ls, lr, ss, sr
):
    f32 = jnp.float32
    k = lax.axis_index("kv")
    t = lax.axis_index("tp")
    rank = k * 2 + t
    ranks = n * 2
    right = {"kv": lax.rem(k + 1, n)}
    left = {"kv": lax.rem(k + n - 1, n)}
    partner = {"tp": 1 - t}
    span = part.shape[3] // CHUNKS
    barrier = pltpu.get_barrier_semaphore()

    def peer(o):
        p = lax.rem(rank + o, ranks)
        return {"kv": p // 2, "tp": lax.rem(p, 2)}

    for o in range(1, ranks):
        pl.semaphore_signal(barrier, inc=1, device_id=peer(o), device_id_type=MESH)
    pl.semaphore_wait(barrier, ranks - 1)

    def cut(c):
        return pl.ds(c * span, span)

    def across(j, c):
        return remote(
            part.at[j, 1 - t, :, cut(c)], pbuf.at[j, :, cut(c)], ps.at[j, c], pr.at[j, c], partner
        )

    def to_right(d, c):
        return remote(
            rout.at[d, :, cut(c)], rbuf.at[d, :, cut(c)], rs.at[d, c], rr.at[d, c], right
        )

    def to_left(d, c):
        return remote(lout.at[d, :, cut(c)], lbuf.at[d, :, cut(c)], ls.at[d, c], lr.at[d, c], left)

    def square(o):
        p = lax.rem(rank + o, ranks)
        return remote(sq.at[p], sqs.at[rank], ss.at[o], sr.at[o], peer(o))

    low = k < n // 2
    for i in range(n):
        j = jnp.where(low, n - 1 - i, i)
        for c in range(CHUNKS):
            across(j, c).start()
    for o in range(1, ranks):
        square(o).start()
    sqs[rank] = sq[rank]

    def pair(j, c):
        across(j, c).wait_recv()
        return part[j, t, :, cut(c)].astype(f32) + pbuf[j, :, cut(c)].astype(f32)

    def rightward():
        for d in range(n - 1, 0, -1):
            for c in range(CHUNKS):
                @pl.when((k < d) & (k == 0))
                def _():
                    rout[d, :, cut(c)] = pair(d, c).astype(rout.dtype)
                    to_right(d, c).start()

                @pl.when((k < d) & (k > 0))
                def _():
                    value = pair(d, c)
                    to_right(d, c).wait_recv()
                    rout[d, :, cut(c)] = (value + rbuf[d, :, cut(c)].astype(f32)).astype(rout.dtype)
                    to_right(d, c).start()

    def leftward():
        for d in range(n - 1):
            for c in range(CHUNKS):
                @pl.when((k > d) & (k == n - 1))
                def _():
                    lout[d, :, cut(c)] = pair(d, c).astype(lout.dtype)
                    to_left(d, c).start()

                @pl.when((k > d) & (k < n - 1))
                def _():
                    value = pair(d, c)
                    to_left(d, c).wait_recv()
                    lout[d, :, cut(c)] = (value + lbuf[d, :, cut(c)].astype(f32)).astype(lout.dtype)
                    to_left(d, c).start()

    @pl.when(k < n // 2)
    def _():
        rightward()
        leftward()

    @pl.when(k >= n // 2)
    def _():
        leftward()
        rightward()

    for c in range(CHUNKS):
        out[:, cut(c)] = pair(k, c)

        @pl.when(k > 0)
        def _():
            to_right(k, c).wait_recv()
            out[:, cut(c)] += rbuf[k, :, cut(c)].astype(f32)

        @pl.when(k < n - 1)
        def _():
            to_left(k, c).wait_recv()
            out[:, cut(c)] += lbuf[k, :, cut(c)].astype(f32)

    for j in range(n):
        for c in range(CHUNKS):
            across(j, c).wait_send()

            @pl.when(k < j)
            def _():
                to_right(j, c).wait_send()

            @pl.when(k > j)
            def _():
                to_left(j, c).wait_send()
    for o in range(1, ranks):
        square(o).wait_send()
        source = lax.rem(rank + ranks - o, ranks)
        remote(sq.at[rank], sqs.at[source], ss.at[o], sr.at[o], peer(o)).wait_recv()


def scattered(partial_value, squares):
    n = lax.axis_size("kv")
    ranks = n * 2
    rows = partial_value.shape[0] // ranks
    cols = partial_value.shape[1]
    squares = jnp.pad(squares.reshape(ranks, 1, rows), ((0, 0), (0, 7), (0, 128 - rows)))
    dma = pltpu.SemaphoreType.DMA
    vmem = pl.BlockSpec(memory_space=pltpu.VMEM)
    kind = partial_value.dtype
    summed, sqs = pl.pallas_call(
        functools.partial(scatter_kernel, n),
        out_shape=[
            jax.ShapeDtypeStruct((rows, cols), jnp.float32),
            jax.ShapeDtypeStruct(squares.shape, jnp.float32),
        ],
        in_specs=[vmem, vmem],
        out_specs=[vmem, vmem],
        scratch_shapes=[pltpu.VMEM((n, rows, cols), kind)] * 5
        + [dma((n, CHUNKS))] * 6
        + [dma((ranks,))] * 2,
        compiler_params=pltpu.CompilerParams(
            collective_id=1, has_side_effects=True, vmem_limit_bytes=32 * 1024 * 1024
        ),
        name="scatter",
    )(partial_value.reshape(n, 2, rows, cols), squares)
    return summed, jnp.sum(sqs[:, 0, :rows], axis=0)


def pick(x, rows, first):
    wide = jnp.broadcast_to(x, (rows, x.shape[1]))
    lane = lax.broadcasted_iota(jnp.int32, wide.shape, 1)
    row = lax.broadcasted_iota(jnp.int32, wide.shape, 0)
    return jnp.sum(jnp.where(lane == row + first, wide, 0.0), axis=1, keepdims=True)


def turn_rows(rows, props, back=False):
    seqs = rows // props
    row = lax.broadcasted_iota(jnp.int32, (rows, rows), 0)
    col = lax.broadcasted_iota(jnp.int32, (rows, rows), 1)
    if back:
        row, col = col, row
    return jnp.where(col == row % seqs * props + row // seqs, 1.0, 0.0).astype(jnp.bfloat16)


def silu_of(x):
    return x / (1.0 + jnp.exp(-x))


def round_of(x):
    return x.astype(jnp.bfloat16).astype(jnp.float32)


def split_of(x):
    high = x.astype(jnp.bfloat16)
    return high, (x - high.astype(jnp.float32)).astype(jnp.bfloat16)


def own_slice(ref, first, count):
    return ref[:, pl.ds(pl.multiple_of(first, 128), count)].astype(jnp.float32)


def lead_kernel(
    n,
    tokens_hbm,
    norm_hbm,
    acc_hbm,
    last_hbm,
    decay_hbm,
    hist_inner_hbm,
    hist_write_hbm,
    hist_read_hbm,
    taps_inner_hbm,
    taps_write_hbm,
    taps_read_hbm,
    state_ref,
    rows_ref,
    base_ref,
    half_ref,
    part_inner_ref,
    part_write_ref,
    part_read_ref,
    own_ref,
    decay_buf,
    wide_buf,
    turned_buf,
    old_buf,
    rs,
    rr,
    ls,
    lr,
    fs,
    fr,
    local_sem,
    state_sems,
    small_sems,
    tokens_ref,
    norm_ref,
    acc_ref,
    last_ref,
    decay_ref,
    hist_inner_ref,
    hist_write_ref,
    hist_read_ref,
    taps_inner_ref,
    taps_write_ref,
    taps_read_ref,
):
    f32 = jnp.float32
    bf16 = jnp.bfloat16
    k = lax.axis_index("kv")
    t = lax.axis_index("tp")
    rank = k * 2 + t
    right = {"kv": lax.rem(k + 1, n)}
    left = {"kv": lax.rem(k + n - 1, n)}
    partner = {"tp": 1 - t}
    barrier = pltpu.get_barrier_semaphore()
    pl.semaphore_signal(barrier, inc=1, device_id=partner, device_id_type=MESH)

    @pl.when(k < n - 1)
    def _():
        pl.semaphore_signal(barrier, inc=1, device_id=right, device_id_type=MESH)

    @pl.when(k > 0)
    def _():
        pl.semaphore_signal(barrier, inc=1, device_id=left, device_id_type=MESH)

    props, heads, seqs = last_ref.shape
    cols = base_ref.shape[1]
    states = base_ref.shape[2]
    hist = hist_inner_ref.shape[0]
    width = taps_inner_ref.shape[0]
    blocks = seqs // BLOCK

    def fetch(b):
        span = pl.ds(b * BLOCK, BLOCK)
        return pltpu.make_async_copy(state_ref.at[span], base_ref.at[span], state_sems.at[b])

    small = [
        pltpu.make_async_copy(src, dst, small_sems.at[i])
        for i, (src, dst) in enumerate(
            [
                (tokens_hbm, tokens_ref),
                (norm_hbm, norm_ref),
                (acc_hbm, acc_ref),
                (last_hbm, last_ref),
                (decay_hbm, decay_ref),
                (hist_inner_hbm, hist_inner_ref),
                (hist_write_hbm, hist_write_ref),
                (hist_read_hbm, hist_read_ref),
                (taps_inner_hbm, taps_inner_ref),
                (taps_write_hbm, taps_write_ref),
                (taps_read_hbm, taps_read_ref),
            ]
        )
    ]
    for c in small:
        c.start()
    for b in range(blocks):
        fetch(b).start()
    for c in small[:2]:
        c.wait()
    own = tokens_ref[...].astype(f32)
    scale = lax.rsqrt(jnp.mean(own * own, axis=-1, keepdims=True) + EPSILON)
    normed = (own * scale * norm_ref[...]).astype(bf16)
    own_ref[...] = jnp.dot(
        turn_rows(own.shape[0], props), normed, preferred_element_type=f32
    ).astype(bf16)

    inside = (k > 0) & (k < n - 1)

    @pl.when(inside)
    def _():
        pl.semaphore_wait(barrier, 3)

    @pl.when(jnp.logical_not(inside))
    def _():
        pl.semaphore_wait(barrier, 2)

    span = own_ref.shape[1] // CHUNKS

    def view(j, c):
        return rows_ref.at[j, t, :, pl.ds(c * span, span)]

    def mine(c):
        return own_ref.at[:, pl.ds(c * span, span)]

    def to_right(s, c):
        j = jnp.maximum(k - s, 0)
        return remote(mine(c) if s == 0 else view(j, c), view(j, c), rs.at[s, c], rr.at[s, c], right)

    def to_left(s, c):
        j = jnp.minimum(k + s, n - 1)
        return remote(mine(c) if s == 0 else view(j, c), view(j, c), ls.at[s, c], lr.at[s, c], left)

    def across(j, c, first=False):
        return remote(mine(c) if first else view(j, c), view(j, c), fs.at[j, c], fr.at[j, c], partner)

    def hop(s, c):
        if s > 0:
            @pl.when(k - s >= 0)
            def _():
                to_right(s - 1, c).wait_recv()

            @pl.when(k + s < n)
            def _():
                to_left(s - 1, c).wait_recv()

        if s < n - 1:
            @pl.when((k - s >= 0) & (k < n - 1))
            def _():
                to_right(s, c).start()

            @pl.when((k + s < n) & (k > 0))
            def _():
                to_left(s, c).start()

        if s == 0:
            across(k, c, True).start()
        else:
            @pl.when(k - s >= 0)
            def _():
                across(k - s, c).start()

            @pl.when(k + s < n)
            def _():
                across(k + s, c).start()

    for c in range(CHUNKS):
        hop(0, c)
    local = pltpu.make_async_copy(own_ref, rows_ref.at[k, t], local_sem)
    local.start()

    for c in small[2:]:
        c.wait()

    acc_row = acc_ref[...]
    rate = pick(-jnp.exp(decay_ref[...]), heads, rank * heads)
    old_weights = [None] * props
    tail = jnp.zeros((heads, seqs), f32)
    for p in reversed(range(props)):
        mask = jnp.where(acc_row > p, 1.0, 0.0)
        old_weights[p] = mask * jnp.exp(tail) * last_ref[p]
        tail = tail + rate * last_ref[p] * mask
    turned = jnp.transpose(jnp.concatenate(old_weights + [jnp.exp(tail)], axis=0))
    lane = lax.broadcasted_iota(jnp.int32, (heads, cols), 1)
    row = lax.broadcasted_iota(jnp.int32, (heads, cols), 0)
    expand = jnp.where(lane // (cols // heads) == row, 1.0, 0.0).astype(bf16)
    for p in range(props):
        w = turned[:, p * heads : (p + 1) * heads]
        high, low = split_of(w)
        wide_buf[p] = jnp.dot(high, expand, preferred_element_type=f32) + jnp.dot(
            low, expand, preferred_element_type=f32
        )
    for h in range(heads):
        at = props * heads + h
        decay_buf[h] = jnp.broadcast_to(turned[:, at : at + 1], (seqs, states))
    acc = jnp.sum(
        jnp.where(
            lax.broadcasted_iota(jnp.int32, (seqs, seqs), 0)
            == lax.broadcasted_iota(jnp.int32, (seqs, seqs), 1),
            jnp.broadcast_to(acc_row, (seqs, seqs)),
            0,
        ).astype(f32),
        axis=1,
        keepdims=True,
    )

    def conv_parts(hist_at, taps, part_ref, b):
        where_at = jnp.broadcast_to(acc[b : b + BLOCK], hist_at[0].shape)
        current = []
        for e in range(width - 1):
            r = hist_at[e]
            for v in range(1, hist - width + 2):
                r = jnp.where(where_at == v, hist_at[e + v], r)
            current.append(r)
        for i in range(width - 1):
            total = taps[0:1] * current[i]
            for e in range(i + 1, width - 1):
                total = total + taps[e - i : e - i + 1] * current[e]
            part_ref[i, b : b + BLOCK, :] = total

    def conv_old(hist_at, taps):
        res = []
        for r in range(hist - width + 1):
            total = taps[0:1] * hist_at[r]
            for e in range(1, width):
                total = total + taps[e : e + 1] * hist_at[r + e]
            res.append(silu_of(total))
        return res

    def slabs(ref, b):
        return [ref[e, b : b + BLOCK, :].astype(f32) for e in range(hist)]

    taps_inner = own_slice(taps_inner_ref, rank * cols, cols)
    taps_write = own_slice(taps_write_ref, rank * states, states)
    taps_read = own_slice(taps_read_ref, rank * states, states)
    per_half = blocks // 2

    def prepare(part):
        lefts, rights = [], []
        for g in range(per_half):
            b = (part * per_half + g) * BLOCK
            h_inner = slabs(hist_inner_ref, b)
            h_write = slabs(hist_write_ref, b)
            olds = conv_old(h_inner, taps_inner)
            lefts += [wide_buf[p, b : b + BLOCK, :] * olds[p] for p in range(props)]
            rights += conv_old(h_write, taps_write)
            conv_parts(h_inner, taps_inner, part_inner_ref, b)
            conv_parts(h_write, taps_write, part_write_ref, b)
            conv_parts(slabs(hist_read_ref, b), taps_read, part_read_ref, b)
        turned_buf[part] = jnp.transpose(jnp.concatenate(lefts, axis=0)).astype(bf16)
        old_buf[part] = jnp.concatenate(rights, axis=0).astype(bf16)

    half_rows = per_half * props * BLOCK
    row = lax.broadcasted_iota(jnp.int32, (half_rows, states), 0)
    seq_of = row // (props * BLOCK) * BLOCK + row % BLOCK

    def update(part, first, count):
        lhs = turned_buf[part]
        old = old_buf[part].astype(f32)
        head_dim = cols // heads

        def pair(i, carry):
            at = first + 2 * i
            rhs = jnp.concatenate(
                [jnp.where(seq_of == at + e, old, 0.0).astype(bf16) for e in range(2)], axis=1
            )
            add = jnp.dot(lhs, rhs, preferred_element_type=f32)
            for e in range(2):
                s = part * (seqs // 2) + at + e
                for h in range(heads):
                    lo, hi = h * head_dim, (h + 1) * head_dim
                    d = decay_buf[h, pl.ds(s, 1), :]
                    new = d * base_ref[s, lo:hi, :] + add[lo:hi, e * states : (e + 1) * states]
                    base_ref[s, lo:hi, :] = new
                    half_ref[s, lo:hi, :] = new.astype(bf16)
            return carry

        lax.fori_loop(0, count // 2, pair, 0)

    hops = [(s, c) for s in range(1, n) for c in range(CHUNKS)]
    done = 0
    for part in range(2):
        prepare(part)
        for g in range(per_half):
            b = part * per_half + g
            fetch(b).wait()
            update(part, g * BLOCK, BLOCK)
            goal = len(hops) * (b + 1) // blocks
            while done < goal:
                hop(*hops[done])
                done += 1
    local.wait()
    for s in range(n - 1):
        for c in range(CHUNKS):
            @pl.when((k - s >= 0) & (k < n - 1))
            def _():
                to_right(s, c).wait_send()

            @pl.when((k + s < n) & (k > 0))
            def _():
                to_left(s, c).wait_send()
    for j in range(n):
        for c in range(CHUNKS):
            across(j, c).wait_send()
            there = rows_ref.at[j, 1 - t, :, pl.ds(c * span, span)]
            remote(there, there, fs.at[j, c], fr.at[j, c], partner).wait_recv()


kept = pltpu.with_memory_space_constraint


def lead(tokens, norm_gain, acc, last, decay_log, hi, hw, hr, ci, cw, cr, state):
    n = lax.axis_size("kv")
    rows, width = tokens.shape
    props, heads, seqs = last.shape
    cols, states = state.shape[1:]
    taps = ci.shape[0]
    dma = pltpu.SemaphoreType.DMA
    vmem = pl.BlockSpec(memory_space=pltpu.VMEM)
    hbm = pl.BlockSpec(memory_space=pltpu.HBM)
    f32, bf16 = jnp.float32, jnp.bfloat16
    shape = jax.ShapeDtypeStruct
    blocks = seqs // BLOCK
    half_rows = seqs // 2 * props
    small = (tokens, norm_gain, acc, last, decay_log, hi, hw, hr, ci, cw, cr)
    return pl.pallas_call(
        functools.partial(lead_kernel, n),
        out_shape=[
            shape((n, 2, rows, width), bf16),
            pltpu.VMEM(state.shape, f32),
            pltpu.VMEM(state.shape, bf16),
            shape((taps - 1, seqs, cols), f32),
            shape((taps - 1, seqs, states), f32),
            shape((taps - 1, seqs, states), f32),
        ],
        in_specs=[hbm] * (len(small) + 1),
        out_specs=[vmem] * 6,
        scratch_shapes=[
            pltpu.VMEM((rows, width), bf16),
            pltpu.VMEM((heads, seqs, states), f32),
            pltpu.VMEM((props, seqs, cols), f32),
            pltpu.VMEM((2, cols, half_rows), bf16),
            pltpu.VMEM((2, half_rows, states), bf16),
        ]
        + [dma((n - 1, CHUNKS))] * 4
        + [dma((n, CHUNKS))] * 2
        + [dma, dma((blocks,)), dma((len(small),))]
        + [pltpu.VMEM(x.shape, x.dtype) for x in small],
        compiler_params=pltpu.CompilerParams(
            collective_id=2, has_side_effects=True, vmem_limit_bytes=8 * 1024 * 1024
        ),
        name="lead",
    )(*[kept(x, pltpu.HBM) for x in small + (state,)])


def core_kernel(
    heads,
    rank_ref,
    rows_ref,
    base_ref,
    half_ref,
    part_inner_ref,
    part_write_ref,
    part_read_ref,
    inner_ref,
    write_ref,
    read_ref,
    step_ref,
    gate_ref,
    outw_ref,
    bias_ref,
    decay_ref,
    skip_ref,
    taps_inner_ref,
    taps_write_ref,
    taps_read_ref,
    gain_ref,
    out_ref,
    sq_ref,
    state_out,
    gate_buf,
    inner_buf,
    write_buf,
    read_buf,
    step_buf,
    un_buf,
    sems,
):
    f32, bf16 = jnp.float32, jnp.bfloat16
    rank = rank_ref[0]
    seqs, cols, states = base_ref.shape
    blocks = seqs // BLOCK
    props = rows_ref.shape[0] // seqs
    width = taps_inner_ref.shape[0]
    head_count = step_ref.shape[0]

    def flush(b):
        span = pl.ds(b * BLOCK, BLOCK)
        return pltpu.make_async_copy(base_ref.at[span], state_out.at[span], sems.at[b])

    for b in range(blocks):
        flush(b).start()
    rows = rows_ref[...]
    tile = 256
    for w_ref, buf in ((inner_ref, inner_buf), (gate_ref, gate_buf)):
        for lo in range(0, cols, tile):
            buf[:, lo : lo + tile] = round_of(
                jnp.dot(rows, w_ref[:, lo : lo + tile], preferred_element_type=f32)
            )
    both = jnp.dot(
        rows, jnp.concatenate([write_ref[...], read_ref[...]], axis=1), preferred_element_type=f32
    )
    write_buf[...] = round_of(both[:, :states])
    read_buf[...] = round_of(both[:, states:])
    nt = (((1,), (1,)), ((), ()))
    step_buf[...] = lax.dot_general(rows, step_ref[...], nt, preferred_element_type=f32)
    taps_inner = own_slice(taps_inner_ref, rank * cols, cols)
    taps_write = own_slice(taps_write_ref, rank * states, states)
    taps_read = own_slice(taps_read_ref, rank * states, states)
    gain = own_slice(gain_ref, rank * cols, cols)
    bias = bias_ref[...]
    rate = -jnp.exp(decay_ref[...])
    skip = skip_ref[...]
    lane = lax.broadcasted_iota(jnp.int32, (2 * head_count, cols), 1)
    row = lax.broadcasted_iota(jnp.int32, (2 * head_count, cols), 0)
    expand = jnp.where(
        lane // (cols // heads) + rank * heads == row % head_count, 1.0, 0.0
    ).astype(bf16)
    lane_of = lax.broadcasted_iota(jnp.int32, (BLOCK, 128), 1)
    row_r = lax.broadcasted_iota(jnp.int32, (props * BLOCK, states), 0) % BLOCK

    def block(r, carry):
        at_row = pl.multiple_of(r * props * BLOCK, props * BLOCK)
        at_seq = pl.multiple_of(r * BLOCK, BLOCK)

        def news(buf, part_ref, taps):
            fresh = [buf[pl.ds(at_row + i * BLOCK, BLOCK), :] for i in range(props)]
            res = []
            for i in range(props):
                total = taps[width - 1 : width] * fresh[i]
                for e in range(1, min(i, width - 1) + 1):
                    total = total + taps[width - 1 - e : width - e] * fresh[i - e]
                if i < width - 1:
                    total = total + part_ref[i, pl.ds(at_seq, BLOCK), :]
                res.append(silu_of(total))
            return res

        inner_new = news(inner_buf, part_inner_ref, taps_inner)
        write_new = [round_of(x) for x in news(write_buf, part_write_ref, taps_write)]
        read_new = [round_of(x) for x in news(read_buf, part_read_ref, taps_read)]
        steps = step_buf[pl.ds(at_row, props * BLOCK), :] + bias
        steps = jnp.maximum(steps, 0.0) + jnp.log1p(jnp.exp(-jnp.abs(steps)))
        step = [steps[i * BLOCK : (i + 1) * BLOCK] for i in range(props)]
        cums = []
        for i in range(props):
            cums.append(rate * step[i] + (cums[-1] if cums else 0.0))
        coefs = []
        where_of = {}
        for i in range(props):
            for j in range(i + 1):
                score = jnp.sum(read_new[i] * write_new[j], axis=-1, keepdims=True)
                c = jnp.exp(cums[i] - cums[j]) * step[j] * score
                if i == j:
                    c = c + skip
                where_of[(i, j)] = len(coefs)
                coefs.append(c)
        first_cum = len(coefs)
        coefs += [jnp.exp(c) for c in cums]
        high, low = split_of(jnp.concatenate(coefs, axis=0))
        wide = jnp.dot(
            jnp.concatenate([high, low], axis=1), expand, preferred_element_type=f32
        )

        def at(e):
            return wide[e * BLOCK : (e + 1) * BLOCK]

        read_all = jnp.concatenate(read_new, axis=0)
        carried = None
        for s in range(0, BLOCK, 2):
            lhs = jnp.concatenate(
                [jnp.where(row_r == s + e, read_all, 0.0).astype(bf16) for e in range(2)], axis=1
            )
            rhs = jnp.concatenate([half_ref[at_seq + s + e] for e in range(2)], axis=1)
            got = lax.dot_general(lhs, rhs, nt, preferred_element_type=f32)
            carried = got if carried is None else carried + got
        squares = jnp.zeros((BLOCK, 128), f32)
        outs = []
        for i in range(props):
            y = at(first_cum + i) * carried[i * BLOCK : (i + 1) * BLOCK]
            for j in range(i + 1):
                y = y + at(where_of[(i, j)]) * inner_new[j]
            g = y * silu_of(gate_buf[pl.ds(at_row + i * BLOCK, BLOCK), :])
            squares = jnp.where(lane_of == i, jnp.sum(g * g, axis=-1, keepdims=True), squares)
            outs.append(g * gain)
        sq_ref[r] = squares
        un_buf[pl.ds(at_row, props * BLOCK), :] = jnp.concatenate(outs, axis=0).astype(bf16)
        return carry

    lax.fori_loop(0, blocks, block, 0)
    un = un_buf[...]
    wide_tile = 512
    for lo in range(0, outw_ref.shape[1], wide_tile):
        out_ref[:, lo : lo + wide_tile] = jnp.dot(
            un, outw_ref[:, lo : lo + wide_tile], preferred_element_type=f32
        ).astype(bf16)
    for b in range(blocks):
        flush(b).wait()


def core(rank, heads, rows, base, half, parts, weights, bias, decay_log, skip, ci, cw, cr, gain):
    seqs, cols, states = base.shape
    tokens = rows.shape[0]
    width = weights[-1].shape[1]
    ranks = seqs // BLOCK
    f32, bf16 = jnp.float32, jnp.bfloat16
    vmem = pl.BlockSpec(memory_space=pltpu.VMEM)
    shape = jax.ShapeDtypeStruct
    return pl.pallas_call(
        functools.partial(core_kernel, heads),
        out_shape=[
            shape((tokens, width), bf16),
            shape((ranks, BLOCK, 128), f32),
            pltpu.HBM(base.shape, f32),
        ],
        in_specs=[pl.BlockSpec(memory_space=pltpu.SMEM)] + [vmem] * 19,
        out_specs=[vmem, vmem, pl.BlockSpec(memory_space=pl.ANY)],
        scratch_shapes=[
            pltpu.VMEM((tokens, cols), f32),
            pltpu.VMEM((tokens, cols), f32),
            pltpu.VMEM((tokens, states), f32),
            pltpu.VMEM((tokens, states), f32),
            pltpu.VMEM((tokens, weights[3].shape[0]), f32),
            pltpu.VMEM((tokens, cols), bf16),
            pltpu.SemaphoreType.DMA((ranks,)),
        ],
        compiler_params=pltpu.CompilerParams(vmem_limit_bytes=8 * 1024 * 1024),
        name="core",
    )(rank, rows, kept(base, pltpu.VMEM), kept(half, pltpu.VMEM), *parts, *weights, bias, decay_log, skip, ci, cw, cr, gain)


def tail_kernel(
    n, channels, part, sq, mixed, sqs, out, turned, pbuf, rbuf, lbuf, rout, lout, ps, pr, rs, rr, ls, lr, ss, sr
):
    f32 = jnp.float32
    k = lax.axis_index("kv")
    t = lax.axis_index("tp")
    rank = k * 2 + t
    ranks = n * 2
    right = {"kv": lax.rem(k + 1, n)}
    left = {"kv": lax.rem(k + n - 1, n)}
    partner = {"tp": 1 - t}
    span = part.shape[3] // CHUNKS
    barrier = pltpu.get_barrier_semaphore()

    def peer(o):
        p = lax.rem(rank + o, ranks)
        return {"kv": p // 2, "tp": lax.rem(p, 2)}

    for o in range(1, ranks):
        pl.semaphore_signal(barrier, inc=1, device_id=peer(o), device_id_type=MESH)
    pl.semaphore_wait(barrier, ranks - 1)

    def cut(c):
        return pl.ds(c * span, span)

    def across(j, c):
        return remote(
            part.at[j, 1 - t, :, cut(c)], pbuf.at[j, :, cut(c)], ps.at[j, c], pr.at[j, c], partner
        )

    def to_right(d, c):
        return remote(
            rout.at[d, :, cut(c)], rbuf.at[d, :, cut(c)], rs.at[d, c], rr.at[d, c], right
        )

    def to_left(d, c):
        return remote(lout.at[d, :, cut(c)], lbuf.at[d, :, cut(c)], ls.at[d, c], lr.at[d, c], left)

    def square(o):
        p = lax.rem(rank + o, ranks)
        return remote(sq.at[p], sqs.at[rank], ss.at[o], sr.at[o], peer(o))

    low = k < n // 2
    for i in range(n):
        j = jnp.where(low, n - 1 - i, i)
        for c in range(CHUNKS):
            across(j, c).start()
    for o in range(1, ranks):
        square(o).start()
    sqs[rank] = sq[rank]

    def pair(j, c):
        across(j, c).wait_recv()
        return part[j, t, :, cut(c)].astype(f32) + pbuf[j, :, cut(c)].astype(f32)

    def rightward():
        for d in range(n - 1, 0, -1):
            for c in range(CHUNKS):
                @pl.when((k < d) & (k == 0))
                def _():
                    rout[d, :, cut(c)] = pair(d, c).astype(rout.dtype)
                    to_right(d, c).start()

                @pl.when((k < d) & (k > 0))
                def _():
                    value = pair(d, c)
                    to_right(d, c).wait_recv()
                    rout[d, :, cut(c)] = (value + rbuf[d, :, cut(c)].astype(f32)).astype(rout.dtype)
                    to_right(d, c).start()

    def leftward():
        for d in range(n - 1):
            for c in range(CHUNKS):
                @pl.when((k > d) & (k == n - 1))
                def _():
                    lout[d, :, cut(c)] = pair(d, c).astype(lout.dtype)
                    to_left(d, c).start()

                @pl.when((k > d) & (k < n - 1))
                def _():
                    value = pair(d, c)
                    to_left(d, c).wait_recv()
                    lout[d, :, cut(c)] = (value + lbuf[d, :, cut(c)].astype(f32)).astype(lout.dtype)
                    to_left(d, c).start()

    @pl.when(k < n // 2)
    def _():
        rightward()
        leftward()

    @pl.when(k >= n // 2)
    def _():
        leftward()
        rightward()

    for c in range(CHUNKS):
        out[:, cut(c)] = pair(k, c)

        @pl.when(k > 0)
        def _():
            to_right(k, c).wait_recv()
            out[:, cut(c)] += rbuf[k, :, cut(c)].astype(f32)

        @pl.when(k < n - 1)
        def _():
            to_left(k, c).wait_recv()
            out[:, cut(c)] += lbuf[k, :, cut(c)].astype(f32)

    for o in range(1, ranks):
        square(o).wait_send()
        source = lax.rem(rank + ranks - o, ranks)
        remote(sq.at[rank], sqs.at[source], ss.at[o], sr.at[o], peer(o)).wait_recv()
    scale = lax.rsqrt(jnp.sum(sqs[...], axis=0) / channels + EPSILON)
    props = out.shape[0] // BLOCK
    for i in range(props):
        rows = out[i * BLOCK : (i + 1) * BLOCK, :] * scale[:, i : i + 1]
        turned[i * BLOCK : (i + 1) * BLOCK, :] = rows
    mixed[...] = jnp.dot(
        turn_rows(out.shape[0], props, True),
        turned[...].astype(mixed.dtype),
        preferred_element_type=f32,
    ).astype(mixed.dtype)
    for j in range(n):
        for c in range(CHUNKS):
            across(j, c).wait_send()

            @pl.when(k < j)
            def _():
                to_right(j, c).wait_send()

            @pl.when(k > j)
            def _():
                to_left(j, c).wait_send()


def finish(partial_value, squares, channels):
    n = lax.axis_size("kv")
    ranks = n * 2
    rows = partial_value.shape[0] // ranks
    cols = partial_value.shape[1]
    dma = pltpu.SemaphoreType.DMA
    vmem = pl.BlockSpec(memory_space=pltpu.VMEM)
    kind = partial_value.dtype
    f32 = jnp.float32
    return pl.pallas_call(
        functools.partial(tail_kernel, n, channels),
        out_shape=jax.ShapeDtypeStruct((rows, cols), kind),
        in_specs=[vmem, vmem],
        out_specs=vmem,
        scratch_shapes=[
            pltpu.VMEM(squares.shape, f32),
            pltpu.VMEM((rows, cols), f32),
            pltpu.VMEM((rows, cols), f32),
        ]
        + [pltpu.VMEM((n, rows, cols), kind)] * 5
        + [dma((n, CHUNKS))] * 6
        + [dma((ranks,))] * 2,
        compiler_params=pltpu.CompilerParams(
            collective_id=3, has_side_effects=True, vmem_limit_bytes=32 * 1024 * 1024
        ),
        name="tail",
    )(partial_value.reshape(n, 2, rows, cols), squares)


def whole_groups(tokens, saved_state, last_steps):
    span = lax.axis_size("kv") * lax.axis_size("tp")
    return span == GROUPS and tokens.shape[0] == BLOCK * last_steps.shape[1]


def quick(
    tokens,
    norm_gain,
    gate_proj,
    inner_proj,
    write_proj,
    read_proj,
    step_proj,
    step_bias,
    decay_log,
    skip_gain,
    conv_inner,
    conv_write,
    conv_read,
    out_gain,
    out_proj,
    saved_state,
    inner_history,
    write_history,
    read_history,
    last_steps,
    accepted,
):
    device_rank = lax.axis_index(("kv", "tp"))
    seqs, heads, head_dim, states = saved_state.shape
    slab = lambda x: x.transpose(1, 0, 2)
    row = lambda x: x.reshape(1, -1)
    weights = (inner_proj, write_proj, read_proj, step_proj.T, gate_proj, out_proj)
    got = lead(
        tokens,
        row(norm_gain),
        row(accepted),
        last_steps.transpose(1, 2, 0),
        row(decay_log),
        slab(inner_history),
        slab(write_history),
        slab(read_history),
        conv_inner,
        conv_write,
        conv_read,
        saved_state.reshape(seqs, heads * head_dim, states),
    )
    rows, base, half = got[:3]
    partial_value, squares, base_state = core(
        device_rank.reshape(1).astype(jnp.int32),
        heads,
        rows.reshape(-1, rows.shape[-1]),
        base,
        half,
        got[3:6],
        weights,
        row(step_bias),
        row(decay_log),
        row(skip_gain),
        conv_inner,
        conv_write,
        conv_read,
        row(out_gain),
    )
    mixed = finish(partial_value, squares, out_gain.shape[0])
    return (mixed, base_state.reshape(saved_state.shape))


def body(
    tokens,
    norm_gain,
    gate_proj,
    inner_proj,
    write_proj,
    read_proj,
    step_proj,
    step_bias,
    decay_log,
    skip_gain,
    conv_inner,
    conv_write,
    conv_read,
    out_gain,
    out_proj,
    saved_state,
    inner_history,
    write_history,
    read_history,
    last_steps,
    accepted,
):
    if whole_groups(tokens, saved_state, last_steps):
        return quick(
            tokens,
            norm_gain,
            gate_proj,
            inner_proj,
            write_proj,
            read_proj,
            step_proj,
            step_bias,
            decay_log,
            skip_gain,
            conv_inner,
            conv_write,
            conv_read,
            out_gain,
            out_proj,
            saved_state,
            inner_history,
            write_history,
            read_history,
            last_steps,
            accepted,
        )
    device_rank = lax.axis_index(("kv", "tp"))
    seq_count = saved_state.shape[0]
    local_heads = saved_state.shape[1]
    head_dim = saved_state.shape[2]
    proposals = last_steps.shape[1]
    inner_cols = inner_proj.shape[1]
    state_cols = write_proj.shape[1]
    token_count = tokens.shape[0]
    own_rows = tokens.astype(jnp.float32)
    normed_own = (
        own_rows
        * lax.rsqrt(jnp.mean(own_rows * own_rows, axis=-1, keepdims=True) + EPSILON)
        * norm_gain
    ).astype(jnp.bfloat16)
    normed = gathered(normed_own)
    normed = normed.reshape(seq_count, proposals, -1).transpose(1, 0, 2)
    normed = normed.reshape(proposals * seq_count, -1)

    def project(weight):
        out = jnp.dot(normed, weight, preferred_element_type=jnp.float32)
        return out.reshape(proposals, seq_count, -1)

    gate_rows = project(gate_proj).astype(jnp.bfloat16)
    inner_rows = project(inner_proj).astype(jnp.bfloat16)
    first_head = device_rank * local_heads
    state_cols = write_proj.shape[1]
    states = saved_state.shape[3]
    step_local = lax.dynamic_slice_in_dim(step_proj, first_head, local_heads, 1)
    step_local = jnp.pad(step_local, ((0, 0), (0, states - local_heads)))
    small = project(jnp.concatenate([write_proj, read_proj, step_local], axis=1))
    par = lax.dynamic_slice_in_dim(
        jnp.stack([step_bias, decay_log, skip_gain]), first_head, local_heads, 1
    )
    slab = lambda x: x.transpose(1, 0, 2)
    hist_inner, hist_write, hist_read = slab(inner_history), slab(write_history), slab(read_history)
    group_span = lax.axis_size("kv") * lax.axis_size("tp") // GROUPS
    if group_span >= 2:
        write_rows = small[:, :, :state_cols].astype(jnp.bfloat16)
        read_rows = small[:, :, state_cols : 2 * state_cols].astype(jnp.bfloat16)
        pieces = (write_rows, read_rows, hist_write, hist_read)
        pieces = tuple(lax.all_gather(x, "tp", axis=2, tiled=True) for x in pieces)
        kv_rank = lax.axis_index("kv")
        bit_count = (group_span // lax.axis_size("tp")).bit_length() - 1
        for bit in range(bit_count):
            partner = swapped(pieces, "kv", bit)
            lower = jnp.bitwise_and(jnp.right_shift(kv_rank, bit), 1) == 0
            pieces = tuple(
                jnp.where(
                    lower,
                    jnp.concatenate([mine, theirs], axis=2),
                    jnp.concatenate([theirs, mine], axis=2),
                )
                for mine, theirs in zip(pieces, partner)
            )
        write_rows, read_rows, hist_write, hist_read = pieces
        small = jnp.concatenate(
            [
                write_rows.astype(jnp.float32),
                read_rows.astype(jnp.float32),
                small[:, :, 2 * state_cols :],
            ],
            axis=2,
        )
    unscaled, squares, base_state = mix(
        device_rank,
        device_rank // group_span,
        accepted[:, None],
        slab(last_steps),
        par,
        gate_rows,
        inner_rows,
        small,
        hist_inner,
        hist_write,
        hist_read,
        conv_inner,
        conv_write,
        conv_read,
        out_gain[None, :],
        saved_state.reshape(seq_count, local_heads * head_dim, -1),
    )
    base_state = base_state.reshape(saved_state.shape)
    unscaled = unscaled.transpose(1, 0, 2).reshape(seq_count * proposals, inner_cols)
    partial_value = jnp.dot(unscaled, out_proj, preferred_element_type=jnp.float32)
    squares = squares[:, :, 0].T.reshape(-1)
    summed, square_own = scattered(partial_value.astype(jnp.bfloat16), squares)
    mixed = (summed * lax.rsqrt(square_own / out_gain.shape[0] + EPSILON)[:, None]).astype(jnp.bfloat16)
    return (mixed, base_state)


def solution(mesh):
    placed = (
        P(("dp", "kv", "tp"), None),
        P(),
        P(None, ("kv", "tp")),
        P(None, ("kv", "tp")),
        P(None, ("kv", "tp")),
        P(None, ("kv", "tp")),
        P(),
        P(),
        P(),
        P(),
        P(),
        P(),
        P(),
        P(),
        P(("kv", "tp"), None),
        P("dp", ("kv", "tp"), None, None),
        P("dp", None, ("kv", "tp")),
        P("dp", None, ("kv", "tp")),
        P("dp", None, ("kv", "tp")),
        P("dp", None, ("kv", "tp")),
        P("dp"),
    )
    return jax.shard_map(
        body,
        mesh=mesh,
        in_specs=placed,
        out_specs=(P(("dp", "kv", "tp"), None), P("dp", ("kv", "tp"), None, None)),
        check_vma=False,
    )
```

```python
import functools

import jax
import jax.numpy as jnp
from jax import lax
from jax.experimental import pallas as pl
from jax.experimental.pallas import tpu as pltpu
from jax.sharding import PartitionSpec as P

GROUPS = 8
EPSILON = 0.1
BLOCK = 8
highest = lax.Precision.HIGHEST


def swapped(value, axis, stride):
    mask = 2**stride
    pairs = [(source, source ^ mask) for source in range(lax.axis_size(axis))]
    return lax.ppermute(value, axis, pairs)


def mix_kernel(
    rank_ref,
    acc_ref,
    steps_ref,
    last_ref,
    par_ref,
    gate_ref,
    inner_ref,
    write_ref,
    read_ref,
    hist_inner_ref,
    hist_write_ref,
    hist_read_ref,
    taps_inner_ref,
    taps_write_ref,
    taps_read_ref,
    gain_ref,
    expand_ref,
    state_ref,
    un_ref,
    sq_ref,
    base_ref,
):
    f32 = jnp.float32
    props = steps_ref.shape[0]
    heads = last_ref.shape[2]
    cols = inner_ref.shape[2]
    states = write_ref.shape[2]
    head_dim = cols // heads
    hist = hist_inner_ref.shape[0]
    width = taps_inner_ref.shape[0]
    acc = acc_ref[...]

    def silu(x):
        return x / (1.0 + jnp.exp(-x))

    def slabs(ref):
        return [ref[k].astype(f32) for k in range(ref.shape[0])]

    round_bf = lambda x: x.astype(jnp.bfloat16).astype(f32)

    def conv(rows, taps_ref):
        taps = taps_ref[...].astype(f32)
        res = []
        for r in range(len(rows) - width + 1):
            v = taps[0:1] * rows[r]
            for k in range(1, width):
                v = v + taps[k : k + 1] * rows[r + k]
            res.append(silu(v))
        return res

    def current(h, new_ref):
        where_at = jnp.broadcast_to(acc, h[0].shape)
        rows = []
        for k in range(width - 1):
            r = h[k]
            for v in range(1, hist - width + 2):
                r = jnp.where(where_at == v, h[k + v], r)
            rows.append(r)
        return rows + [round_bf(x) for x in slabs(new_ref)]

    h_inner = slabs(hist_inner_ref)
    inner_old = conv(h_inner, taps_inner_ref)
    inner_new = conv(current(h_inner, inner_ref), taps_inner_ref)
    h_write = slabs(hist_write_ref)
    write_old = [round_bf(x) for x in conv(h_write, taps_write_ref)]
    write_new = [round_bf(x) for x in conv(current(h_write, write_ref), taps_write_ref)]
    read_new = [round_bf(x) for x in conv(current(slabs(hist_read_ref), read_ref), taps_read_ref)]

    bias = par_ref[0:1]
    rate = -jnp.exp(par_ref[1:2])
    skip = par_ref[2:3]
    acc_h = jnp.broadcast_to(acc, (BLOCK, heads))
    masks = [jnp.where(acc_h > t, 1.0, 0.0) for t in range(props)]
    logs = [rate * last_ref[t] * masks[t] for t in range(props)]
    coefs = [None] * props
    tail = jnp.zeros((BLOCK, heads), f32)
    for t in reversed(range(props)):
        coefs[t] = masks[t] * jnp.exp(tail) * last_ref[t]
        tail = tail + logs[t]
    decay = jnp.exp(tail)
    step = []
    for t in range(props):
        x = steps_ref[t][:, :heads] + bias
        step.append(jnp.maximum(x, 0.0) + jnp.log1p(jnp.exp(-jnp.abs(x))))
    cums = []
    for t in range(props):
        cums.append(rate * step[t] + (cums[-1] if cums else 0.0))
    where_of = {}
    for i in range(props):
        for j in range(i + 1):
            score = jnp.sum(read_new[i] * write_new[j], axis=-1, keepdims=True)
            c = jnp.exp(cums[i] - cums[j]) * step[j] * score
            if i == j:
                c = c + skip
            where_of[(i, j)] = len(coefs)
            coefs.append(c)
    first_cum = len(coefs)
    for i in range(props):
        coefs.append(jnp.exp(cums[i]))
    wide = jnp.dot(
        jnp.concatenate(coefs, axis=0),
        expand_ref[...],
        precision=highest,
        preferred_element_type=f32,
    )

    def at(k):
        return wide[k * BLOCK : (k + 1) * BLOCK]

    left = jnp.concatenate([at(t) * inner_old[t] for t in range(props)], axis=0)
    high = round_bf(left)
    both = jnp.concatenate([high, left - high], axis=0)
    turned = jnp.transpose(both).astype(jnp.bfloat16)
    write_all = jnp.concatenate(write_old + write_old, axis=0)
    read_all = jnp.concatenate(read_new, axis=0)
    seq_w = lax.broadcasted_iota(jnp.int32, write_all.shape, 0) % BLOCK
    seq_r = lax.broadcasted_iota(jnp.int32, read_all.shape, 0) % BLOCK
    carried = jnp.zeros((props * BLOCK, cols), f32)
    for s in range(BLOCK):
        right = jnp.where(seq_w == s, write_all, 0.0).astype(jnp.bfloat16)
        update = jnp.dot(turned, right, preferred_element_type=f32)
        parts = []
        for h in range(heads):
            lo, hi = h * head_dim, (h + 1) * head_dim
            d = jnp.broadcast_to(decay[s : s + 1, h : h + 1], (head_dim, states))
            new = d * state_ref[s, lo:hi, :] + update[lo:hi]
            base_ref[s, lo:hi, :] = new
            parts.append(new.astype(jnp.bfloat16))
        asked = jnp.where(seq_r == s, read_all, 0.0).astype(jnp.bfloat16)
        carried = carried + lax.dot_general(
            asked,
            jnp.concatenate(parts, axis=0),
            (((1,), (1,)), ((), ())),
            preferred_element_type=f32,
        )
    for i in range(props):
        y = at(first_cum + i) * carried[i * BLOCK : (i + 1) * BLOCK]
        for j in range(i + 1):
            y = y + at(where_of[(i, j)]) * inner_new[j]
        g = y * silu(gate_ref[i].astype(f32))
        sq_ref[i] = jnp.broadcast_to(jnp.sum(g * g, axis=-1, keepdims=True), sq_ref.shape[1:])
        un_ref[i] = (g * gain_ref[...]).astype(un_ref.dtype)


def mix(rank, group, acc, last, par, gate, inner, small, hi, hw, hr, ci, cw, cr, gain, state):
    props, seqs, heads = last.shape
    cols, states = state.shape[1], state.shape[2]
    expand = (jnp.arange(cols)[None, :] // (cols // heads) == jnp.arange(heads)[:, None]).astype(
        jnp.float32
    )
    hist = hi.shape[0]
    width = ci.shape[0]

    def slab(lead, last_dim):
        return pl.BlockSpec((lead, BLOCK, last_dim), lambda g, r: (0, g, 0))

    def piece(which):
        return pl.BlockSpec((props, BLOCK, states), lambda g, r: (0, g, which))

    def own(rows, last_dim, which):
        return pl.BlockSpec((rows, last_dim), lambda g, r: (0, r[which]))

    state_spec = pl.BlockSpec((BLOCK, cols, states), lambda g, r: (g, 0, 0))
    return pl.pallas_call(
        mix_kernel,
        grid_spec=pltpu.PrefetchScalarGridSpec(
            num_scalar_prefetch=1,
            grid=(seqs // BLOCK,),
            in_specs=[
                pl.BlockSpec((BLOCK, 1), lambda g, r: (g, 0)),
                piece(2),
                slab(props, heads),
                pl.BlockSpec(par.shape, lambda g, r: (0, 0)),
                slab(props, cols),
                slab(props, cols),
                piece(0),
                piece(1),
                slab(hist, cols),
                slab(hist, states),
                slab(hist, states),
                own(width, cols, 0),
                own(width, states, 1),
                own(width, states, 1),
                own(1, cols, 0),
                pl.BlockSpec(expand.shape, lambda g, r: (0, 0)),
                state_spec,
            ],
            out_specs=[slab(props, cols), slab(props, 128), state_spec],
        ),
        out_shape=[
            jax.ShapeDtypeStruct((props, seqs, cols), jnp.bfloat16),
            jax.ShapeDtypeStruct((props, seqs, 128), jnp.float32),
            jax.ShapeDtypeStruct(state.shape, jnp.float32),
        ],
        compiler_params=pltpu.CompilerParams(
            dimension_semantics=("arbitrary",), vmem_limit_bytes=48 * 1024 * 1024
        ),
        name="mix",
    )(
        jnp.stack([rank, group]).astype(jnp.int32),
        acc, small, last, par, gate, inner, small, small, hi, hw, hr, ci, cw, cr, gain, expand, state,
    )


MESH = pl.DeviceIdType.MESH
CHUNKS = 2


def remote(src, dst, send, recv, where):
    return pltpu.make_async_remote_copy(
        src_ref=src, dst_ref=dst, send_sem=send, recv_sem=recv, device_id=where, device_id_type=MESH
    )


def gather_kernel(n, own_ref, out_ref, rs, rr, ls, lr, fs, fr, local_sem):
    k = lax.axis_index("kv")
    t = lax.axis_index("tp")
    right = {"kv": lax.rem(k + 1, n)}
    left = {"kv": lax.rem(k + n - 1, n)}
    partner = {"tp": 1 - t}
    span = own_ref.shape[1] // CHUNKS
    barrier = pltpu.get_barrier_semaphore()
    pl.semaphore_signal(barrier, inc=1, device_id=partner, device_id_type=MESH)

    @pl.when(k < n - 1)
    def _():
        pl.semaphore_signal(barrier, inc=1, device_id=right, device_id_type=MESH)

    @pl.when(k > 0)
    def _():
        pl.semaphore_signal(barrier, inc=1, device_id=left, device_id_type=MESH)

    inner = (k > 0) & (k < n - 1)

    @pl.when(inner)
    def _():
        pl.semaphore_wait(barrier, 3)

    @pl.when(jnp.logical_not(inner))
    def _():
        pl.semaphore_wait(barrier, 2)

    def view(j, c):
        return out_ref.at[j, t, :, pl.ds(c * span, span)]

    def own(c):
        return own_ref.at[:, pl.ds(c * span, span)]

    def to_right(s, c):
        j = jnp.maximum(k - s, 0)
        return remote(own(c) if s == 0 else view(j, c), view(j, c), rs.at[s, c], rr.at[s, c], right)

    def to_left(s, c):
        j = jnp.minimum(k + s, n - 1)
        return remote(own(c) if s == 0 else view(j, c), view(j, c), ls.at[s, c], lr.at[s, c], left)

    def across(j, c, mine=False):
        return remote(own(c) if mine else view(j, c), view(j, c), fs.at[j, c], fr.at[j, c], partner)

    for s in range(n - 1):
        for c in range(CHUNKS):
            if s > 0:
                @pl.when(k - s >= 0)
                def _():
                    to_right(s - 1, c).wait_recv()

                @pl.when(k + s < n)
                def _():
                    to_left(s - 1, c).wait_recv()

            @pl.when((k - s >= 0) & (k < n - 1))
            def _():
                to_right(s, c).start()

            @pl.when((k + s < n) & (k > 0))
            def _():
                to_left(s, c).start()

            if s == 0:
                across(k, c, True).start()
            else:
                @pl.when(k - s >= 0)
                def _():
                    across(k - s, c).start()

                @pl.when(k + s < n)
                def _():
                    across(k + s, c).start()
        if s == 0:
            local = pltpu.make_async_copy(own_ref, out_ref.at[k, t], local_sem)
            local.start()
            local.wait()
    s = n - 1
    for c in range(CHUNKS):
        @pl.when(k - s >= 0)
        def _():
            to_right(s - 1, c).wait_recv()
            across(k - s, c).start()

        @pl.when(k + s < n)
        def _():
            to_left(s - 1, c).wait_recv()
            across(k + s, c).start()
    for s in range(n - 1):
        for c in range(CHUNKS):
            @pl.when((k - s >= 0) & (k < n - 1))
            def _():
                to_right(s, c).wait_send()

            @pl.when((k + s < n) & (k > 0))
            def _():
                to_left(s, c).wait_send()
    for j in range(n):
        for c in range(CHUNKS):
            across(j, c).wait_send()
            remote(
                out_ref.at[j, 1 - t, :, pl.ds(c * span, span)],
                out_ref.at[j, 1 - t, :, pl.ds(c * span, span)],
                fs.at[j, c],
                fr.at[j, c],
                partner,
            ).wait_recv()


def gathered(own):
    n = lax.axis_size("kv")
    rows, cols = own.shape
    dma = pltpu.SemaphoreType.DMA
    out = pl.pallas_call(
        functools.partial(gather_kernel, n),
        out_shape=jax.ShapeDtypeStruct((n, 2, rows, cols), own.dtype),
        in_specs=[pl.BlockSpec(memory_space=pltpu.VMEM)],
        out_specs=pl.BlockSpec(memory_space=pltpu.VMEM),
        scratch_shapes=[dma((n - 1, CHUNKS))] * 4 + [dma((n, CHUNKS))] * 2 + [dma],
        compiler_params=pltpu.CompilerParams(
            collective_id=0, has_side_effects=True, vmem_limit_bytes=32 * 1024 * 1024
        ),
        name="gather",
    )(own)
    return out.reshape(n * 2 * rows, cols)


def scatter_kernel(
    n, part, sq, out, sqs, pbuf, rbuf, lbuf, rout, lout, ps, pr, rs, rr, ls, lr, ss, sr
):
    f32 = jnp.float32
    k = lax.axis_index("kv")
    t = lax.axis_index("tp")
    rank = k * 2 + t
    ranks = n * 2
    right = {"kv": lax.rem(k + 1, n)}
    left = {"kv": lax.rem(k + n - 1, n)}
    partner = {"tp": 1 - t}
    span = part.shape[3] // CHUNKS
    barrier = pltpu.get_barrier_semaphore()

    def peer(o):
        p = lax.rem(rank + o, ranks)
        return {"kv": p // 2, "tp": lax.rem(p, 2)}

    for o in range(1, ranks):
        pl.semaphore_signal(barrier, inc=1, device_id=peer(o), device_id_type=MESH)
    pl.semaphore_wait(barrier, ranks - 1)

    def cut(c):
        return pl.ds(c * span, span)

    def across(j, c):
        return remote(
            part.at[j, 1 - t, :, cut(c)], pbuf.at[j, :, cut(c)], ps.at[j, c], pr.at[j, c], partner
        )

    def to_right(d, c):
        return remote(
            rout.at[d, :, cut(c)], rbuf.at[d, :, cut(c)], rs.at[d, c], rr.at[d, c], right
        )

    def to_left(d, c):
        return remote(lout.at[d, :, cut(c)], lbuf.at[d, :, cut(c)], ls.at[d, c], lr.at[d, c], left)

    def square(o):
        p = lax.rem(rank + o, ranks)
        return remote(sq.at[p], sqs.at[rank], ss.at[o], sr.at[o], peer(o))

    low = k < n // 2
    for i in range(n):
        j = jnp.where(low, n - 1 - i, i)
        for c in range(CHUNKS):
            across(j, c).start()
    for o in range(1, ranks):
        square(o).start()
    sqs[rank] = sq[rank]

    def pair(j, c):
        across(j, c).wait_recv()
        return part[j, t, :, cut(c)].astype(f32) + pbuf[j, :, cut(c)].astype(f32)

    def rightward():
        for d in range(n - 1, 0, -1):
            for c in range(CHUNKS):
                @pl.when((k < d) & (k == 0))
                def _():
                    rout[d, :, cut(c)] = pair(d, c).astype(rout.dtype)
                    to_right(d, c).start()

                @pl.when((k < d) & (k > 0))
                def _():
                    value = pair(d, c)
                    to_right(d, c).wait_recv()
                    rout[d, :, cut(c)] = (value + rbuf[d, :, cut(c)].astype(f32)).astype(rout.dtype)
                    to_right(d, c).start()

    def leftward():
        for d in range(n - 1):
            for c in range(CHUNKS):
                @pl.when((k > d) & (k == n - 1))
                def _():
                    lout[d, :, cut(c)] = pair(d, c).astype(lout.dtype)
                    to_left(d, c).start()

                @pl.when((k > d) & (k < n - 1))
                def _():
                    value = pair(d, c)
                    to_left(d, c).wait_recv()
                    lout[d, :, cut(c)] = (value + lbuf[d, :, cut(c)].astype(f32)).astype(lout.dtype)
                    to_left(d, c).start()

    @pl.when(k < n // 2)
    def _():
        rightward()
        leftward()

    @pl.when(k >= n // 2)
    def _():
        leftward()
        rightward()

    for c in range(CHUNKS):
        out[:, cut(c)] = pair(k, c)

        @pl.when(k > 0)
        def _():
            to_right(k, c).wait_recv()
            out[:, cut(c)] += rbuf[k, :, cut(c)].astype(f32)

        @pl.when(k < n - 1)
        def _():
            to_left(k, c).wait_recv()
            out[:, cut(c)] += lbuf[k, :, cut(c)].astype(f32)

    for j in range(n):
        for c in range(CHUNKS):
            across(j, c).wait_send()

            @pl.when(k < j)
            def _():
                to_right(j, c).wait_send()

            @pl.when(k > j)
            def _():
                to_left(j, c).wait_send()
    for o in range(1, ranks):
        square(o).wait_send()
        source = lax.rem(rank + ranks - o, ranks)
        remote(sq.at[rank], sqs.at[source], ss.at[o], sr.at[o], peer(o)).wait_recv()


def scattered(partial_value, squares):
    n = lax.axis_size("kv")
    ranks = n * 2
    rows = partial_value.shape[0] // ranks
    cols = partial_value.shape[1]
    squares = jnp.pad(squares.reshape(ranks, 1, rows), ((0, 0), (0, 7), (0, 128 - rows)))
    dma = pltpu.SemaphoreType.DMA
    vmem = pl.BlockSpec(memory_space=pltpu.VMEM)
    kind = partial_value.dtype
    summed, sqs = pl.pallas_call(
        functools.partial(scatter_kernel, n),
        out_shape=[
            jax.ShapeDtypeStruct((rows, cols), jnp.float32),
            jax.ShapeDtypeStruct(squares.shape, jnp.float32),
        ],
        in_specs=[vmem, vmem],
        out_specs=[vmem, vmem],
        scratch_shapes=[pltpu.VMEM((n, rows, cols), kind)] * 5
        + [dma((n, CHUNKS))] * 6
        + [dma((ranks,))] * 2,
        compiler_params=pltpu.CompilerParams(
            collective_id=1, has_side_effects=True, vmem_limit_bytes=32 * 1024 * 1024
        ),
        name="scatter",
    )(partial_value.reshape(n, 2, rows, cols), squares)
    return summed, jnp.sum(sqs[:, 0, :rows], axis=0)


AHEAD = 3
CARRY = 4
HOPS_AT = (0, 1, 1, 2, 3, 4, 5, 6)


def pick(x, rows, first):
    wide = jnp.broadcast_to(x, (rows, x.shape[1]))
    lane = lax.broadcasted_iota(jnp.int32, wide.shape, 1)
    row = lax.broadcasted_iota(jnp.int32, wide.shape, 0)
    return jnp.sum(jnp.where(lane == row + first, wide, 0.0), axis=1, keepdims=True)


def turn_rows(rows, props, back=False):
    seqs = rows // props
    row = lax.broadcasted_iota(jnp.int32, (rows, rows), 0)
    col = lax.broadcasted_iota(jnp.int32, (rows, rows), 1)
    if back:
        row, col = col, row
    return jnp.where(col == row % seqs * props + row // seqs, 1.0, 0.0).astype(jnp.bfloat16)


def silu_of(x):
    return x / (1.0 + jnp.exp(-x))


def round_of(x):
    return x.astype(jnp.bfloat16).astype(jnp.float32)


def split_of(x):
    high = x.astype(jnp.bfloat16)
    return high, (x - high.astype(jnp.float32)).astype(jnp.bfloat16)


def own_slice(ref, first, count):
    return ref[:, pl.ds(pl.multiple_of(first, 128), count)].astype(jnp.float32)


def lead_kernel(
    n,
    tokens_hbm,
    norm_hbm,
    acc_hbm,
    last_hbm,
    decay_hbm,
    hist_inner_hbm,
    hist_write_hbm,
    hist_read_hbm,
    taps_inner_hbm,
    taps_write_hbm,
    taps_read_hbm,
    state_ref,
    inner_hbm,
    write_hbm,
    read_hbm,
    step_hbm,
    gate_hbm,
    outw_hbm,
    rows_ref,
    base_ref,
    half_ref,
    part_inner_ref,
    part_write_ref,
    part_read_ref,
    inner_ref,
    write_ref,
    read_ref,
    step_ref,
    gate_ref,
    outw_ref,
    own_ref,
    decay_buf,
    wide_buf,
    turned_buf,
    old_buf,
    rs,
    rr,
    ls,
    lr,
    fs,
    fr,
    local_sem,
    state_sems,
    small_sems,
    weight_sems,
    tokens_ref,
    norm_ref,
    acc_ref,
    last_ref,
    decay_ref,
    hist_inner_ref,
    hist_write_ref,
    hist_read_ref,
    taps_inner_ref,
    taps_write_ref,
    taps_read_ref,
):
    f32 = jnp.float32
    bf16 = jnp.bfloat16
    k = lax.axis_index("kv")
    t = lax.axis_index("tp")
    rank = k * 2 + t
    right = {"kv": lax.rem(k + 1, n)}
    left = {"kv": lax.rem(k + n - 1, n)}
    partner = {"tp": 1 - t}
    barrier = pltpu.get_barrier_semaphore()
    pl.semaphore_signal(barrier, inc=1, device_id=partner, device_id_type=MESH)

    @pl.when(k < n - 1)
    def _():
        pl.semaphore_signal(barrier, inc=1, device_id=right, device_id_type=MESH)

    @pl.when(k > 0)
    def _():
        pl.semaphore_signal(barrier, inc=1, device_id=left, device_id_type=MESH)

    props, heads, seqs = last_ref.shape
    cols = base_ref.shape[1]
    states = base_ref.shape[2]
    hist = hist_inner_ref.shape[0]
    width = taps_inner_ref.shape[0]
    blocks = seqs // BLOCK

    def fetch(b):
        span = pl.ds(b * BLOCK, BLOCK)
        return pltpu.make_async_copy(state_ref.at[span], base_ref.at[span], state_sems.at[b])

    small = [
        pltpu.make_async_copy(src, dst, small_sems.at[i])
        for i, (src, dst) in enumerate(
            [
                (tokens_hbm, tokens_ref),
                (norm_hbm, norm_ref),
                (acc_hbm, acc_ref),
                (last_hbm, last_ref),
                (decay_hbm, decay_ref),
                (hist_inner_hbm, hist_inner_ref),
                (hist_write_hbm, hist_write_ref),
                (hist_read_hbm, hist_read_ref),
                (taps_inner_hbm, taps_inner_ref),
                (taps_write_hbm, taps_write_ref),
                (taps_read_hbm, taps_read_ref),
            ]
        )
    ]
    for c in small:
        c.start()
    weights = [
        pltpu.make_async_copy(src, dst, weight_sems.at[i])
        for i, (src, dst) in enumerate(
            [
                (inner_hbm, inner_ref),
                (write_hbm, write_ref),
                (read_hbm, read_ref),
                (step_hbm, step_ref),
                (gate_hbm, gate_ref),
                (outw_hbm, outw_ref),
            ]
        )
    ]
    queue = [fetch(b) for b in range(blocks)] + weights
    for c in queue[:AHEAD]:
        c.start()
    for c in small[:2]:
        c.wait()
    own = tokens_ref[...].astype(f32)
    scale = lax.rsqrt(jnp.mean(own * own, axis=-1, keepdims=True) + EPSILON)
    normed = (own * scale * norm_ref[...]).astype(bf16)
    own_ref[...] = jnp.dot(
        turn_rows(own.shape[0], props), normed, preferred_element_type=f32
    ).astype(bf16)

    inside = (k > 0) & (k < n - 1)

    @pl.when(inside)
    def _():
        pl.semaphore_wait(barrier, 3)

    @pl.when(jnp.logical_not(inside))
    def _():
        pl.semaphore_wait(barrier, 2)

    span = own_ref.shape[1] // CHUNKS

    def view(j, c):
        return rows_ref.at[j, t, :, pl.ds(c * span, span)]

    def mine(c):
        return own_ref.at[:, pl.ds(c * span, span)]

    def to_right(s, c):
        j = jnp.maximum(k - s, 0)
        return remote(mine(c) if s == 0 else view(j, c), view(j, c), rs.at[s, c], rr.at[s, c], right)

    def to_left(s, c):
        j = jnp.minimum(k + s, n - 1)
        return remote(mine(c) if s == 0 else view(j, c), view(j, c), ls.at[s, c], lr.at[s, c], left)

    def across(j, c, first=False):
        return remote(mine(c) if first else view(j, c), view(j, c), fs.at[j, c], fr.at[j, c], partner)

    def hop(s, c):
        if s > 0:
            @pl.when(k - s >= 0)
            def _():
                to_right(s - 1, c).wait_recv()

            @pl.when(k + s < n)
            def _():
                to_left(s - 1, c).wait_recv()

        if s < n - 1:
            @pl.when((k - s >= 0) & (k < n - 1))
            def _():
                to_right(s, c).start()

            @pl.when((k + s < n) & (k > 0))
            def _():
                to_left(s, c).start()

        if s == 0:
            across(k, c, True).start()
        else:
            @pl.when(k - s >= 0)
            def _():
                across(k - s, c).start()

            @pl.when(k + s < n)
            def _():
                across(k + s, c).start()

    for c in range(CHUNKS):
        hop(0, c)
    local = pltpu.make_async_copy(own_ref, rows_ref.at[k, t], local_sem)
    local.start()

    for c in small[2:]:
        c.wait()

    acc_row = acc_ref[...]
    rate = pick(-jnp.exp(decay_ref[...]), heads, rank * heads)
    old_weights = [None] * props
    tail = jnp.zeros((heads, seqs), f32)
    for p in reversed(range(props)):
        mask = jnp.where(acc_row > p, 1.0, 0.0)
        old_weights[p] = mask * jnp.exp(tail) * last_ref[p]
        tail = tail + rate * last_ref[p] * mask
    turned = jnp.transpose(jnp.concatenate(old_weights + [jnp.exp(tail)], axis=0))
    lane = lax.broadcasted_iota(jnp.int32, (heads, cols), 1)
    row = lax.broadcasted_iota(jnp.int32, (heads, cols), 0)
    expand = jnp.where(lane // (cols // heads) == row, 1.0, 0.0).astype(bf16)
    for p in range(props):
        w = turned[:, p * heads : (p + 1) * heads]
        high, low = split_of(w)
        wide_buf[p] = jnp.dot(high, expand, preferred_element_type=f32) + jnp.dot(
            low, expand, preferred_element_type=f32
        )
    for h in range(heads):
        at = props * heads + h
        decay_buf[h] = jnp.broadcast_to(turned[:, at : at + 1], (seqs, states))
    acc = jnp.sum(
        jnp.where(
            lax.broadcasted_iota(jnp.int32, (seqs, seqs), 0)
            == lax.broadcasted_iota(jnp.int32, (seqs, seqs), 1),
            jnp.broadcast_to(acc_row, (seqs, seqs)),
            0,
        ).astype(f32),
        axis=1,
        keepdims=True,
    )

    def conv_parts(hist_at, taps, part_ref, b):
        where_at = jnp.broadcast_to(acc[b : b + BLOCK], hist_at[0].shape)
        current = []
        for e in range(width - 1):
            r = hist_at[e]
            for v in range(1, hist - width + 2):
                r = jnp.where(where_at == v, hist_at[e + v], r)
            current.append(r)
        for i in range(width - 1):
            total = taps[0:1] * current[i]
            for e in range(i + 1, width - 1):
                total = total + taps[e - i : e - i + 1] * current[e]
            part_ref[i, b : b + BLOCK, :] = total

    def conv_old(hist_at, taps):
        res = []
        for r in range(hist - width + 1):
            total = taps[0:1] * hist_at[r]
            for e in range(1, width):
                total = total + taps[e : e + 1] * hist_at[r + e]
            res.append(silu_of(total))
        return res

    def slabs(ref, b):
        return [ref[e, b : b + BLOCK, :].astype(f32) for e in range(hist)]

    taps_inner = own_slice(taps_inner_ref, rank * cols, cols)
    taps_write = own_slice(taps_write_ref, rank * states, states)
    taps_read = own_slice(taps_read_ref, rank * states, states)
    per_half = blocks // 2

    def prepare(part):
        lefts, rights = [], []
        for g in range(per_half):
            b = (part * per_half + g) * BLOCK
            h_inner = slabs(hist_inner_ref, b)
            h_write = slabs(hist_write_ref, b)
            olds = conv_old(h_inner, taps_inner)
            lefts += [wide_buf[p, b : b + BLOCK, :] * olds[p] for p in range(props)]
            rights += conv_old(h_write, taps_write)
            conv_parts(h_inner, taps_inner, part_inner_ref, b)
            conv_parts(h_write, taps_write, part_write_ref, b)
            conv_parts(slabs(hist_read_ref, b), taps_read, part_read_ref, b)
        turned_buf[part] = jnp.transpose(jnp.concatenate(lefts, axis=0)).astype(bf16)
        old_buf[part] = jnp.concatenate(rights, axis=0).astype(bf16)

    half_rows = per_half * props * BLOCK
    row = lax.broadcasted_iota(jnp.int32, (half_rows, states), 0)
    seq_of = row // (props * BLOCK) * BLOCK + row % BLOCK

    def update(part, first, count):
        lhs = turned_buf[part]
        old = old_buf[part].astype(f32)
        head_dim = cols // heads

        adds = []
        for i in range(0, count, 2):
            rhs = jnp.concatenate(
                [jnp.where(seq_of == first + i + e, old, 0.0).astype(bf16) for e in range(2)],
                axis=1,
            )
            adds.append(jnp.dot(lhs, rhs, preferred_element_type=f32))
        for i in range(count):
            s = part * (seqs // 2) + first + i
            add = adds[i // 2]
            side = i % 2 * states
            for h in range(heads):
                lo, hi = h * head_dim, (h + 1) * head_dim
                new = decay_buf[h, s : s + 1, :] * base_ref[s, lo:hi, :]
                new = new + add[lo:hi, side : side + states]
                base_ref[s, lo:hi, :] = new
                half_ref[s, lo:hi, :] = new.astype(bf16)

    hops = [(s, c) for s in range(1, n) for c in range(CHUNKS)]
    done = 0
    for part in range(2):
        prepare(part)
        for g in range(per_half):
            b = part * per_half + g
            queue[b].wait()
            more = queue[b + AHEAD : b + AHEAD + 1] if b + 1 < blocks else queue[b + AHEAD :]
            for c in more:
                c.start()
            update(part, g * BLOCK, BLOCK)
            goal = len(hops) * HOPS_AT[b] // 6
            while done < goal:
                hop(*hops[done])
                done += 1
    for w in weights:
        w.wait()
    local.wait()
    for s in range(n - 1):
        for c in range(CHUNKS):
            @pl.when((k - s >= 0) & (k < n - 1))
            def _():
                to_right(s, c).wait_send()

            @pl.when((k + s < n) & (k > 0))
            def _():
                to_left(s, c).wait_send()
    for j in range(n):
        for c in range(CHUNKS):
            across(j, c).wait_send()
            there = rows_ref.at[j, 1 - t, :, pl.ds(c * span, span)]
            remote(there, there, fs.at[j, c], fr.at[j, c], partner).wait_recv()


kept = pltpu.with_memory_space_constraint


def lead(tokens, norm_gain, acc, last, decay_log, hi, hw, hr, ci, cw, cr, state, weights):
    n = lax.axis_size("kv")
    rows, width = tokens.shape
    props, heads, seqs = last.shape
    cols, states = state.shape[1:]
    taps = ci.shape[0]
    dma = pltpu.SemaphoreType.DMA
    vmem = pl.BlockSpec(memory_space=pltpu.VMEM)
    hbm = pl.BlockSpec(memory_space=pltpu.HBM)
    f32, bf16 = jnp.float32, jnp.bfloat16
    shape = jax.ShapeDtypeStruct
    blocks = seqs // BLOCK
    half_rows = seqs // 2 * props
    small = (tokens, norm_gain, acc, last, decay_log, hi, hw, hr, ci, cw, cr)
    return pl.pallas_call(
        functools.partial(lead_kernel, n),
        out_shape=[
            shape((n, 2, rows, width), bf16),
            pltpu.VMEM(state.shape, f32),
            pltpu.VMEM(state.shape, bf16),
            shape((taps - 1, seqs, cols), f32),
            shape((taps - 1, seqs, states), f32),
            shape((taps - 1, seqs, states), f32),
        ]
        + [pltpu.VMEM(w.shape, w.dtype) for w in weights],
        in_specs=[hbm] * (len(small) + 1 + len(weights)),
        out_specs=[vmem] * (6 + len(weights)),
        scratch_shapes=[
            pltpu.VMEM((rows, width), bf16),
            pltpu.VMEM((heads, seqs, states), f32),
            pltpu.VMEM((props, seqs, cols), f32),
            pltpu.VMEM((2, cols, half_rows), bf16),
            pltpu.VMEM((2, half_rows, states), bf16),
        ]
        + [dma((n - 1, CHUNKS))] * 4
        + [dma((n, CHUNKS))] * 2
        + [dma, dma((blocks,)), dma((len(small),)), dma((len(weights),))]
        + [pltpu.VMEM(x.shape, x.dtype) for x in small],
        compiler_params=pltpu.CompilerParams(
            collective_id=2, has_side_effects=True, vmem_limit_bytes=8 * 1024 * 1024
        ),
        name="lead",
    )(*[kept(x, pltpu.HBM) for x in small + (state,) + weights])


def core_kernel(
    heads,
    rank_ref,
    rows_ref,
    base_ref,
    half_ref,
    part_inner_ref,
    part_write_ref,
    part_read_ref,
    inner_ref,
    write_ref,
    read_ref,
    step_ref,
    gate_ref,
    outw_ref,
    bias_ref,
    decay_ref,
    skip_ref,
    taps_inner_ref,
    taps_write_ref,
    taps_read_ref,
    gain_ref,
    out_ref,
    sq_ref,
    state_out,
    gate_buf,
    inner_buf,
    write_buf,
    read_buf,
    step_buf,
    un_buf,
    carried_buf,
    wide_buf,
    sems,
):
    f32, bf16 = jnp.float32, jnp.bfloat16
    rank = rank_ref[0]
    seqs, cols, states = base_ref.shape
    blocks = seqs // BLOCK
    props = rows_ref.shape[0] // seqs
    width = taps_inner_ref.shape[0]
    head_count = step_ref.shape[0]

    def flush(b):
        span = pl.ds(b * BLOCK, BLOCK)
        return pltpu.make_async_copy(base_ref.at[span], state_out.at[span], sems.at[b])

    for b in range(blocks):
        flush(b).start()
    rows = rows_ref[...]
    tile = 256
    for w_ref, buf in ((inner_ref, inner_buf), (gate_ref, gate_buf)):
        for lo in range(0, cols, tile):
            buf[:, lo : lo + tile] = round_of(
                jnp.dot(rows, w_ref[:, lo : lo + tile], preferred_element_type=f32)
            )
    both = jnp.dot(
        rows, jnp.concatenate([write_ref[...], read_ref[...]], axis=1), preferred_element_type=f32
    )
    write_buf[...] = round_of(both[:, :states])
    read_buf[...] = round_of(both[:, states:])
    nt = (((1,), (1,)), ((), ()))
    step_buf[...] = lax.dot_general(rows, step_ref[...], nt, preferred_element_type=f32)
    taps_inner = own_slice(taps_inner_ref, rank * cols, cols)
    taps_write = own_slice(taps_write_ref, rank * states, states)
    taps_read = own_slice(taps_read_ref, rank * states, states)
    gain = own_slice(gain_ref, rank * cols, cols)
    bias = bias_ref[...]
    rate = -jnp.exp(decay_ref[...])
    skip = skip_ref[...]
    lane = lax.broadcasted_iota(jnp.int32, (2 * head_count, cols), 1)
    row = lax.broadcasted_iota(jnp.int32, (2 * head_count, cols), 0)
    expand = jnp.where(
        lane // (cols // heads) + rank * heads == row % head_count, 1.0, 0.0
    ).astype(bf16)
    lane_of = lax.broadcasted_iota(jnp.int32, (BLOCK, 128), 1)

    rows_of = props * BLOCK
    pairs_of = {}
    for i in range(props):
        for j in range(i + 1):
            pairs_of[(i, j)] = len(pairs_of)
    first_cum = len(pairs_of)

    def prepare(r):
        at_row = pl.multiple_of(r * rows_of, rows_of)
        at_seq = pl.multiple_of(r * BLOCK, BLOCK)

        def news(buf, part_ref, taps):
            fresh = [buf[pl.ds(at_row + i * BLOCK, BLOCK), :] for i in range(props)]
            res = []
            for i in range(props):
                total = taps[width - 1 : width] * fresh[i]
                for e in range(1, min(i, width - 1) + 1):
                    total = total + taps[width - 1 - e : width - e] * fresh[i - e]
                if i < width - 1:
                    total = total + part_ref[i, pl.ds(at_seq, BLOCK), :]
                res.append(silu_of(total))
            return res

        inner_new = news(inner_buf, part_inner_ref, taps_inner)
        for i in range(props):
            inner_buf[pl.ds(at_row + i * BLOCK, BLOCK), :] = inner_new[i]
        write_new = [round_of(x) for x in news(write_buf, part_write_ref, taps_write)]
        read_new = [round_of(x) for x in news(read_buf, part_read_ref, taps_read)]
        for i in range(props):
            read_buf[pl.ds(at_row + i * BLOCK, BLOCK), :] = read_new[i]
        steps = step_buf[pl.ds(at_row, rows_of), :] + bias
        steps = jnp.maximum(steps, 0.0) + jnp.log1p(jnp.exp(-jnp.abs(steps)))
        step = [steps[i * BLOCK : (i + 1) * BLOCK] for i in range(props)]
        cums = []
        for i in range(props):
            cums.append(rate * step[i] + (cums[-1] if cums else 0.0))
        coefs = []
        for i, j in pairs_of:
            score = jnp.sum(read_new[i] * write_new[j], axis=-1, keepdims=True)
            c = jnp.exp(cums[i] - cums[j]) * step[j] * score
            coefs.append(c + skip if i == j else c)
        coefs += [jnp.exp(c) for c in cums]
        high, low = split_of(jnp.concatenate(coefs, axis=0))
        wide_buf[r] = jnp.dot(
            jnp.concatenate([high, low], axis=1), expand, preferred_element_type=f32
        )

    def carry_over(first):
        span = CARRY * rows_of
        at_row = first * rows_of
        asked = jnp.transpose(read_buf[at_row : at_row + span, :])
        col = lax.broadcasted_iota(jnp.int32, asked.shape, 1)
        seq_of = col // rows_of * BLOCK + col % BLOCK
        total = None
        for s in range(0, CARRY * BLOCK, 2):
            at = first * BLOCK + s
            lhs = jnp.concatenate([half_ref[at + e] for e in range(2)], axis=1)
            rhs = jnp.concatenate(
                [jnp.where(seq_of == s + e, asked, 0.0).astype(bf16) for e in range(2)], axis=0
            )
            got = jnp.dot(lhs, rhs, preferred_element_type=f32)
            total = got if total is None else total + got
        carried_buf[at_row : at_row + span, :] = jnp.transpose(total)

    def finish_rows(r):
        at_row = pl.multiple_of(r * rows_of, rows_of)

        def at(e):
            return wide_buf[r, e * BLOCK : (e + 1) * BLOCK, :]

        def part(buf, i):
            return buf[pl.ds(at_row + i * BLOCK, BLOCK), :]

        squares = jnp.zeros((BLOCK, 128), f32)
        outs = []
        for i in range(props):
            y = at(first_cum + i) * part(carried_buf, i)
            for j in range(i + 1):
                y = y + at(pairs_of[(i, j)]) * part(inner_buf, j)
            g = y * silu_of(part(gate_buf, i))
            squares = jnp.where(lane_of == i, jnp.sum(g * g, axis=-1, keepdims=True), squares)
            outs.append(g * gain)
        sq_ref[r] = squares
        un_buf[pl.ds(at_row, rows_of), :] = jnp.concatenate(outs, axis=0).astype(bf16)

    def each(fn, lo, hi, step):
        def run(i, carry):
            for u in range(step):
                fn(lo + i * step + u)
            return carry

        lax.fori_loop(0, (hi - lo) // step, run, 0)

    each(prepare, 0, blocks, 2)
    for first in range(0, blocks, CARRY):
        carry_over(first)
    each(finish_rows, 0, blocks, 2)
    un = un_buf[...]
    wide_tile = 512
    for lo in range(0, outw_ref.shape[1], wide_tile):
        out_ref[:, lo : lo + wide_tile] = jnp.dot(
            un, outw_ref[:, lo : lo + wide_tile], preferred_element_type=f32
        ).astype(bf16)
    for b in range(blocks):
        flush(b).wait()


def core(rank, heads, rows, base, half, parts, weights, bias, decay_log, skip, ci, cw, cr, gain):
    seqs, cols, states = base.shape
    tokens = rows.shape[0]
    width = weights[-1].shape[1]
    ranks = seqs // BLOCK
    props = tokens // seqs
    coefs = props * (props + 1) // 2 + props
    f32, bf16 = jnp.float32, jnp.bfloat16
    vmem = pl.BlockSpec(memory_space=pltpu.VMEM)
    shape = jax.ShapeDtypeStruct
    return pl.pallas_call(
        functools.partial(core_kernel, heads),
        out_shape=[
            shape((tokens, width), bf16),
            shape((ranks, BLOCK, 128), f32),
            pltpu.HBM(base.shape, f32),
        ],
        in_specs=[pl.BlockSpec(memory_space=pltpu.SMEM)] + [vmem] * 19,
        out_specs=[vmem, vmem, pl.BlockSpec(memory_space=pl.ANY)],
        scratch_shapes=[
            pltpu.VMEM((tokens, cols), f32),
            pltpu.VMEM((tokens, cols), f32),
            pltpu.VMEM((tokens, states), f32),
            pltpu.VMEM((tokens, states), f32),
            pltpu.VMEM((tokens, weights[3].shape[0]), f32),
            pltpu.VMEM((tokens, cols), bf16),
            pltpu.VMEM((tokens, cols), f32),
            pltpu.VMEM((ranks, coefs * BLOCK, cols), f32),
            pltpu.SemaphoreType.DMA((ranks,)),
        ],
        compiler_params=pltpu.CompilerParams(vmem_limit_bytes=8 * 1024 * 1024),
        name="core",
    )(rank, rows, kept(base, pltpu.VMEM), kept(half, pltpu.VMEM), *parts, *[kept(w, pltpu.VMEM) for w in weights], bias, decay_log, skip, ci, cw, cr, gain)


def tail_kernel(
    n, channels, part, sq, mixed, sqs, out, turned, pbuf, rbuf, lbuf, rout, lout, ps, pr, rs, rr, ls, lr, ss, sr
):
    f32 = jnp.float32
    k = lax.axis_index("kv")
    t = lax.axis_index("tp")
    rank = k * 2 + t
    ranks = n * 2
    right = {"kv": lax.rem(k + 1, n)}
    left = {"kv": lax.rem(k + n - 1, n)}
    partner = {"tp": 1 - t}
    span = part.shape[3] // CHUNKS
    barrier = pltpu.get_barrier_semaphore()

    def peer(o):
        p = lax.rem(rank + o, ranks)
        return {"kv": p // 2, "tp": lax.rem(p, 2)}

    for o in range(1, ranks):
        pl.semaphore_signal(barrier, inc=1, device_id=peer(o), device_id_type=MESH)
    pl.semaphore_wait(barrier, ranks - 1)

    def cut(c):
        return pl.ds(c * span, span)

    def across(j, c):
        return remote(
            part.at[j, 1 - t, :, cut(c)], pbuf.at[j, :, cut(c)], ps.at[j, c], pr.at[j, c], partner
        )

    def to_right(d, c):
        return remote(
            rout.at[d, :, cut(c)], rbuf.at[d, :, cut(c)], rs.at[d, c], rr.at[d, c], right
        )

    def to_left(d, c):
        return remote(lout.at[d, :, cut(c)], lbuf.at[d, :, cut(c)], ls.at[d, c], lr.at[d, c], left)

    def square(o):
        p = lax.rem(rank + o, ranks)
        return remote(sq.at[p], sqs.at[rank], ss.at[o], sr.at[o], peer(o))

    low = k < n // 2
    for i in range(n):
        j = jnp.where(low, n - 1 - i, i)
        for c in range(CHUNKS):
            across(j, c).start()
    for o in range(1, ranks):
        square(o).start()
    sqs[rank] = sq[rank]

    def pair(j, c):
        across(j, c).wait_recv()
        return part[j, t, :, cut(c)].astype(f32) + pbuf[j, :, cut(c)].astype(f32)

    def rightward():
        for d in range(n - 1, 0, -1):
            for c in range(CHUNKS):
                @pl.when((k < d) & (k == 0))
                def _():
                    rout[d, :, cut(c)] = pair(d, c).astype(rout.dtype)
                    to_right(d, c).start()

                @pl.when((k < d) & (k > 0))
                def _():
                    value = pair(d, c)
                    to_right(d, c).wait_recv()
                    rout[d, :, cut(c)] = (value + rbuf[d, :, cut(c)].astype(f32)).astype(rout.dtype)
                    to_right(d, c).start()

    def leftward():
        for d in range(n - 1):
            for c in range(CHUNKS):
                @pl.when((k > d) & (k == n - 1))
                def _():
                    lout[d, :, cut(c)] = pair(d, c).astype(lout.dtype)
                    to_left(d, c).start()

                @pl.when((k > d) & (k < n - 1))
                def _():
                    value = pair(d, c)
                    to_left(d, c).wait_recv()
                    lout[d, :, cut(c)] = (value + lbuf[d, :, cut(c)].astype(f32)).astype(lout.dtype)
                    to_left(d, c).start()

    @pl.when(k < n // 2)
    def _():
        rightward()
        leftward()

    @pl.when(k >= n // 2)
    def _():
        leftward()
        rightward()

    for c in range(CHUNKS):
        out[:, cut(c)] = pair(k, c)

        @pl.when(k > 0)
        def _():
            to_right(k, c).wait_recv()
            out[:, cut(c)] += rbuf[k, :, cut(c)].astype(f32)

        @pl.when(k < n - 1)
        def _():
            to_left(k, c).wait_recv()
            out[:, cut(c)] += lbuf[k, :, cut(c)].astype(f32)

    for o in range(1, ranks):
        square(o).wait_send()
        source = lax.rem(rank + ranks - o, ranks)
        remote(sq.at[rank], sqs.at[source], ss.at[o], sr.at[o], peer(o)).wait_recv()
    scale = lax.rsqrt(jnp.sum(sqs[...], axis=0) / channels + EPSILON)
    props = out.shape[0] // BLOCK
    for i in range(props):
        rows = out[i * BLOCK : (i + 1) * BLOCK, :] * scale[:, i : i + 1]
        turned[i * BLOCK : (i + 1) * BLOCK, :] = rows
    mixed[...] = jnp.dot(
        turn_rows(out.shape[0], props, True),
        turned[...].astype(mixed.dtype),
        preferred_element_type=f32,
    ).astype(mixed.dtype)
    for j in range(n):
        for c in range(CHUNKS):
            across(j, c).wait_send()

            @pl.when(k < j)
            def _():
                to_right(j, c).wait_send()

            @pl.when(k > j)
            def _():
                to_left(j, c).wait_send()


def finish(partial_value, squares, channels):
    n = lax.axis_size("kv")
    ranks = n * 2
    rows = partial_value.shape[0] // ranks
    cols = partial_value.shape[1]
    dma = pltpu.SemaphoreType.DMA
    vmem = pl.BlockSpec(memory_space=pltpu.VMEM)
    kind = partial_value.dtype
    f32 = jnp.float32
    return pl.pallas_call(
        functools.partial(tail_kernel, n, channels),
        out_shape=jax.ShapeDtypeStruct((rows, cols), kind),
        in_specs=[vmem, vmem],
        out_specs=vmem,
        scratch_shapes=[
            pltpu.VMEM(squares.shape, f32),
            pltpu.VMEM((rows, cols), f32),
            pltpu.VMEM((rows, cols), f32),
        ]
        + [pltpu.VMEM((n, rows, cols), kind)] * 5
        + [dma((n, CHUNKS))] * 6
        + [dma((ranks,))] * 2,
        compiler_params=pltpu.CompilerParams(
            collective_id=3, has_side_effects=True, vmem_limit_bytes=32 * 1024 * 1024
        ),
        name="tail",
    )(partial_value.reshape(n, 2, rows, cols), squares)


def whole_groups(tokens, saved_state, last_steps):
    span = lax.axis_size("kv") * lax.axis_size("tp")
    return span == GROUPS and tokens.shape[0] == BLOCK * last_steps.shape[1]


def quick(
    tokens,
    norm_gain,
    gate_proj,
    inner_proj,
    write_proj,
    read_proj,
    step_proj,
    step_bias,
    decay_log,
    skip_gain,
    conv_inner,
    conv_write,
    conv_read,
    out_gain,
    out_proj,
    saved_state,
    inner_history,
    write_history,
    read_history,
    last_steps,
    accepted,
):
    device_rank = lax.axis_index(("kv", "tp"))
    seqs, heads, head_dim, states = saved_state.shape
    slab = lambda x: x.transpose(1, 0, 2)
    row = lambda x: x.reshape(1, -1)
    weights = (inner_proj, write_proj, read_proj, step_proj.T, gate_proj, out_proj)
    got = lead(
        tokens,
        row(norm_gain),
        row(accepted),
        last_steps.transpose(1, 2, 0),
        row(decay_log),
        slab(inner_history),
        slab(write_history),
        slab(read_history),
        conv_inner,
        conv_write,
        conv_read,
        saved_state.reshape(seqs, heads * head_dim, states),
        weights,
    )
    rows, base, half = got[:3]
    partial_value, squares, base_state = core(
        device_rank.reshape(1).astype(jnp.int32),
        heads,
        rows.reshape(-1, rows.shape[-1]),
        base,
        half,
        got[3:6],
        got[6:],
        row(step_bias),
        row(decay_log),
        row(skip_gain),
        conv_inner,
        conv_write,
        conv_read,
        row(out_gain),
    )
    mixed = finish(partial_value, squares, out_gain.shape[0])
    return (mixed, base_state.reshape(saved_state.shape))


def body(
    tokens,
    norm_gain,
    gate_proj,
    inner_proj,
    write_proj,
    read_proj,
    step_proj,
    step_bias,
    decay_log,
    skip_gain,
    conv_inner,
    conv_write,
    conv_read,
    out_gain,
    out_proj,
    saved_state,
    inner_history,
    write_history,
    read_history,
    last_steps,
    accepted,
):
    if whole_groups(tokens, saved_state, last_steps):
        return quick(
            tokens,
            norm_gain,
            gate_proj,
            inner_proj,
            write_proj,
            read_proj,
            step_proj,
            step_bias,
            decay_log,
            skip_gain,
            conv_inner,
            conv_write,
            conv_read,
            out_gain,
            out_proj,
            saved_state,
            inner_history,
            write_history,
            read_history,
            last_steps,
            accepted,
        )
    device_rank = lax.axis_index(("kv", "tp"))
    seq_count = saved_state.shape[0]
    local_heads = saved_state.shape[1]
    head_dim = saved_state.shape[2]
    proposals = last_steps.shape[1]
    inner_cols = inner_proj.shape[1]
    state_cols = write_proj.shape[1]
    token_count = tokens.shape[0]
    own_rows = tokens.astype(jnp.float32)
    normed_own = (
        own_rows
        * lax.rsqrt(jnp.mean(own_rows * own_rows, axis=-1, keepdims=True) + EPSILON)
        * norm_gain
    ).astype(jnp.bfloat16)
    normed = gathered(normed_own)
    normed = normed.reshape(seq_count, proposals, -1).transpose(1, 0, 2)
    normed = normed.reshape(proposals * seq_count, -1)

    def project(weight):
        out = jnp.dot(normed, weight, preferred_element_type=jnp.float32)
        return out.reshape(proposals, seq_count, -1)

    gate_rows = project(gate_proj).astype(jnp.bfloat16)
    inner_rows = project(inner_proj).astype(jnp.bfloat16)
    first_head = device_rank * local_heads
    state_cols = write_proj.shape[1]
    states = saved_state.shape[3]
    step_local = lax.dynamic_slice_in_dim(step_proj, first_head, local_heads, 1)
    step_local = jnp.pad(step_local, ((0, 0), (0, states - local_heads)))
    small = project(jnp.concatenate([write_proj, read_proj, step_local], axis=1))
    par = lax.dynamic_slice_in_dim(
        jnp.stack([step_bias, decay_log, skip_gain]), first_head, local_heads, 1
    )
    slab = lambda x: x.transpose(1, 0, 2)
    hist_inner, hist_write, hist_read = slab(inner_history), slab(write_history), slab(read_history)
    group_span = lax.axis_size("kv") * lax.axis_size("tp") // GROUPS
    if group_span >= 2:
        write_rows = small[:, :, :state_cols].astype(jnp.bfloat16)
        read_rows = small[:, :, state_cols : 2 * state_cols].astype(jnp.bfloat16)
        pieces = (write_rows, read_rows, hist_write, hist_read)
        pieces = tuple(lax.all_gather(x, "tp", axis=2, tiled=True) for x in pieces)
        kv_rank = lax.axis_index("kv")
        bit_count = (group_span // lax.axis_size("tp")).bit_length() - 1
        for bit in range(bit_count):
            partner = swapped(pieces, "kv", bit)
            lower = jnp.bitwise_and(jnp.right_shift(kv_rank, bit), 1) == 0
            pieces = tuple(
                jnp.where(
                    lower,
                    jnp.concatenate([mine, theirs], axis=2),
                    jnp.concatenate([theirs, mine], axis=2),
                )
                for mine, theirs in zip(pieces, partner)
            )
        write_rows, read_rows, hist_write, hist_read = pieces
        small = jnp.concatenate(
            [
                write_rows.astype(jnp.float32),
                read_rows.astype(jnp.float32),
                small[:, :, 2 * state_cols :],
            ],
            axis=2,
        )
    unscaled, squares, base_state = mix(
        device_rank,
        device_rank // group_span,
        accepted[:, None],
        slab(last_steps),
        par,
        gate_rows,
        inner_rows,
        small,
        hist_inner,
        hist_write,
        hist_read,
        conv_inner,
        conv_write,
        conv_read,
        out_gain[None, :],
        saved_state.reshape(seq_count, local_heads * head_dim, -1),
    )
    base_state = base_state.reshape(saved_state.shape)
    unscaled = unscaled.transpose(1, 0, 2).reshape(seq_count * proposals, inner_cols)
    partial_value = jnp.dot(unscaled, out_proj, preferred_element_type=jnp.float32)
    squares = squares[:, :, 0].T.reshape(-1)
    summed, square_own = scattered(partial_value.astype(jnp.bfloat16), squares)
    mixed = (summed * lax.rsqrt(square_own / out_gain.shape[0] + EPSILON)[:, None]).astype(jnp.bfloat16)
    return (mixed, base_state)


def solution(mesh):
    placed = (
        P(("dp", "kv", "tp"), None),
        P(),
        P(None, ("kv", "tp")),
        P(None, ("kv", "tp")),
        P(None, ("kv", "tp")),
        P(None, ("kv", "tp")),
        P(),
        P(),
        P(),
        P(),
        P(),
        P(),
        P(),
        P(),
        P(("kv", "tp"), None),
        P("dp", ("kv", "tp"), None, None),
        P("dp", None, ("kv", "tp")),
        P("dp", None, ("kv", "tp")),
        P("dp", None, ("kv", "tp")),
        P("dp", None, ("kv", "tp")),
        P("dp"),
    )
    return jax.shard_map(
        body,
        mesh=mesh,
        in_specs=placed,
        out_specs=(P(("dp", "kv", "tp"), None), P("dp", ("kv", "tp"), None, None)),
        check_vma=False,
    )
```

```python
import functools

import jax
import jax.numpy as jnp
from jax import lax
from jax.experimental import pallas as pl
from jax.experimental.pallas import tpu as pltpu
from jax.sharding import PartitionSpec as P

GROUPS = 8
EPSILON = 0.1
BLOCK = 8
highest = lax.Precision.HIGHEST


def swapped(value, axis, stride):
    mask = 2**stride
    pairs = [(source, source ^ mask) for source in range(lax.axis_size(axis))]
    return lax.ppermute(value, axis, pairs)


def mix_kernel(
    rank_ref,
    acc_ref,
    steps_ref,
    last_ref,
    par_ref,
    gate_ref,
    inner_ref,
    write_ref,
    read_ref,
    hist_inner_ref,
    hist_write_ref,
    hist_read_ref,
    taps_inner_ref,
    taps_write_ref,
    taps_read_ref,
    gain_ref,
    expand_ref,
    state_ref,
    un_ref,
    sq_ref,
    base_ref,
):
    f32 = jnp.float32
    props = steps_ref.shape[0]
    heads = last_ref.shape[2]
    cols = inner_ref.shape[2]
    states = write_ref.shape[2]
    head_dim = cols // heads
    hist = hist_inner_ref.shape[0]
    width = taps_inner_ref.shape[0]
    acc = acc_ref[...]

    def silu(x):
        return x / (1.0 + jnp.exp(-x))

    def slabs(ref):
        return [ref[k].astype(f32) for k in range(ref.shape[0])]

    round_bf = lambda x: x.astype(jnp.bfloat16).astype(f32)

    def conv(rows, taps_ref):
        taps = taps_ref[...].astype(f32)
        res = []
        for r in range(len(rows) - width + 1):
            v = taps[0:1] * rows[r]
            for k in range(1, width):
                v = v + taps[k : k + 1] * rows[r + k]
            res.append(silu(v))
        return res

    def current(h, new_ref):
        where_at = jnp.broadcast_to(acc, h[0].shape)
        rows = []
        for k in range(width - 1):
            r = h[k]
            for v in range(1, hist - width + 2):
                r = jnp.where(where_at == v, h[k + v], r)
            rows.append(r)
        return rows + [round_bf(x) for x in slabs(new_ref)]

    h_inner = slabs(hist_inner_ref)
    inner_old = conv(h_inner, taps_inner_ref)
    inner_new = conv(current(h_inner, inner_ref), taps_inner_ref)
    h_write = slabs(hist_write_ref)
    write_old = [round_bf(x) for x in conv(h_write, taps_write_ref)]
    write_new = [round_bf(x) for x in conv(current(h_write, write_ref), taps_write_ref)]
    read_new = [round_bf(x) for x in conv(current(slabs(hist_read_ref), read_ref), taps_read_ref)]

    bias = par_ref[0:1]
    rate = -jnp.exp(par_ref[1:2])
    skip = par_ref[2:3]
    acc_h = jnp.broadcast_to(acc, (BLOCK, heads))
    masks = [jnp.where(acc_h > t, 1.0, 0.0) for t in range(props)]
    logs = [rate * last_ref[t] * masks[t] for t in range(props)]
    coefs = [None] * props
    tail = jnp.zeros((BLOCK, heads), f32)
    for t in reversed(range(props)):
        coefs[t] = masks[t] * jnp.exp(tail) * last_ref[t]
        tail = tail + logs[t]
    decay = jnp.exp(tail)
    step = []
    for t in range(props):
        x = steps_ref[t][:, :heads] + bias
        step.append(jnp.maximum(x, 0.0) + jnp.log1p(jnp.exp(-jnp.abs(x))))
    cums = []
    for t in range(props):
        cums.append(rate * step[t] + (cums[-1] if cums else 0.0))
    where_of = {}
    for i in range(props):
        for j in range(i + 1):
            score = jnp.sum(read_new[i] * write_new[j], axis=-1, keepdims=True)
            c = jnp.exp(cums[i] - cums[j]) * step[j] * score
            if i == j:
                c = c + skip
            where_of[(i, j)] = len(coefs)
            coefs.append(c)
    first_cum = len(coefs)
    for i in range(props):
        coefs.append(jnp.exp(cums[i]))
    wide = jnp.dot(
        jnp.concatenate(coefs, axis=0),
        expand_ref[...],
        precision=highest,
        preferred_element_type=f32,
    )

    def at(k):
        return wide[k * BLOCK : (k + 1) * BLOCK]

    left = jnp.concatenate([at(t) * inner_old[t] for t in range(props)], axis=0)
    high = round_bf(left)
    both = jnp.concatenate([high, left - high], axis=0)
    turned = jnp.transpose(both).astype(jnp.bfloat16)
    write_all = jnp.concatenate(write_old + write_old, axis=0)
    read_all = jnp.concatenate(read_new, axis=0)
    seq_w = lax.broadcasted_iota(jnp.int32, write_all.shape, 0) % BLOCK
    seq_r = lax.broadcasted_iota(jnp.int32, read_all.shape, 0) % BLOCK
    carried = jnp.zeros((props * BLOCK, cols), f32)
    for s in range(BLOCK):
        right = jnp.where(seq_w == s, write_all, 0.0).astype(jnp.bfloat16)
        update = jnp.dot(turned, right, preferred_element_type=f32)
        parts = []
        for h in range(heads):
            lo, hi = h * head_dim, (h + 1) * head_dim
            d = jnp.broadcast_to(decay[s : s + 1, h : h + 1], (head_dim, states))
            new = d * state_ref[s, lo:hi, :] + update[lo:hi]
            base_ref[s, lo:hi, :] = new
            parts.append(new.astype(jnp.bfloat16))
        asked = jnp.where(seq_r == s, read_all, 0.0).astype(jnp.bfloat16)
        carried = carried + lax.dot_general(
            asked,
            jnp.concatenate(parts, axis=0),
            (((1,), (1,)), ((), ())),
            preferred_element_type=f32,
        )
    for i in range(props):
        y = at(first_cum + i) * carried[i * BLOCK : (i + 1) * BLOCK]
        for j in range(i + 1):
            y = y + at(where_of[(i, j)]) * inner_new[j]
        g = y * silu(gate_ref[i].astype(f32))
        sq_ref[i] = jnp.broadcast_to(jnp.sum(g * g, axis=-1, keepdims=True), sq_ref.shape[1:])
        un_ref[i] = (g * gain_ref[...]).astype(un_ref.dtype)


def mix(rank, group, acc, last, par, gate, inner, small, hi, hw, hr, ci, cw, cr, gain, state):
    props, seqs, heads = last.shape
    cols, states = state.shape[1], state.shape[2]
    expand = (jnp.arange(cols)[None, :] // (cols // heads) == jnp.arange(heads)[:, None]).astype(
        jnp.float32
    )
    hist = hi.shape[0]
    width = ci.shape[0]

    def slab(lead, last_dim):
        return pl.BlockSpec((lead, BLOCK, last_dim), lambda g, r: (0, g, 0))

    def piece(which):
        return pl.BlockSpec((props, BLOCK, states), lambda g, r: (0, g, which))

    def own(rows, last_dim, which):
        return pl.BlockSpec((rows, last_dim), lambda g, r: (0, r[which]))

    state_spec = pl.BlockSpec((BLOCK, cols, states), lambda g, r: (g, 0, 0))
    return pl.pallas_call(
        mix_kernel,
        grid_spec=pltpu.PrefetchScalarGridSpec(
            num_scalar_prefetch=1,
            grid=(seqs // BLOCK,),
            in_specs=[
                pl.BlockSpec((BLOCK, 1), lambda g, r: (g, 0)),
                piece(2),
                slab(props, heads),
                pl.BlockSpec(par.shape, lambda g, r: (0, 0)),
                slab(props, cols),
                slab(props, cols),
                piece(0),
                piece(1),
                slab(hist, cols),
                slab(hist, states),
                slab(hist, states),
                own(width, cols, 0),
                own(width, states, 1),
                own(width, states, 1),
                own(1, cols, 0),
                pl.BlockSpec(expand.shape, lambda g, r: (0, 0)),
                state_spec,
            ],
            out_specs=[slab(props, cols), slab(props, 128), state_spec],
        ),
        out_shape=[
            jax.ShapeDtypeStruct((props, seqs, cols), jnp.bfloat16),
            jax.ShapeDtypeStruct((props, seqs, 128), jnp.float32),
            jax.ShapeDtypeStruct(state.shape, jnp.float32),
        ],
        compiler_params=pltpu.CompilerParams(
            dimension_semantics=("arbitrary",), vmem_limit_bytes=48 * 1024 * 1024
        ),
        name="mix",
    )(
        jnp.stack([rank, group]).astype(jnp.int32),
        acc, small, last, par, gate, inner, small, small, hi, hw, hr, ci, cw, cr, gain, expand, state,
    )


MESH = pl.DeviceIdType.MESH
CHUNKS = 2


def remote(src, dst, send, recv, where):
    return pltpu.make_async_remote_copy(
        src_ref=src, dst_ref=dst, send_sem=send, recv_sem=recv, device_id=where, device_id_type=MESH
    )


def gather_kernel(n, own_ref, out_ref, rs, rr, ls, lr, fs, fr, local_sem):
    k = lax.axis_index("kv")
    t = lax.axis_index("tp")
    right = {"kv": lax.rem(k + 1, n)}
    left = {"kv": lax.rem(k + n - 1, n)}
    partner = {"tp": 1 - t}
    span = own_ref.shape[1] // CHUNKS
    barrier = pltpu.get_barrier_semaphore()
    pl.semaphore_signal(barrier, inc=1, device_id=partner, device_id_type=MESH)

    @pl.when(k < n - 1)
    def _():
        pl.semaphore_signal(barrier, inc=1, device_id=right, device_id_type=MESH)

    @pl.when(k > 0)
    def _():
        pl.semaphore_signal(barrier, inc=1, device_id=left, device_id_type=MESH)

    inner = (k > 0) & (k < n - 1)

    @pl.when(inner)
    def _():
        pl.semaphore_wait(barrier, 3)

    @pl.when(jnp.logical_not(inner))
    def _():
        pl.semaphore_wait(barrier, 2)

    def view(j, c):
        return out_ref.at[j, t, :, pl.ds(c * span, span)]

    def own(c):
        return own_ref.at[:, pl.ds(c * span, span)]

    def to_right(s, c):
        j = jnp.maximum(k - s, 0)
        return remote(own(c) if s == 0 else view(j, c), view(j, c), rs.at[s, c], rr.at[s, c], right)

    def to_left(s, c):
        j = jnp.minimum(k + s, n - 1)
        return remote(own(c) if s == 0 else view(j, c), view(j, c), ls.at[s, c], lr.at[s, c], left)

    def across(j, c, mine=False):
        return remote(own(c) if mine else view(j, c), view(j, c), fs.at[j, c], fr.at[j, c], partner)

    for s in range(n - 1):
        for c in range(CHUNKS):
            if s > 0:
                @pl.when(k - s >= 0)
                def _():
                    to_right(s - 1, c).wait_recv()

                @pl.when(k + s < n)
                def _():
                    to_left(s - 1, c).wait_recv()

            @pl.when((k - s >= 0) & (k < n - 1))
            def _():
                to_right(s, c).start()

            @pl.when((k + s < n) & (k > 0))
            def _():
                to_left(s, c).start()

            if s == 0:
                across(k, c, True).start()
            else:
                @pl.when(k - s >= 0)
                def _():
                    across(k - s, c).start()

                @pl.when(k + s < n)
                def _():
                    across(k + s, c).start()
        if s == 0:
            local = pltpu.make_async_copy(own_ref, out_ref.at[k, t], local_sem)
            local.start()
            local.wait()
    s = n - 1
    for c in range(CHUNKS):
        @pl.when(k - s >= 0)
        def _():
            to_right(s - 1, c).wait_recv()
            across(k - s, c).start()

        @pl.when(k + s < n)
        def _():
            to_left(s - 1, c).wait_recv()
            across(k + s, c).start()
    for s in range(n - 1):
        for c in range(CHUNKS):
            @pl.when((k - s >= 0) & (k < n - 1))
            def _():
                to_right(s, c).wait_send()

            @pl.when((k + s < n) & (k > 0))
            def _():
                to_left(s, c).wait_send()
    for j in range(n):
        for c in range(CHUNKS):
            across(j, c).wait_send()
            remote(
                out_ref.at[j, 1 - t, :, pl.ds(c * span, span)],
                out_ref.at[j, 1 - t, :, pl.ds(c * span, span)],
                fs.at[j, c],
                fr.at[j, c],
                partner,
            ).wait_recv()


def gathered(own):
    n = lax.axis_size("kv")
    rows, cols = own.shape
    dma = pltpu.SemaphoreType.DMA
    out = pl.pallas_call(
        functools.partial(gather_kernel, n),
        out_shape=jax.ShapeDtypeStruct((n, 2, rows, cols), own.dtype),
        in_specs=[pl.BlockSpec(memory_space=pltpu.VMEM)],
        out_specs=pl.BlockSpec(memory_space=pltpu.VMEM),
        scratch_shapes=[dma((n - 1, CHUNKS))] * 4 + [dma((n, CHUNKS))] * 2 + [dma],
        compiler_params=pltpu.CompilerParams(
            collective_id=0, has_side_effects=True, vmem_limit_bytes=32 * 1024 * 1024
        ),
        name="gather",
    )(own)
    return out.reshape(n * 2 * rows, cols)


def scatter_kernel(
    n, part, sq, out, sqs, pbuf, rbuf, lbuf, rout, lout, ps, pr, rs, rr, ls, lr, ss, sr
):
    f32 = jnp.float32
    k = lax.axis_index("kv")
    t = lax.axis_index("tp")
    rank = k * 2 + t
    ranks = n * 2
    right = {"kv": lax.rem(k + 1, n)}
    left = {"kv": lax.rem(k + n - 1, n)}
    partner = {"tp": 1 - t}
    span = part.shape[3] // CHUNKS
    barrier = pltpu.get_barrier_semaphore()

    def peer(o):
        p = lax.rem(rank + o, ranks)
        return {"kv": p // 2, "tp": lax.rem(p, 2)}

    for o in range(1, ranks):
        pl.semaphore_signal(barrier, inc=1, device_id=peer(o), device_id_type=MESH)
    pl.semaphore_wait(barrier, ranks - 1)

    def cut(c):
        return pl.ds(c * span, span)

    def across(j, c):
        return remote(
            part.at[j, 1 - t, :, cut(c)], pbuf.at[j, :, cut(c)], ps.at[j, c], pr.at[j, c], partner
        )

    def to_right(d, c):
        return remote(
            rout.at[d, :, cut(c)], rbuf.at[d, :, cut(c)], rs.at[d, c], rr.at[d, c], right
        )

    def to_left(d, c):
        return remote(lout.at[d, :, cut(c)], lbuf.at[d, :, cut(c)], ls.at[d, c], lr.at[d, c], left)

    def square(o):
        p = lax.rem(rank + o, ranks)
        return remote(sq.at[p], sqs.at[rank], ss.at[o], sr.at[o], peer(o))

    low = k < n // 2
    for i in range(n):
        j = jnp.where(low, n - 1 - i, i)
        for c in range(CHUNKS):
            across(j, c).start()
    for o in range(1, ranks):
        square(o).start()
    sqs[rank] = sq[rank]

    def pair(j, c):
        across(j, c).wait_recv()
        return part[j, t, :, cut(c)].astype(f32) + pbuf[j, :, cut(c)].astype(f32)

    def rightward():
        for d in range(n - 1, 0, -1):
            for c in range(CHUNKS):
                @pl.when((k < d) & (k == 0))
                def _():
                    rout[d, :, cut(c)] = pair(d, c).astype(rout.dtype)
                    to_right(d, c).start()

                @pl.when((k < d) & (k > 0))
                def _():
                    value = pair(d, c)
                    to_right(d, c).wait_recv()
                    rout[d, :, cut(c)] = (value + rbuf[d, :, cut(c)].astype(f32)).astype(rout.dtype)
                    to_right(d, c).start()

    def leftward():
        for d in range(n - 1):
            for c in range(CHUNKS):
                @pl.when((k > d) & (k == n - 1))
                def _():
                    lout[d, :, cut(c)] = pair(d, c).astype(lout.dtype)
                    to_left(d, c).start()

                @pl.when((k > d) & (k < n - 1))
                def _():
                    value = pair(d, c)
                    to_left(d, c).wait_recv()
                    lout[d, :, cut(c)] = (value + lbuf[d, :, cut(c)].astype(f32)).astype(lout.dtype)
                    to_left(d, c).start()

    @pl.when(k < n // 2)
    def _():
        rightward()
        leftward()

    @pl.when(k >= n // 2)
    def _():
        leftward()
        rightward()

    for c in range(CHUNKS):
        out[:, cut(c)] = pair(k, c)

        @pl.when(k > 0)
        def _():
            to_right(k, c).wait_recv()
            out[:, cut(c)] += rbuf[k, :, cut(c)].astype(f32)

        @pl.when(k < n - 1)
        def _():
            to_left(k, c).wait_recv()
            out[:, cut(c)] += lbuf[k, :, cut(c)].astype(f32)

    for j in range(n):
        for c in range(CHUNKS):
            across(j, c).wait_send()

            @pl.when(k < j)
            def _():
                to_right(j, c).wait_send()

            @pl.when(k > j)
            def _():
                to_left(j, c).wait_send()
    for o in range(1, ranks):
        square(o).wait_send()
        source = lax.rem(rank + ranks - o, ranks)
        remote(sq.at[rank], sqs.at[source], ss.at[o], sr.at[o], peer(o)).wait_recv()


def scattered(partial_value, squares):
    n = lax.axis_size("kv")
    ranks = n * 2
    rows = partial_value.shape[0] // ranks
    cols = partial_value.shape[1]
    squares = jnp.pad(squares.reshape(ranks, 1, rows), ((0, 0), (0, 7), (0, 128 - rows)))
    dma = pltpu.SemaphoreType.DMA
    vmem = pl.BlockSpec(memory_space=pltpu.VMEM)
    kind = partial_value.dtype
    summed, sqs = pl.pallas_call(
        functools.partial(scatter_kernel, n),
        out_shape=[
            jax.ShapeDtypeStruct((rows, cols), jnp.float32),
            jax.ShapeDtypeStruct(squares.shape, jnp.float32),
        ],
        in_specs=[vmem, vmem],
        out_specs=[vmem, vmem],
        scratch_shapes=[pltpu.VMEM((n, rows, cols), kind)] * 5
        + [dma((n, CHUNKS))] * 6
        + [dma((ranks,))] * 2,
        compiler_params=pltpu.CompilerParams(
            collective_id=1, has_side_effects=True, vmem_limit_bytes=32 * 1024 * 1024
        ),
        name="scatter",
    )(partial_value.reshape(n, 2, rows, cols), squares)
    return summed, jnp.sum(sqs[:, 0, :rows], axis=0)


AHEAD = 3
CARRY = 4
HOPS_AT = (0, 1, 1, 2, 3, 4, 5, 6)


def pick(x, rows, first):
    wide = jnp.broadcast_to(x, (rows, x.shape[1]))
    lane = lax.broadcasted_iota(jnp.int32, wide.shape, 1)
    row = lax.broadcasted_iota(jnp.int32, wide.shape, 0)
    return jnp.sum(jnp.where(lane == row + first, wide, 0.0), axis=1, keepdims=True)


def turn_rows(rows, props, back=False):
    seqs = rows // props
    row = lax.broadcasted_iota(jnp.int32, (rows, rows), 0)
    col = lax.broadcasted_iota(jnp.int32, (rows, rows), 1)
    if back:
        row, col = col, row
    return jnp.where(col == row % seqs * props + row // seqs, 1.0, 0.0).astype(jnp.bfloat16)


def silu_of(x):
    return x / (1.0 + jnp.exp(-x))


def round_of(x):
    return x.astype(jnp.bfloat16).astype(jnp.float32)


def split_of(x):
    high = x.astype(jnp.bfloat16)
    return high, (x - high.astype(jnp.float32)).astype(jnp.bfloat16)


def own_slice(ref, first, count):
    return ref[:, pl.ds(pl.multiple_of(first, 128), count)].astype(jnp.float32)


def lead_kernel(
    n,
    tokens_hbm,
    norm_hbm,
    acc_hbm,
    last_hbm,
    decay_hbm,
    hist_inner_hbm,
    hist_write_hbm,
    hist_read_hbm,
    taps_inner_hbm,
    taps_write_hbm,
    taps_read_hbm,
    state_ref,
    inner_hbm,
    write_hbm,
    read_hbm,
    step_hbm,
    gate_hbm,
    outw_hbm,
    rows_ref,
    base_ref,
    half_ref,
    part_inner_ref,
    part_write_ref,
    part_read_ref,
    inner_ref,
    write_ref,
    read_ref,
    step_ref,
    gate_ref,
    outw_ref,
    own_ref,
    decay_buf,
    wide_buf,
    turned_buf,
    old_buf,
    rs,
    rr,
    ls,
    lr,
    fs,
    fr,
    local_sem,
    state_sems,
    small_sems,
    weight_sems,
    tokens_ref,
    norm_ref,
    acc_ref,
    last_ref,
    decay_ref,
    hist_inner_ref,
    hist_write_ref,
    hist_read_ref,
    taps_inner_ref,
    taps_write_ref,
    taps_read_ref,
):
    f32 = jnp.float32
    bf16 = jnp.bfloat16
    k = lax.axis_index("kv")
    t = lax.axis_index("tp")
    rank = k * 2 + t
    right = {"kv": lax.rem(k + 1, n)}
    left = {"kv": lax.rem(k + n - 1, n)}
    partner = {"tp": 1 - t}
    barrier = pltpu.get_barrier_semaphore()
    pl.semaphore_signal(barrier, inc=1, device_id=partner, device_id_type=MESH)

    @pl.when(k < n - 1)
    def _():
        pl.semaphore_signal(barrier, inc=1, device_id=right, device_id_type=MESH)

    @pl.when(k > 0)
    def _():
        pl.semaphore_signal(barrier, inc=1, device_id=left, device_id_type=MESH)

    props, heads, seqs = last_ref.shape
    cols = base_ref.shape[1]
    states = base_ref.shape[2]
    hist = hist_inner_ref.shape[0]
    width = taps_inner_ref.shape[0]
    blocks = seqs // BLOCK

    def fetch(b):
        span = pl.ds(b * BLOCK, BLOCK)
        return pltpu.make_async_copy(state_ref.at[span], base_ref.at[span], state_sems.at[b])

    small = [
        pltpu.make_async_copy(src, dst, small_sems.at[i])
        for i, (src, dst) in enumerate(
            [
                (tokens_hbm, tokens_ref),
                (norm_hbm, norm_ref),
                (acc_hbm, acc_ref),
                (last_hbm, last_ref),
                (decay_hbm, decay_ref),
                (hist_inner_hbm, hist_inner_ref),
                (hist_write_hbm, hist_write_ref),
                (hist_read_hbm, hist_read_ref),
                (taps_inner_hbm, taps_inner_ref),
                (taps_write_hbm, taps_write_ref),
                (taps_read_hbm, taps_read_ref),
            ]
        )
    ]
    for c in small:
        c.start()
    weights = [
        pltpu.make_async_copy(src, dst, weight_sems.at[i])
        for i, (src, dst) in enumerate(
            [
                (inner_hbm, inner_ref),
                (write_hbm, write_ref),
                (read_hbm, read_ref),
                (step_hbm, step_ref),
                (gate_hbm, gate_ref),
                (outw_hbm, outw_ref),
            ]
        )
    ]
    queue = [fetch(b) for b in range(blocks)] + weights
    for c in queue[:AHEAD]:
        c.start()
    for c in small[:2]:
        c.wait()
    own = tokens_ref[...].astype(f32)
    scale = lax.rsqrt(jnp.mean(own * own, axis=-1, keepdims=True) + EPSILON)
    normed = (own * scale * norm_ref[...]).astype(bf16)
    own_ref[...] = jnp.dot(
        turn_rows(own.shape[0], props), normed, preferred_element_type=f32
    ).astype(bf16)

    inside = (k > 0) & (k < n - 1)

    @pl.when(inside)
    def _():
        pl.semaphore_wait(barrier, 3)

    @pl.when(jnp.logical_not(inside))
    def _():
        pl.semaphore_wait(barrier, 2)

    span = own_ref.shape[1] // CHUNKS

    def view(j, c):
        return rows_ref.at[j, t, :, pl.ds(c * span, span)]

    def mine(c):
        return own_ref.at[:, pl.ds(c * span, span)]

    def to_right(s, c):
        j = jnp.maximum(k - s, 0)
        return remote(mine(c) if s == 0 else view(j, c), view(j, c), rs.at[s, c], rr.at[s, c], right)

    def to_left(s, c):
        j = jnp.minimum(k + s, n - 1)
        return remote(mine(c) if s == 0 else view(j, c), view(j, c), ls.at[s, c], lr.at[s, c], left)

    def across(j, c, first=False):
        return remote(mine(c) if first else view(j, c), view(j, c), fs.at[j, c], fr.at[j, c], partner)

    def hop(s, c):
        if s > 0:
            @pl.when(k - s >= 0)
            def _():
                to_right(s - 1, c).wait_recv()

            @pl.when(k + s < n)
            def _():
                to_left(s - 1, c).wait_recv()

        if s < n - 1:
            @pl.when((k - s >= 0) & (k < n - 1))
            def _():
                to_right(s, c).start()

            @pl.when((k + s < n) & (k > 0))
            def _():
                to_left(s, c).start()

        if s == 0:
            across(k, c, True).start()
        else:
            @pl.when(k - s >= 0)
            def _():
                across(k - s, c).start()

            @pl.when(k + s < n)
            def _():
                across(k + s, c).start()

    for c in range(CHUNKS):
        hop(0, c)
    local = pltpu.make_async_copy(own_ref, rows_ref.at[k, t], local_sem)
    local.start()

    for c in small[2:]:
        c.wait()

    acc_row = acc_ref[...]
    rate = pick(-jnp.exp(decay_ref[...]), heads, rank * heads)
    old_weights = [None] * props
    tail = jnp.zeros((heads, seqs), f32)
    for p in reversed(range(props)):
        mask = jnp.where(acc_row > p, 1.0, 0.0)
        old_weights[p] = mask * jnp.exp(tail) * last_ref[p]
        tail = tail + rate * last_ref[p] * mask
    turned = jnp.transpose(jnp.concatenate(old_weights + [jnp.exp(tail)], axis=0))
    lane = lax.broadcasted_iota(jnp.int32, (heads, cols), 1)
    row = lax.broadcasted_iota(jnp.int32, (heads, cols), 0)
    expand = jnp.where(lane // (cols // heads) == row, 1.0, 0.0).astype(bf16)
    for p in range(props):
        w = turned[:, p * heads : (p + 1) * heads]
        high, low = split_of(w)
        wide_buf[p] = jnp.dot(high, expand, preferred_element_type=f32) + jnp.dot(
            low, expand, preferred_element_type=f32
        )
    for h in range(heads):
        at = props * heads + h
        decay_buf[h] = jnp.broadcast_to(turned[:, at : at + 1], (seqs, states))
    acc = jnp.sum(
        jnp.where(
            lax.broadcasted_iota(jnp.int32, (seqs, seqs), 0)
            == lax.broadcasted_iota(jnp.int32, (seqs, seqs), 1),
            jnp.broadcast_to(acc_row, (seqs, seqs)),
            0,
        ).astype(f32),
        axis=1,
        keepdims=True,
    )

    def conv_parts(hist_at, taps, part_ref, b):
        where_at = jnp.broadcast_to(acc[b : b + BLOCK], hist_at[0].shape)
        current = []
        for e in range(width - 1):
            r = hist_at[e]
            for v in range(1, hist - width + 2):
                r = jnp.where(where_at == v, hist_at[e + v], r)
            current.append(r)
        for i in range(width - 1):
            total = taps[0:1] * current[i]
            for e in range(i + 1, width - 1):
                total = total + taps[e - i : e - i + 1] * current[e]
            part_ref[i, b : b + BLOCK, :] = total

    def conv_old(hist_at, taps):
        res = []
        for r in range(hist - width + 1):
            total = taps[0:1] * hist_at[r]
            for e in range(1, width):
                total = total + taps[e : e + 1] * hist_at[r + e]
            res.append(silu_of(total))
        return res

    def slabs(ref, b):
        return [ref[e, b : b + BLOCK, :].astype(f32) for e in range(hist)]

    taps_inner = own_slice(taps_inner_ref, rank * cols, cols)
    taps_write = own_slice(taps_write_ref, rank * states, states)
    taps_read = own_slice(taps_read_ref, rank * states, states)
    per_half = blocks // 2

    def prepare(part):
        lefts, rights = [], []
        for g in range(per_half):
            b = (part * per_half + g) * BLOCK
            h_inner = slabs(hist_inner_ref, b)
            h_write = slabs(hist_write_ref, b)
            olds = conv_old(h_inner, taps_inner)
            lefts += [wide_buf[p, b : b + BLOCK, :] * olds[p] for p in range(props)]
            rights += conv_old(h_write, taps_write)
            conv_parts(h_inner, taps_inner, part_inner_ref, b)
            conv_parts(h_write, taps_write, part_write_ref, b)
            conv_parts(slabs(hist_read_ref, b), taps_read, part_read_ref, b)
        turned_buf[part] = jnp.transpose(jnp.concatenate(lefts, axis=0)).astype(bf16)
        old_buf[part] = jnp.concatenate(rights, axis=0).astype(bf16)

    half_rows = per_half * props * BLOCK
    row = lax.broadcasted_iota(jnp.int32, (half_rows, states), 0)
    seq_of = row // (props * BLOCK) * BLOCK + row % BLOCK

    def update(part, first, count):
        lhs = turned_buf[part]
        old = old_buf[part].astype(f32)
        head_dim = cols // heads

        adds = []
        for i in range(0, count, 2):
            rhs = jnp.concatenate(
                [jnp.where(seq_of == first + i + e, old, 0.0).astype(bf16) for e in range(2)],
                axis=1,
            )
            adds.append(jnp.dot(lhs, rhs, preferred_element_type=f32))
        for i in range(count):
            s = part * (seqs // 2) + first + i
            add = adds[i // 2]
            side = i % 2 * states
            for h in range(heads):
                lo, hi = h * head_dim, (h + 1) * head_dim
                new = decay_buf[h, s : s + 1, :] * base_ref[s, lo:hi, :]
                new = new + add[lo:hi, side : side + states]
                base_ref[s, lo:hi, :] = new
                half_ref[s, lo:hi, :] = new.astype(bf16)

    hops = [(s, c) for s in range(1, n) for c in range(CHUNKS)]
    done = 0
    for part in range(2):
        prepare(part)
        for g in range(per_half):
            b = part * per_half + g
            queue[b].wait()
            more = queue[b + AHEAD : b + AHEAD + 1] if b + 1 < blocks else queue[b + AHEAD :]
            for c in more:
                c.start()
            update(part, g * BLOCK, BLOCK)
            goal = len(hops) * HOPS_AT[b] // 6
            while done < goal:
                hop(*hops[done])
                done += 1
    for w in weights:
        w.wait()
    local.wait()
    for s in range(n - 1):
        for c in range(CHUNKS):
            @pl.when((k - s >= 0) & (k < n - 1))
            def _():
                to_right(s, c).wait_send()

            @pl.when((k + s < n) & (k > 0))
            def _():
                to_left(s, c).wait_send()
    for j in range(n):
        for c in range(CHUNKS):
            across(j, c).wait_send()
            there = rows_ref.at[j, 1 - t, :, pl.ds(c * span, span)]
            remote(there, there, fs.at[j, c], fr.at[j, c], partner).wait_recv()


kept = pltpu.with_memory_space_constraint


def lead(tokens, norm_gain, acc, last, decay_log, hi, hw, hr, ci, cw, cr, state, weights):
    n = lax.axis_size("kv")
    rows, width = tokens.shape
    props, heads, seqs = last.shape
    cols, states = state.shape[1:]
    taps = ci.shape[0]
    dma = pltpu.SemaphoreType.DMA
    vmem = pl.BlockSpec(memory_space=pltpu.VMEM)
    hbm = pl.BlockSpec(memory_space=pltpu.HBM)
    f32, bf16 = jnp.float32, jnp.bfloat16
    shape = jax.ShapeDtypeStruct
    blocks = seqs // BLOCK
    half_rows = seqs // 2 * props
    small = (tokens, norm_gain, acc, last, decay_log, hi, hw, hr, ci, cw, cr)
    return pl.pallas_call(
        functools.partial(lead_kernel, n),
        out_shape=[
            shape((n, 2, rows, width), bf16),
            pltpu.VMEM(state.shape, f32),
            pltpu.VMEM(state.shape, bf16),
            shape((taps - 1, seqs, cols), f32),
            shape((taps - 1, seqs, states), f32),
            shape((taps - 1, seqs, states), f32),
        ]
        + [pltpu.VMEM(w.shape, w.dtype) for w in weights],
        in_specs=[hbm] * (len(small) + 1 + len(weights)),
        out_specs=[vmem] * (6 + len(weights)),
        scratch_shapes=[
            pltpu.VMEM((rows, width), bf16),
            pltpu.VMEM((heads, seqs, states), f32),
            pltpu.VMEM((props, seqs, cols), f32),
            pltpu.VMEM((2, cols, half_rows), bf16),
            pltpu.VMEM((2, half_rows, states), bf16),
        ]
        + [dma((n - 1, CHUNKS))] * 4
        + [dma((n, CHUNKS))] * 2
        + [dma, dma((blocks,)), dma((len(small),)), dma((len(weights),))]
        + [pltpu.VMEM(x.shape, x.dtype) for x in small],
        compiler_params=pltpu.CompilerParams(
            collective_id=2, has_side_effects=True, vmem_limit_bytes=8 * 1024 * 1024
        ),
        name="lead",
    )(*[kept(x, pltpu.HBM) for x in small + (state,) + weights])


def carry_over(first, props, half_ref, read_ref, carried_ref):
    rows_of = props * BLOCK
    span = CARRY * rows_of
    asked = jnp.transpose(read_ref[pl.ds(pl.multiple_of(first * rows_of, span), span), :])
    col = lax.broadcasted_iota(jnp.int32, asked.shape, 1)
    seq_of = col // rows_of * BLOCK + col % BLOCK
    total = None
    for s in range(0, CARRY * BLOCK, 2):
        lhs = jnp.concatenate([half_ref[first * BLOCK + s + e] for e in range(2)], axis=1)
        rhs = jnp.concatenate(
            [jnp.where(seq_of == s + e, asked, 0.0).astype(jnp.bfloat16) for e in range(2)], axis=0
        )
        got = jnp.dot(lhs, rhs, preferred_element_type=jnp.float32)
        total = got if total is None else total + got
    carried_ref[...] = jnp.transpose(total)


def mix_rows(first, props, gain, wide_ref, inner_ref, gate_ref, carried_ref, un_ref, put_square):
    rows_of = props * BLOCK
    pairs_of = pairs_up_to(props)
    lane_of = lax.broadcasted_iota(jnp.int32, (BLOCK, 128), 1)

    def one(b):
        r = first + b
        near = pl.multiple_of(b * rows_of, rows_of)
        at_row = pl.multiple_of(r * rows_of, rows_of)

        def at(e):
            return wide_ref[r, e * BLOCK : (e + 1) * BLOCK, :]

        def part(ref, i):
            return ref[pl.ds(at_row + i * BLOCK, BLOCK), :]

        squares = jnp.zeros((BLOCK, 128), jnp.float32)
        outs = []
        for i in range(props):
            y = at(len(pairs_of) + i) * carried_ref[pl.ds(near + i * BLOCK, BLOCK), :]
            for j in range(i + 1):
                y = y + at(pairs_of[(i, j)]) * part(inner_ref, j)
            g = y * silu_of(part(gate_ref, i))
            squares = jnp.where(lane_of == i, jnp.sum(g * g, axis=-1, keepdims=True), squares)
            outs.append(g * gain)
        put_square(b, squares)
        un_ref[pl.ds(near, rows_of), :] = jnp.concatenate(outs, axis=0).astype(jnp.bfloat16)

    each(one, 0, CARRY, 2)


def each(fn, lo, hi, step):
    def run(i, carry):
        for u in range(step):
            fn(lo + i * step + u)
        return carry

    lax.fori_loop(0, (hi - lo) // step, run, 0)


def pairs_up_to(props):
    order = [(i, j) for i in range(props) for j in range(i + 1)]
    return {p: e for e, p in enumerate(order)}


def out_tiles(un_ref, outw_ref, put):
    un = un_ref[...]
    tile = 512
    for lo in range(0, outw_ref.shape[1], tile):
        got = jnp.dot(un, outw_ref[:, lo : lo + tile], preferred_element_type=jnp.float32)
        put(pl.ds(lo, tile), got.astype(jnp.bfloat16))


def core_kernel(
    heads,
    rank_ref,
    rows_ref,
    base_ref,
    half_ref,
    part_inner_ref,
    part_write_ref,
    part_read_ref,
    inner_ref,
    write_ref,
    read_ref,
    step_ref,
    gate_ref,
    outw_ref,
    bias_ref,
    decay_ref,
    skip_ref,
    taps_inner_ref,
    taps_write_ref,
    taps_read_ref,
    gain_ref,
    out_ref,
    sq_ref,
    state_out,
    gate_buf,
    inner_buf,
    read_buf,
    wide_buf,
    write_buf,
    step_buf,
    un_buf,
    carried_buf,
    sems,
):
    f32, bf16 = jnp.float32, jnp.bfloat16
    rank = rank_ref[0]
    seqs, cols, states = base_ref.shape
    blocks = seqs // BLOCK
    props = rows_ref.shape[0] // seqs
    width = taps_inner_ref.shape[0]
    head_count = step_ref.shape[0]

    def flush(b):
        span = pl.ds(b * BLOCK, BLOCK)
        return pltpu.make_async_copy(base_ref.at[span], state_out.at[span], sems.at[b])

    for b in range(blocks):
        flush(b).start()
    rows = rows_ref[...]
    tile = 256
    for w_ref, buf in ((inner_ref, inner_buf), (gate_ref, gate_buf)):
        for lo in range(0, cols, tile):
            buf[:, lo : lo + tile] = round_of(
                jnp.dot(rows, w_ref[:, lo : lo + tile], preferred_element_type=f32)
            )
    both = jnp.dot(
        rows, jnp.concatenate([write_ref[...], read_ref[...]], axis=1), preferred_element_type=f32
    )
    write_buf[...] = round_of(both[:, :states])
    read_buf[...] = round_of(both[:, states:])
    nt = (((1,), (1,)), ((), ()))
    step_buf[...] = lax.dot_general(rows, step_ref[...], nt, preferred_element_type=f32)
    taps_inner = own_slice(taps_inner_ref, rank * cols, cols)
    taps_write = own_slice(taps_write_ref, rank * states, states)
    taps_read = own_slice(taps_read_ref, rank * states, states)
    gain = own_slice(gain_ref, rank * cols, cols)
    bias = bias_ref[...]
    rate = -jnp.exp(decay_ref[...])
    skip = skip_ref[...]
    lane = lax.broadcasted_iota(jnp.int32, (2 * head_count, cols), 1)
    row = lax.broadcasted_iota(jnp.int32, (2 * head_count, cols), 0)
    expand = jnp.where(
        lane // (cols // heads) + rank * heads == row % head_count, 1.0, 0.0
    ).astype(bf16)

    rows_of = props * BLOCK
    pairs_of = pairs_up_to(props)

    def prepare(r):
        at_row = pl.multiple_of(r * rows_of, rows_of)
        at_seq = pl.multiple_of(r * BLOCK, BLOCK)

        def news(buf, part_ref, taps):
            fresh = [buf[pl.ds(at_row + i * BLOCK, BLOCK), :] for i in range(props)]
            res = []
            for i in range(props):
                total = taps[width - 1 : width] * fresh[i]
                for e in range(1, min(i, width - 1) + 1):
                    total = total + taps[width - 1 - e : width - e] * fresh[i - e]
                if i < width - 1:
                    total = total + part_ref[i, pl.ds(at_seq, BLOCK), :]
                res.append(silu_of(total))
            return res

        inner_new = news(inner_buf, part_inner_ref, taps_inner)
        for i in range(props):
            inner_buf[pl.ds(at_row + i * BLOCK, BLOCK), :] = inner_new[i]
        write_new = [round_of(x) for x in news(write_buf, part_write_ref, taps_write)]
        read_new = [round_of(x) for x in news(read_buf, part_read_ref, taps_read)]
        for i in range(props):
            read_buf[pl.ds(at_row + i * BLOCK, BLOCK), :] = read_new[i]
        steps = step_buf[pl.ds(at_row, rows_of), :] + bias
        steps = jnp.maximum(steps, 0.0) + jnp.log1p(jnp.exp(-jnp.abs(steps)))
        step = [steps[i * BLOCK : (i + 1) * BLOCK] for i in range(props)]
        cums = []
        for i in range(props):
            cums.append(rate * step[i] + (cums[-1] if cums else 0.0))
        coefs = []
        for i, j in pairs_of:
            score = jnp.sum(read_new[i] * write_new[j], axis=-1, keepdims=True)
            c = jnp.exp(cums[i] - cums[j]) * step[j] * score
            coefs.append(c + skip if i == j else c)
        coefs += [jnp.exp(c) for c in cums]
        high, low = split_of(jnp.concatenate(coefs, axis=0))
        wide_buf[r] = jnp.dot(
            jnp.concatenate([high, low], axis=1), expand, preferred_element_type=f32
        )

    each(prepare, 0, blocks, 2)
    first = jnp.where(rank < blocks // 2, CARRY, 0)

    def put_square(e, squares):
        sq_ref[e] = squares

    carry_over(first, props, half_ref, read_buf, carried_buf)
    mix_rows(
        first, props, gain, wide_buf, inner_buf, gate_buf, carried_buf, un_buf, put_square
    )

    def put(cut, got):
        out_ref[:, cut] = got

    out_tiles(un_buf, outw_ref, put)
    for b in range(blocks):
        flush(b).wait()


def core(rank, heads, rows, base, half, parts, weights, bias, decay_log, skip, ci, cw, cr, gain):
    seqs, cols, states = base.shape
    tokens = rows.shape[0]
    width = weights[-1].shape[1]
    ranks = seqs // BLOCK
    props = tokens // seqs
    coefs = props * (props + 1) // 2 + props
    f32, bf16 = jnp.float32, jnp.bfloat16
    vmem = pl.BlockSpec(memory_space=pltpu.VMEM)
    shape = jax.ShapeDtypeStruct
    kept_in = pltpu.VMEM
    return pl.pallas_call(
        functools.partial(core_kernel, heads),
        out_shape=[
            kept_in((tokens // 2, width), bf16),
            kept_in((ranks // 2, BLOCK, 128), f32),
            pltpu.HBM(base.shape, f32),
            kept_in((tokens, cols), f32),
            kept_in((tokens, cols), f32),
            kept_in((tokens, states), f32),
            kept_in((ranks, coefs * BLOCK, cols), f32),
        ],
        in_specs=[pl.BlockSpec(memory_space=pltpu.SMEM)] + [vmem] * 19,
        out_specs=[vmem, vmem, pl.BlockSpec(memory_space=pl.ANY)] + [vmem] * 4,
        scratch_shapes=[
            pltpu.VMEM((tokens, states), f32),
            pltpu.VMEM((tokens, weights[3].shape[0]), f32),
            pltpu.VMEM((tokens // 2, cols), bf16),
            pltpu.VMEM((tokens // 2, cols), f32),
            pltpu.SemaphoreType.DMA((ranks,)),
        ],
        compiler_params=pltpu.CompilerParams(vmem_limit_bytes=8 * 1024 * 1024),
        name="core",
    )(rank, rows, kept(base, pltpu.VMEM), kept(half, pltpu.VMEM), *parts, *[kept(w, pltpu.VMEM) for w in weights], bias, decay_log, skip, ci, cw, cr, gain)


def tail_kernel(
    n,
    props,
    channels,
    far,
    far_sq,
    gate,
    inner,
    read,
    wide,
    half,
    outw,
    gain_ref,
    mixed,
    near,
    near_sq,
    carried,
    un,
    out,
    out_sq,
    pbuf,
    rbuf,
    lbuf,
    rout,
    lout,
    psq,
    rsq,
    lsq,
    routq,
    loutq,
    ps,
    pr,
    rs,
    rr,
    ls,
    lr,
):
    f32 = jnp.float32
    k = lax.axis_index("kv")
    t = lax.axis_index("tp")
    rank = k * 2 + t
    mid = n // 2
    right = {"kv": lax.rem(k + 1, n)}
    left = {"kv": lax.rem(k + n - 1, n)}
    partner = {"tp": 1 - t}
    span = far.shape[3] // CHUNKS
    rows = far.shape[2]
    barrier = pltpu.get_barrier_semaphore()

    low = k < mid
    first = jnp.where(low, 0, CARRY)
    inside = (k > 0) & (k < n - 1)
    pl.semaphore_signal(barrier, inc=1, device_id=partner, device_id_type=MESH)

    @pl.when(k < n - 1)
    def _():
        pl.semaphore_signal(barrier, inc=1, device_id=right, device_id_type=MESH)

    @pl.when(k > 0)
    def _():
        pl.semaphore_signal(barrier, inc=1, device_id=left, device_id_type=MESH)

    @pl.when(inside)
    def _():
        pl.semaphore_wait(barrier, 3)

    @pl.when(jnp.logical_not(inside))
    def _():
        pl.semaphore_wait(barrier, 2)

    pieces = range(CHUNKS + 1)

    def piece(data, squares, lead, c):
        if c == CHUNKS:
            return squares.at[lead]
        return data.at[(*lead, slice(None), pl.ds(c * span, span))]

    def across(away, i, c):
        at = jnp.where(low, mid - 1 - i, i)
        j = jnp.where(low, (mid if away else 0) + at, at + (0 if away else mid))
        lead = (at, 1 - t)
        src = piece(far, far_sq, lead, c) if away else piece(near, near_sq, lead, c)
        return remote(src, piece(pbuf, psq, (j,), c), ps.at[j, c], pr.at[j, c], partner)

    def arrived(j, c):
        there = piece(pbuf, psq, (j,), c)
        return remote(there, there, ps.at[j, c], pr.at[j, c], partner)

    def to_right(d, c):
        src, dst = piece(rout, routq, (d,), c), piece(rbuf, rsq, (d,), c)
        return remote(src, dst, rs.at[d, c], rr.at[d, c], right)

    def to_left(d, c):
        src, dst = piece(lout, loutq, (d,), c), piece(lbuf, lsq, (d,), c)
        return remote(src, dst, ls.at[d, c], lr.at[d, c], left)

    for i in range(mid):
        for c in pieces:
            across(True, i, c).start()


    def read_of(data, squares, lead, c):
        return piece(data, squares, lead, c)[...].astype(f32)

    def pair(away, at, j, c):
        arrived(j, c).wait_recv()
        lead = (at, t)
        own = read_of(far, far_sq, lead, c) if away else read_of(near, near_sq, lead, c)
        return own + read_of(pbuf, psq, (j,), c)

    def pair_low(j, c):
        return pair(j >= mid, j % mid, j, c)

    def pair_high(j, c):
        return pair(j < mid, j % mid, j, c)

    def send_right(value, d, c):
        ref = piece(rout, routq, (d,), c)
        ref[...] = value.astype(ref.dtype)
        to_right(d, c).start()

    def send_left(value, d, c):
        ref = piece(lout, loutq, (d,), c)
        ref[...] = value.astype(ref.dtype)
        to_left(d, c).start()

    @pl.when(k == 0)
    def _():
        for d in range(n - 1, mid - 1, -1):
            for c in pieces:
                send_right(pair_low(d, c), d, c)

    @pl.when(k == n - 1)
    def _():
        for d in range(mid):
            for c in pieces:
                send_left(pair_high(d, c), d, c)

    def put_square(e, squares):
        near_sq[lax.div(e, 2), lax.rem(e, 2)] = squares

    carry_over(first, props, half, read, carried)
    gain = own_slice(gain_ref, rank * gate.shape[1], gate.shape[1])
    mix_rows(first, props, gain, wide, inner, gate, carried, un, put_square)
    def put(at, got):
        for j in range(mid):
            for side in range(2):
                lo = (j * 2 + side) * rows
                near[j, side, :, at] = got[lo : lo + rows]

    out_tiles(un, outw, put)
    for i in range(mid):
        for c in pieces:
            across(False, i, c).start()

    def rightward(pair_of, skip):
        for d in range(n - 1, 0, -1):
            for c in pieces:
                if d < skip:
                    @pl.when(k == 0)
                    def _():
                        send_right(pair_of(d, c), d, c)

                @pl.when((k < d) & (k > 0))
                def _():
                    value = pair_of(d, c)
                    to_right(d, c).wait_recv()
                    send_right(value + read_of(rbuf, rsq, (d,), c), d, c)

    def leftward(pair_of, skip):
        for d in range(n - 1):
            for c in pieces:
                if d >= skip:
                    @pl.when(k == n - 1)
                    def _():
                        send_left(pair_of(d, c), d, c)

                @pl.when((k > d) & (k < n - 1))
                def _():
                    value = pair_of(d, c)
                    to_left(d, c).wait_recv()
                    send_left(value + read_of(lbuf, lsq, (d,), c), d, c)

    def total(at, c):
        ref = out_sq if c == CHUNKS else out.at[:, pl.ds(c * span, span)]
        ref[...] = pair(False, at, k, c)

        @pl.when(k > 0)
        def _():
            to_right(k, c).wait_recv()
            ref[...] += read_of(rbuf, rsq, (k,), c)

        @pl.when(k < n - 1)
        def _():
            to_left(k, c).wait_recv()
            ref[...] += read_of(lbuf, lsq, (k,), c)

    @pl.when(low)
    def _():
        rightward(pair_low, mid)
        leftward(pair_low, mid)

    @pl.when(jnp.logical_not(low))
    def _():
        leftward(pair_high, mid)
        rightward(pair_high, mid)

    for c in pieces:
        total(k - jnp.where(low, 0, mid), c)
    scale = lax.rsqrt(out_sq[...] / channels + EPSILON)
    for i in range(props):
        out[i * BLOCK : (i + 1) * BLOCK, :] = (
            out[i * BLOCK : (i + 1) * BLOCK, :] * scale[:, i : i + 1]
        )
    mixed[...] = jnp.dot(
        turn_rows(rows, props, True), out[...].astype(mixed.dtype), preferred_element_type=f32
    ).astype(mixed.dtype)
    for j in range(n):
        for c in pieces:
            arrived(j, c).wait_send()

            @pl.when(k < j)
            def _():
                to_right(j, c).wait_send()

            @pl.when(k > j)
            def _():
                to_left(j, c).wait_send()


def finish(far, squares, near, half, outw, gain, props, channels):
    n = lax.axis_size("kv")
    ranks = n * 2
    tokens, cols = near[0].shape
    rows = tokens // ranks
    width = far.shape[1]
    dma = pltpu.SemaphoreType.DMA
    vmem = pl.BlockSpec(memory_space=pltpu.VMEM)
    kind = far.dtype
    f32 = jnp.float32
    refs = [far.reshape(n // 2, 2, rows, width), squares.reshape(n // 2, 2, BLOCK, 128), *near, half, outw]
    return pl.pallas_call(
        functools.partial(tail_kernel, n, props, channels),
        out_shape=jax.ShapeDtypeStruct((rows, width), kind),
        in_specs=[vmem] * (len(refs) + 1),
        out_specs=vmem,
        scratch_shapes=[
            pltpu.VMEM((n // 2, 2, rows, width), kind),
            pltpu.VMEM((n // 2, 2, BLOCK, 128), f32),
            pltpu.VMEM((tokens // 2, cols), f32),
            pltpu.VMEM((tokens // 2, cols), kind),
            pltpu.VMEM((rows, width), f32),
            pltpu.VMEM((BLOCK, 128), f32),
        ]
        + [pltpu.VMEM((n, rows, width), kind)] * 5
        + [pltpu.VMEM((n, BLOCK, 128), f32)] * 5
        + [dma((n, CHUNKS + 1))] * 6,
        compiler_params=pltpu.CompilerParams(
            collective_id=3, has_side_effects=True, vmem_limit_bytes=12 * 1024 * 1024
        ),
        name="tail",
    )(*[kept(x, pltpu.VMEM) for x in refs], gain)


def whole_groups(tokens, saved_state, last_steps):
    span = lax.axis_size("kv") * lax.axis_size("tp")
    return span == GROUPS and tokens.shape[0] == BLOCK * last_steps.shape[1]


def quick(
    tokens,
    norm_gain,
    gate_proj,
    inner_proj,
    write_proj,
    read_proj,
    step_proj,
    step_bias,
    decay_log,
    skip_gain,
    conv_inner,
    conv_write,
    conv_read,
    out_gain,
    out_proj,
    saved_state,
    inner_history,
    write_history,
    read_history,
    last_steps,
    accepted,
):
    device_rank = lax.axis_index(("kv", "tp"))
    seqs, heads, head_dim, states = saved_state.shape
    slab = lambda x: x.transpose(1, 0, 2)
    row = lambda x: x.reshape(1, -1)
    weights = (inner_proj, write_proj, read_proj, step_proj.T, gate_proj, out_proj)
    got = lead(
        tokens,
        row(norm_gain),
        row(accepted),
        last_steps.transpose(1, 2, 0),
        row(decay_log),
        slab(inner_history),
        slab(write_history),
        slab(read_history),
        conv_inner,
        conv_write,
        conv_read,
        saved_state.reshape(seqs, heads * head_dim, states),
        weights,
    )
    rows, base, half = got[:3]
    far, squares, base_state, *near = core(
        device_rank.reshape(1).astype(jnp.int32),
        heads,
        rows.reshape(-1, rows.shape[-1]),
        base,
        half,
        got[3:6],
        got[6:],
        row(step_bias),
        row(decay_log),
        row(skip_gain),
        conv_inner,
        conv_write,
        conv_read,
        row(out_gain),
    )
    mixed = finish(
        far, squares, near, half, got[-1], row(out_gain), last_steps.shape[1], out_gain.shape[0]
    )
    return (mixed, base_state.reshape(saved_state.shape))


def body(
    tokens,
    norm_gain,
    gate_proj,
    inner_proj,
    write_proj,
    read_proj,
    step_proj,
    step_bias,
    decay_log,
    skip_gain,
    conv_inner,
    conv_write,
    conv_read,
    out_gain,
    out_proj,
    saved_state,
    inner_history,
    write_history,
    read_history,
    last_steps,
    accepted,
):
    if whole_groups(tokens, saved_state, last_steps):
        return quick(
            tokens,
            norm_gain,
            gate_proj,
            inner_proj,
            write_proj,
            read_proj,
            step_proj,
            step_bias,
            decay_log,
            skip_gain,
            conv_inner,
            conv_write,
            conv_read,
            out_gain,
            out_proj,
            saved_state,
            inner_history,
            write_history,
            read_history,
            last_steps,
            accepted,
        )
    device_rank = lax.axis_index(("kv", "tp"))
    seq_count = saved_state.shape[0]
    local_heads = saved_state.shape[1]
    head_dim = saved_state.shape[2]
    proposals = last_steps.shape[1]
    inner_cols = inner_proj.shape[1]
    state_cols = write_proj.shape[1]
    token_count = tokens.shape[0]
    own_rows = tokens.astype(jnp.float32)
    normed_own = (
        own_rows
        * lax.rsqrt(jnp.mean(own_rows * own_rows, axis=-1, keepdims=True) + EPSILON)
        * norm_gain
    ).astype(jnp.bfloat16)
    normed = gathered(normed_own)
    normed = normed.reshape(seq_count, proposals, -1).transpose(1, 0, 2)
    normed = normed.reshape(proposals * seq_count, -1)

    def project(weight):
        out = jnp.dot(normed, weight, preferred_element_type=jnp.float32)
        return out.reshape(proposals, seq_count, -1)

    gate_rows = project(gate_proj).astype(jnp.bfloat16)
    inner_rows = project(inner_proj).astype(jnp.bfloat16)
    first_head = device_rank * local_heads
    state_cols = write_proj.shape[1]
    states = saved_state.shape[3]
    step_local = lax.dynamic_slice_in_dim(step_proj, first_head, local_heads, 1)
    step_local = jnp.pad(step_local, ((0, 0), (0, states - local_heads)))
    small = project(jnp.concatenate([write_proj, read_proj, step_local], axis=1))
    par = lax.dynamic_slice_in_dim(
        jnp.stack([step_bias, decay_log, skip_gain]), first_head, local_heads, 1
    )
    slab = lambda x: x.transpose(1, 0, 2)
    hist_inner, hist_write, hist_read = slab(inner_history), slab(write_history), slab(read_history)
    group_span = lax.axis_size("kv") * lax.axis_size("tp") // GROUPS
    if group_span >= 2:
        write_rows = small[:, :, :state_cols].astype(jnp.bfloat16)
        read_rows = small[:, :, state_cols : 2 * state_cols].astype(jnp.bfloat16)
        pieces = (write_rows, read_rows, hist_write, hist_read)
        pieces = tuple(lax.all_gather(x, "tp", axis=2, tiled=True) for x in pieces)
        kv_rank = lax.axis_index("kv")
        bit_count = (group_span // lax.axis_size("tp")).bit_length() - 1
        for bit in range(bit_count):
            partner = swapped(pieces, "kv", bit)
            lower = jnp.bitwise_and(jnp.right_shift(kv_rank, bit), 1) == 0
            pieces = tuple(
                jnp.where(
                    lower,
                    jnp.concatenate([mine, theirs], axis=2),
                    jnp.concatenate([theirs, mine], axis=2),
                )
                for mine, theirs in zip(pieces, partner)
            )
        write_rows, read_rows, hist_write, hist_read = pieces
        small = jnp.concatenate(
            [
                write_rows.astype(jnp.float32),
                read_rows.astype(jnp.float32),
                small[:, :, 2 * state_cols :],
            ],
            axis=2,
        )
    unscaled, squares, base_state = mix(
        device_rank,
        device_rank // group_span,
        accepted[:, None],
        slab(last_steps),
        par,
        gate_rows,
        inner_rows,
        small,
        hist_inner,
        hist_write,
        hist_read,
        conv_inner,
        conv_write,
        conv_read,
        out_gain[None, :],
        saved_state.reshape(seq_count, local_heads * head_dim, -1),
    )
    base_state = base_state.reshape(saved_state.shape)
    unscaled = unscaled.transpose(1, 0, 2).reshape(seq_count * proposals, inner_cols)
    partial_value = jnp.dot(unscaled, out_proj, preferred_element_type=jnp.float32)
    squares = squares[:, :, 0].T.reshape(-1)
    summed, square_own = scattered(partial_value.astype(jnp.bfloat16), squares)
    mixed = (summed * lax.rsqrt(square_own / out_gain.shape[0] + EPSILON)[:, None]).astype(jnp.bfloat16)
    return (mixed, base_state)


def solution(mesh):
    placed = (
        P(("dp", "kv", "tp"), None),
        P(),
        P(None, ("kv", "tp")),
        P(None, ("kv", "tp")),
        P(None, ("kv", "tp")),
        P(None, ("kv", "tp")),
        P(),
        P(),
        P(),
        P(),
        P(),
        P(),
        P(),
        P(),
        P(("kv", "tp"), None),
        P("dp", ("kv", "tp"), None, None),
        P("dp", None, ("kv", "tp")),
        P("dp", None, ("kv", "tp")),
        P("dp", None, ("kv", "tp")),
        P("dp", None, ("kv", "tp")),
        P("dp"),
    )
    return jax.shard_map(
        body,
        mesh=mesh,
        in_specs=placed,
        out_specs=(P(("dp", "kv", "tp"), None), P("dp", ("kv", "tp"), None, None)),
        check_vma=False,
    )
```

```python
import functools

import jax
import jax.numpy as jnp
from jax import lax
from jax.experimental import pallas as pl
from jax.experimental.pallas import tpu as pltpu
from jax.sharding import PartitionSpec as P

GROUPS = 8
EPSILON = 0.1
BLOCK = 8
highest = lax.Precision.HIGHEST


def swapped(value, axis, stride):
    mask = 2**stride
    pairs = [(source, source ^ mask) for source in range(lax.axis_size(axis))]
    return lax.ppermute(value, axis, pairs)


def mix_kernel(
    rank_ref,
    acc_ref,
    steps_ref,
    last_ref,
    par_ref,
    gate_ref,
    inner_ref,
    write_ref,
    read_ref,
    hist_inner_ref,
    hist_write_ref,
    hist_read_ref,
    taps_inner_ref,
    taps_write_ref,
    taps_read_ref,
    gain_ref,
    expand_ref,
    state_ref,
    un_ref,
    sq_ref,
    base_ref,
):
    f32 = jnp.float32
    props = steps_ref.shape[0]
    heads = last_ref.shape[2]
    cols = inner_ref.shape[2]
    states = write_ref.shape[2]
    head_dim = cols // heads
    hist = hist_inner_ref.shape[0]
    width = taps_inner_ref.shape[0]
    acc = acc_ref[...]

    def silu(x):
        return x / (1.0 + jnp.exp(-x))

    def slabs(ref):
        return [ref[k].astype(f32) for k in range(ref.shape[0])]

    round_bf = lambda x: x.astype(jnp.bfloat16).astype(f32)

    def conv(rows, taps_ref):
        taps = taps_ref[...].astype(f32)
        res = []
        for r in range(len(rows) - width + 1):
            v = taps[0:1] * rows[r]
            for k in range(1, width):
                v = v + taps[k : k + 1] * rows[r + k]
            res.append(silu(v))
        return res

    def current(h, new_ref):
        where_at = jnp.broadcast_to(acc, h[0].shape)
        rows = []
        for k in range(width - 1):
            r = h[k]
            for v in range(1, hist - width + 2):
                r = jnp.where(where_at == v, h[k + v], r)
            rows.append(r)
        return rows + [round_bf(x) for x in slabs(new_ref)]

    h_inner = slabs(hist_inner_ref)
    inner_old = conv(h_inner, taps_inner_ref)
    inner_new = conv(current(h_inner, inner_ref), taps_inner_ref)
    h_write = slabs(hist_write_ref)
    write_old = [round_bf(x) for x in conv(h_write, taps_write_ref)]
    write_new = [round_bf(x) for x in conv(current(h_write, write_ref), taps_write_ref)]
    read_new = [round_bf(x) for x in conv(current(slabs(hist_read_ref), read_ref), taps_read_ref)]

    bias = par_ref[0:1]
    rate = -jnp.exp(par_ref[1:2])
    skip = par_ref[2:3]
    acc_h = jnp.broadcast_to(acc, (BLOCK, heads))
    masks = [jnp.where(acc_h > t, 1.0, 0.0) for t in range(props)]
    logs = [rate * last_ref[t] * masks[t] for t in range(props)]
    coefs = [None] * props
    tail = jnp.zeros((BLOCK, heads), f32)
    for t in reversed(range(props)):
        coefs[t] = masks[t] * jnp.exp(tail) * last_ref[t]
        tail = tail + logs[t]
    decay = jnp.exp(tail)
    step = []
    for t in range(props):
        x = steps_ref[t][:, :heads] + bias
        step.append(jnp.maximum(x, 0.0) + jnp.log1p(jnp.exp(-jnp.abs(x))))
    cums = []
    for t in range(props):
        cums.append(rate * step[t] + (cums[-1] if cums else 0.0))
    where_of = {}
    for i in range(props):
        for j in range(i + 1):
            score = jnp.sum(read_new[i] * write_new[j], axis=-1, keepdims=True)
            c = jnp.exp(cums[i] - cums[j]) * step[j] * score
            if i == j:
                c = c + skip
            where_of[(i, j)] = len(coefs)
            coefs.append(c)
    first_cum = len(coefs)
    for i in range(props):
        coefs.append(jnp.exp(cums[i]))
    wide = jnp.dot(
        jnp.concatenate(coefs, axis=0),
        expand_ref[...],
        precision=highest,
        preferred_element_type=f32,
    )

    def at(k):
        return wide[k * BLOCK : (k + 1) * BLOCK]

    left = jnp.concatenate([at(t) * inner_old[t] for t in range(props)], axis=0)
    high = round_bf(left)
    both = jnp.concatenate([high, left - high], axis=0)
    turned = jnp.transpose(both).astype(jnp.bfloat16)
    write_all = jnp.concatenate(write_old + write_old, axis=0)
    read_all = jnp.concatenate(read_new, axis=0)
    seq_w = lax.broadcasted_iota(jnp.int32, write_all.shape, 0) % BLOCK
    seq_r = lax.broadcasted_iota(jnp.int32, read_all.shape, 0) % BLOCK
    carried = jnp.zeros((props * BLOCK, cols), f32)
    for s in range(BLOCK):
        right = jnp.where(seq_w == s, write_all, 0.0).astype(jnp.bfloat16)
        update = jnp.dot(turned, right, preferred_element_type=f32)
        parts = []
        for h in range(heads):
            lo, hi = h * head_dim, (h + 1) * head_dim
            d = jnp.broadcast_to(decay[s : s + 1, h : h + 1], (head_dim, states))
            new = d * state_ref[s, lo:hi, :] + update[lo:hi]
            base_ref[s, lo:hi, :] = new
            parts.append(new.astype(jnp.bfloat16))
        asked = jnp.where(seq_r == s, read_all, 0.0).astype(jnp.bfloat16)
        carried = carried + lax.dot_general(
            asked,
            jnp.concatenate(parts, axis=0),
            (((1,), (1,)), ((), ())),
            preferred_element_type=f32,
        )
    for i in range(props):
        y = at(first_cum + i) * carried[i * BLOCK : (i + 1) * BLOCK]
        for j in range(i + 1):
            y = y + at(where_of[(i, j)]) * inner_new[j]
        g = y * silu(gate_ref[i].astype(f32))
        sq_ref[i] = jnp.broadcast_to(jnp.sum(g * g, axis=-1, keepdims=True), sq_ref.shape[1:])
        un_ref[i] = (g * gain_ref[...]).astype(un_ref.dtype)


def mix(rank, group, acc, last, par, gate, inner, small, hi, hw, hr, ci, cw, cr, gain, state):
    props, seqs, heads = last.shape
    cols, states = state.shape[1], state.shape[2]
    expand = (jnp.arange(cols)[None, :] // (cols // heads) == jnp.arange(heads)[:, None]).astype(
        jnp.float32
    )
    hist = hi.shape[0]
    width = ci.shape[0]

    def slab(lead, last_dim):
        return pl.BlockSpec((lead, BLOCK, last_dim), lambda g, r: (0, g, 0))

    def piece(which):
        return pl.BlockSpec((props, BLOCK, states), lambda g, r: (0, g, which))

    def own(rows, last_dim, which):
        return pl.BlockSpec((rows, last_dim), lambda g, r: (0, r[which]))

    state_spec = pl.BlockSpec((BLOCK, cols, states), lambda g, r: (g, 0, 0))
    return pl.pallas_call(
        mix_kernel,
        grid_spec=pltpu.PrefetchScalarGridSpec(
            num_scalar_prefetch=1,
            grid=(seqs // BLOCK,),
            in_specs=[
                pl.BlockSpec((BLOCK, 1), lambda g, r: (g, 0)),
                piece(2),
                slab(props, heads),
                pl.BlockSpec(par.shape, lambda g, r: (0, 0)),
                slab(props, cols),
                slab(props, cols),
                piece(0),
                piece(1),
                slab(hist, cols),
                slab(hist, states),
                slab(hist, states),
                own(width, cols, 0),
                own(width, states, 1),
                own(width, states, 1),
                own(1, cols, 0),
                pl.BlockSpec(expand.shape, lambda g, r: (0, 0)),
                state_spec,
            ],
            out_specs=[slab(props, cols), slab(props, 128), state_spec],
        ),
        out_shape=[
            jax.ShapeDtypeStruct((props, seqs, cols), jnp.bfloat16),
            jax.ShapeDtypeStruct((props, seqs, 128), jnp.float32),
            jax.ShapeDtypeStruct(state.shape, jnp.float32),
        ],
        compiler_params=pltpu.CompilerParams(
            dimension_semantics=("arbitrary",), vmem_limit_bytes=48 * 1024 * 1024
        ),
        name="mix",
    )(
        jnp.stack([rank, group]).astype(jnp.int32),
        acc, small, last, par, gate, inner, small, small, hi, hw, hr, ci, cw, cr, gain, expand, state,
    )


MESH = pl.DeviceIdType.MESH
CHUNKS = 2


def remote(src, dst, send, recv, where):
    return pltpu.make_async_remote_copy(
        src_ref=src, dst_ref=dst, send_sem=send, recv_sem=recv, device_id=where, device_id_type=MESH
    )


def gather_kernel(n, own_ref, out_ref, rs, rr, ls, lr, fs, fr, local_sem):
    k = lax.axis_index("kv")
    t = lax.axis_index("tp")
    right = {"kv": lax.rem(k + 1, n)}
    left = {"kv": lax.rem(k + n - 1, n)}
    partner = {"tp": 1 - t}
    span = own_ref.shape[1] // CHUNKS
    barrier = pltpu.get_barrier_semaphore()
    pl.semaphore_signal(barrier, inc=1, device_id=partner, device_id_type=MESH)

    @pl.when(k < n - 1)
    def _():
        pl.semaphore_signal(barrier, inc=1, device_id=right, device_id_type=MESH)

    @pl.when(k > 0)
    def _():
        pl.semaphore_signal(barrier, inc=1, device_id=left, device_id_type=MESH)

    inner = (k > 0) & (k < n - 1)

    @pl.when(inner)
    def _():
        pl.semaphore_wait(barrier, 3)

    @pl.when(jnp.logical_not(inner))
    def _():
        pl.semaphore_wait(barrier, 2)

    def view(j, c):
        return out_ref.at[j, t, :, pl.ds(c * span, span)]

    def own(c):
        return own_ref.at[:, pl.ds(c * span, span)]

    def to_right(s, c):
        j = jnp.maximum(k - s, 0)
        return remote(own(c) if s == 0 else view(j, c), view(j, c), rs.at[s, c], rr.at[s, c], right)

    def to_left(s, c):
        j = jnp.minimum(k + s, n - 1)
        return remote(own(c) if s == 0 else view(j, c), view(j, c), ls.at[s, c], lr.at[s, c], left)

    def across(j, c, mine=False):
        return remote(own(c) if mine else view(j, c), view(j, c), fs.at[j, c], fr.at[j, c], partner)

    for s in range(n - 1):
        for c in range(CHUNKS):
            if s > 0:
                @pl.when(k - s >= 0)
                def _():
                    to_right(s - 1, c).wait_recv()

                @pl.when(k + s < n)
                def _():
                    to_left(s - 1, c).wait_recv()

            @pl.when((k - s >= 0) & (k < n - 1))
            def _():
                to_right(s, c).start()

            @pl.when((k + s < n) & (k > 0))
            def _():
                to_left(s, c).start()

            if s == 0:
                across(k, c, True).start()
            else:
                @pl.when(k - s >= 0)
                def _():
                    across(k - s, c).start()

                @pl.when(k + s < n)
                def _():
                    across(k + s, c).start()
        if s == 0:
            local = pltpu.make_async_copy(own_ref, out_ref.at[k, t], local_sem)
            local.start()
            local.wait()
    s = n - 1
    for c in range(CHUNKS):
        @pl.when(k - s >= 0)
        def _():
            to_right(s - 1, c).wait_recv()
            across(k - s, c).start()

        @pl.when(k + s < n)
        def _():
            to_left(s - 1, c).wait_recv()
            across(k + s, c).start()
    for s in range(n - 1):
        for c in range(CHUNKS):
            @pl.when((k - s >= 0) & (k < n - 1))
            def _():
                to_right(s, c).wait_send()

            @pl.when((k + s < n) & (k > 0))
            def _():
                to_left(s, c).wait_send()
    for j in range(n):
        for c in range(CHUNKS):
            across(j, c).wait_send()
            remote(
                out_ref.at[j, 1 - t, :, pl.ds(c * span, span)],
                out_ref.at[j, 1 - t, :, pl.ds(c * span, span)],
                fs.at[j, c],
                fr.at[j, c],
                partner,
            ).wait_recv()


def gathered(own):
    n = lax.axis_size("kv")
    rows, cols = own.shape
    dma = pltpu.SemaphoreType.DMA
    out = pl.pallas_call(
        functools.partial(gather_kernel, n),
        out_shape=jax.ShapeDtypeStruct((n, 2, rows, cols), own.dtype),
        in_specs=[pl.BlockSpec(memory_space=pltpu.VMEM)],
        out_specs=pl.BlockSpec(memory_space=pltpu.VMEM),
        scratch_shapes=[dma((n - 1, CHUNKS))] * 4 + [dma((n, CHUNKS))] * 2 + [dma],
        compiler_params=pltpu.CompilerParams(
            collective_id=0, has_side_effects=True, vmem_limit_bytes=32 * 1024 * 1024
        ),
        name="gather",
    )(own)
    return out.reshape(n * 2 * rows, cols)


def scatter_kernel(
    n, part, sq, out, sqs, pbuf, rbuf, lbuf, rout, lout, ps, pr, rs, rr, ls, lr, ss, sr
):
    f32 = jnp.float32
    k = lax.axis_index("kv")
    t = lax.axis_index("tp")
    rank = k * 2 + t
    ranks = n * 2
    right = {"kv": lax.rem(k + 1, n)}
    left = {"kv": lax.rem(k + n - 1, n)}
    partner = {"tp": 1 - t}
    span = part.shape[3] // CHUNKS
    barrier = pltpu.get_barrier_semaphore()

    def peer(o):
        p = lax.rem(rank + o, ranks)
        return {"kv": p // 2, "tp": lax.rem(p, 2)}

    for o in range(1, ranks):
        pl.semaphore_signal(barrier, inc=1, device_id=peer(o), device_id_type=MESH)
    pl.semaphore_wait(barrier, ranks - 1)

    def cut(c):
        return pl.ds(c * span, span)

    def across(j, c):
        return remote(
            part.at[j, 1 - t, :, cut(c)], pbuf.at[j, :, cut(c)], ps.at[j, c], pr.at[j, c], partner
        )

    def to_right(d, c):
        return remote(
            rout.at[d, :, cut(c)], rbuf.at[d, :, cut(c)], rs.at[d, c], rr.at[d, c], right
        )

    def to_left(d, c):
        return remote(lout.at[d, :, cut(c)], lbuf.at[d, :, cut(c)], ls.at[d, c], lr.at[d, c], left)

    def square(o):
        p = lax.rem(rank + o, ranks)
        return remote(sq.at[p], sqs.at[rank], ss.at[o], sr.at[o], peer(o))

    low = k < n // 2
    for i in range(n):
        j = jnp.where(low, n - 1 - i, i)
        for c in range(CHUNKS):
            across(j, c).start()
    for o in range(1, ranks):
        square(o).start()
    sqs[rank] = sq[rank]

    def pair(j, c):
        across(j, c).wait_recv()
        return part[j, t, :, cut(c)].astype(f32) + pbuf[j, :, cut(c)].astype(f32)

    def rightward():
        for d in range(n - 1, 0, -1):
            for c in range(CHUNKS):
                @pl.when((k < d) & (k == 0))
                def _():
                    rout[d, :, cut(c)] = pair(d, c).astype(rout.dtype)
                    to_right(d, c).start()

                @pl.when((k < d) & (k > 0))
                def _():
                    value = pair(d, c)
                    to_right(d, c).wait_recv()
                    rout[d, :, cut(c)] = (value + rbuf[d, :, cut(c)].astype(f32)).astype(rout.dtype)
                    to_right(d, c).start()

    def leftward():
        for d in range(n - 1):
            for c in range(CHUNKS):
                @pl.when((k > d) & (k == n - 1))
                def _():
                    lout[d, :, cut(c)] = pair(d, c).astype(lout.dtype)
                    to_left(d, c).start()

                @pl.when((k > d) & (k < n - 1))
                def _():
                    value = pair(d, c)
                    to_left(d, c).wait_recv()
                    lout[d, :, cut(c)] = (value + lbuf[d, :, cut(c)].astype(f32)).astype(lout.dtype)
                    to_left(d, c).start()

    @pl.when(k < n // 2)
    def _():
        rightward()
        leftward()

    @pl.when(k >= n // 2)
    def _():
        leftward()
        rightward()

    for c in range(CHUNKS):
        out[:, cut(c)] = pair(k, c)

        @pl.when(k > 0)
        def _():
            to_right(k, c).wait_recv()
            out[:, cut(c)] += rbuf[k, :, cut(c)].astype(f32)

        @pl.when(k < n - 1)
        def _():
            to_left(k, c).wait_recv()
            out[:, cut(c)] += lbuf[k, :, cut(c)].astype(f32)

    for j in range(n):
        for c in range(CHUNKS):
            across(j, c).wait_send()

            @pl.when(k < j)
            def _():
                to_right(j, c).wait_send()

            @pl.when(k > j)
            def _():
                to_left(j, c).wait_send()
    for o in range(1, ranks):
        square(o).wait_send()
        source = lax.rem(rank + ranks - o, ranks)
        remote(sq.at[rank], sqs.at[source], ss.at[o], sr.at[o], peer(o)).wait_recv()


def scattered(partial_value, squares):
    n = lax.axis_size("kv")
    ranks = n * 2
    rows = partial_value.shape[0] // ranks
    cols = partial_value.shape[1]
    squares = jnp.pad(squares.reshape(ranks, 1, rows), ((0, 0), (0, 7), (0, 128 - rows)))
    dma = pltpu.SemaphoreType.DMA
    vmem = pl.BlockSpec(memory_space=pltpu.VMEM)
    kind = partial_value.dtype
    summed, sqs = pl.pallas_call(
        functools.partial(scatter_kernel, n),
        out_shape=[
            jax.ShapeDtypeStruct((rows, cols), jnp.float32),
            jax.ShapeDtypeStruct(squares.shape, jnp.float32),
        ],
        in_specs=[vmem, vmem],
        out_specs=[vmem, vmem],
        scratch_shapes=[pltpu.VMEM((n, rows, cols), kind)] * 5
        + [dma((n, CHUNKS))] * 6
        + [dma((ranks,))] * 2,
        compiler_params=pltpu.CompilerParams(
            collective_id=1, has_side_effects=True, vmem_limit_bytes=32 * 1024 * 1024
        ),
        name="scatter",
    )(partial_value.reshape(n, 2, rows, cols), squares)
    return summed, jnp.sum(sqs[:, 0, :rows], axis=0)


AHEAD = 3
CARRY = 4
HOPS_IN = (1, 2, 3, 4, 5, 6, 6, 6)
HOPS_END = (0, 0, 0, 1, 2, 3, 4, 6)
SPLITS = 2


def pick(x, rows, first):
    wide = jnp.broadcast_to(x, (rows, x.shape[1]))
    lane = lax.broadcasted_iota(jnp.int32, wide.shape, 1)
    row = lax.broadcasted_iota(jnp.int32, wide.shape, 0)
    return jnp.sum(jnp.where(lane == row + first, wide, 0.0), axis=1, keepdims=True)


def turn_rows(rows, props, back=False):
    seqs = rows // props
    row = lax.broadcasted_iota(jnp.int32, (rows, rows), 0)
    col = lax.broadcasted_iota(jnp.int32, (rows, rows), 1)
    if back:
        row, col = col, row
    return jnp.where(col == row % seqs * props + row // seqs, 1.0, 0.0).astype(jnp.bfloat16)


def silu_of(x):
    half = 0.5 * x
    return half + half * jnp.tanh(half)


def round_of(x):
    return x.astype(jnp.bfloat16).astype(jnp.float32)


def split_of(x):
    high = x.astype(jnp.bfloat16)
    return high, (x - high.astype(jnp.float32)).astype(jnp.bfloat16)


def own_slice(ref, first, count):
    return ref[:, pl.ds(pl.multiple_of(first, 128), count)].astype(jnp.float32)


def lead_kernel(
    n,
    tokens_hbm,
    norm_hbm,
    acc_hbm,
    last_hbm,
    decay_hbm,
    hist_inner_hbm,
    hist_write_hbm,
    hist_read_hbm,
    taps_inner_hbm,
    taps_write_hbm,
    taps_read_hbm,
    state_ref,
    inner_hbm,
    write_hbm,
    read_hbm,
    step_hbm,
    gate_hbm,
    outw_hbm,
    rows_ref,
    base_ref,
    half_ref,
    part_inner_ref,
    part_write_ref,
    part_read_ref,
    inner_ref,
    write_ref,
    read_ref,
    step_ref,
    gate_ref,
    outw_ref,
    own_ref,
    decay_buf,
    wide_buf,
    turned_buf,
    old_buf,
    rs,
    rr,
    ls,
    lr,
    fs,
    fr,
    local_sem,
    state_sems,
    small_sems,
    weight_sems,
    tokens_ref,
    norm_ref,
    acc_ref,
    last_ref,
    decay_ref,
    hist_inner_ref,
    hist_write_ref,
    hist_read_ref,
    taps_inner_ref,
    taps_write_ref,
    taps_read_ref,
):
    f32 = jnp.float32
    bf16 = jnp.bfloat16
    k = lax.axis_index("kv")
    t = lax.axis_index("tp")
    rank = k * 2 + t
    right = {"kv": lax.rem(k + 1, n)}
    left = {"kv": lax.rem(k + n - 1, n)}
    partner = {"tp": 1 - t}
    barrier = pltpu.get_barrier_semaphore()
    pl.semaphore_signal(barrier, inc=1, device_id=partner, device_id_type=MESH)

    @pl.when(k < n - 1)
    def _():
        pl.semaphore_signal(barrier, inc=1, device_id=right, device_id_type=MESH)

    @pl.when(k > 0)
    def _():
        pl.semaphore_signal(barrier, inc=1, device_id=left, device_id_type=MESH)

    props, heads, seqs = last_ref.shape
    cols = base_ref.shape[1]
    states = base_ref.shape[2]
    hist = hist_inner_ref.shape[0]
    width = taps_inner_ref.shape[0]
    blocks = seqs // BLOCK

    def fetch(b):
        span = pl.ds(b * BLOCK, BLOCK)
        return pltpu.make_async_copy(state_ref.at[span], base_ref.at[span], state_sems.at[b])

    small = [
        pltpu.make_async_copy(src, dst, small_sems.at[i])
        for i, (src, dst) in enumerate(
            [
                (tokens_hbm, tokens_ref),
                (norm_hbm, norm_ref),
                (acc_hbm, acc_ref),
                (last_hbm, last_ref),
                (decay_hbm, decay_ref),
                (hist_inner_hbm, hist_inner_ref),
                (hist_write_hbm, hist_write_ref),
                (hist_read_hbm, hist_read_ref),
                (taps_inner_hbm, taps_inner_ref),
                (taps_write_hbm, taps_write_ref),
                (taps_read_hbm, taps_read_ref),
            ]
        )
    ]
    for c in small:
        c.start()
    weights = [
        pltpu.make_async_copy(src, dst, weight_sems.at[i])
        for i, (src, dst) in enumerate(
            [
                (inner_hbm, inner_ref),
                (write_hbm, write_ref),
                (read_hbm, read_ref),
                (step_hbm, step_ref),
                (gate_hbm, gate_ref),
                (outw_hbm, outw_ref),
            ]
        )
    ]
    queue = [fetch(b) for b in range(blocks)] + weights
    for c in queue[:AHEAD]:
        c.start()
    for c in small[:2]:
        c.wait()
    own = tokens_ref[...].astype(f32)
    scale = lax.rsqrt(jnp.mean(own * own, axis=-1, keepdims=True) + EPSILON)
    normed = (own * scale * norm_ref[...]).astype(bf16)
    own_ref[...] = jnp.dot(
        turn_rows(own.shape[0], props), normed, preferred_element_type=f32
    ).astype(bf16)

    inside = (k > 0) & (k < n - 1)

    @pl.when(inside)
    def _():
        pl.semaphore_wait(barrier, 3)

    @pl.when(jnp.logical_not(inside))
    def _():
        pl.semaphore_wait(barrier, 2)

    span = own_ref.shape[1] // SPLITS

    def view(j, c):
        return rows_ref.at[j, t, :, pl.ds(c * span, span)]

    def mine(c):
        return own_ref.at[:, pl.ds(c * span, span)]

    def to_right(s, c):
        j = jnp.maximum(k - s, 0)
        return remote(mine(c) if s == 0 else view(j, c), view(j, c), rs.at[s, c], rr.at[s, c], right)

    def to_left(s, c):
        j = jnp.minimum(k + s, n - 1)
        return remote(mine(c) if s == 0 else view(j, c), view(j, c), ls.at[s, c], lr.at[s, c], left)

    def across(j, c, first=False):
        return remote(mine(c) if first else view(j, c), view(j, c), fs.at[j, c], fr.at[j, c], partner)

    def hop(s, c):
        if s > 0:
            @pl.when(k - s >= 0)
            def _():
                to_right(s - 1, c).wait_recv()

            @pl.when(k + s < n)
            def _():
                to_left(s - 1, c).wait_recv()

        if s < n - 1:
            @pl.when((k - s >= 0) & (k < n - 1))
            def _():
                to_right(s, c).start()

            @pl.when((k + s < n) & (k > 0))
            def _():
                to_left(s, c).start()

        if s == 0:
            across(k, c, True).start()
        else:
            @pl.when(k - s >= 0)
            def _():
                across(k - s, c).start()

            @pl.when(k + s < n)
            def _():
                across(k + s, c).start()

    for c in range(SPLITS):
        hop(0, c)
    local = pltpu.make_async_copy(own_ref, rows_ref.at[k, t], local_sem)
    local.start()

    for c in small[2:]:
        c.wait()

    acc_row = acc_ref[...]
    rate = pick(-jnp.exp(decay_ref[...]), heads, rank * heads)
    old_weights = [None] * props
    tail = jnp.zeros((heads, seqs), f32)
    for p in reversed(range(props)):
        mask = jnp.where(acc_row > p, 1.0, 0.0)
        old_weights[p] = mask * jnp.exp(tail) * last_ref[p]
        tail = tail + rate * last_ref[p] * mask
    turned = jnp.transpose(jnp.concatenate(old_weights + [jnp.exp(tail)], axis=0))
    lane = lax.broadcasted_iota(jnp.int32, (heads, cols), 1)
    row = lax.broadcasted_iota(jnp.int32, (heads, cols), 0)
    expand = jnp.where(lane // (cols // heads) == row, 1.0, 0.0).astype(bf16)
    for p in range(props):
        w = turned[:, p * heads : (p + 1) * heads]
        high, low = split_of(w)
        wide_buf[p] = jnp.dot(high, expand, preferred_element_type=f32) + jnp.dot(
            low, expand, preferred_element_type=f32
        )
    for h in range(heads):
        at = props * heads + h
        decay_buf[h] = jnp.broadcast_to(turned[:, at : at + 1], (seqs, states))
    acc = jnp.sum(
        jnp.where(
            lax.broadcasted_iota(jnp.int32, (seqs, seqs), 0)
            == lax.broadcasted_iota(jnp.int32, (seqs, seqs), 1),
            jnp.broadcast_to(acc_row, (seqs, seqs)),
            0,
        ).astype(f32),
        axis=1,
        keepdims=True,
    )

    def conv_parts(hist_at, taps, part_ref, b):
        where_at = jnp.broadcast_to(acc[b : b + BLOCK], hist_at[0].shape)
        current = []
        for e in range(width - 1):
            r = hist_at[e]
            for v in range(1, hist - width + 2):
                r = jnp.where(where_at == v, hist_at[e + v], r)
            current.append(r)
        for i in range(width - 1):
            total = taps[0:1] * current[i]
            for e in range(i + 1, width - 1):
                total = total + taps[e - i : e - i + 1] * current[e]
            part_ref[i, b : b + BLOCK, :] = total

    def conv_old(hist_at, taps):
        res = []
        for r in range(hist - width + 1):
            total = taps[0:1] * hist_at[r]
            for e in range(1, width):
                total = total + taps[e : e + 1] * hist_at[r + e]
            res.append(silu_of(total))
        return res

    def slabs(ref, b):
        return [ref[e, b : b + BLOCK, :].astype(f32) for e in range(hist)]

    taps_inner = own_slice(taps_inner_ref, rank * cols, cols)
    taps_write = own_slice(taps_write_ref, rank * states, states)
    taps_read = own_slice(taps_read_ref, rank * states, states)
    per_half = blocks // 2

    def prepare(part):
        lefts, rights = [], []
        for g in range(per_half):
            b = (part * per_half + g) * BLOCK
            h_inner = slabs(hist_inner_ref, b)
            h_write = slabs(hist_write_ref, b)
            olds = conv_old(h_inner, taps_inner)
            lefts += [wide_buf[p, b : b + BLOCK, :] * olds[p] for p in range(props)]
            rights += conv_old(h_write, taps_write)
            conv_parts(h_inner, taps_inner, part_inner_ref, b)
            conv_parts(h_write, taps_write, part_write_ref, b)
            conv_parts(slabs(hist_read_ref, b), taps_read, part_read_ref, b)
        turned_buf[part] = jnp.transpose(jnp.concatenate(lefts, axis=0)).astype(bf16)
        old_buf[part] = jnp.concatenate(rights, axis=0).astype(bf16)

    half_rows = per_half * props * BLOCK
    row = lax.broadcasted_iota(jnp.int32, (half_rows, states), 0)
    seq_of = row // (props * BLOCK) * BLOCK + row % BLOCK

    def update(part, first, count):
        lhs = turned_buf[part]
        old = old_buf[part].astype(f32)
        head_dim = cols // heads

        adds = []
        for i in range(0, count, 2):
            rhs = jnp.concatenate(
                [jnp.where(seq_of == first + i + e, old, 0.0).astype(bf16) for e in range(2)],
                axis=1,
            )
            adds.append(jnp.dot(lhs, rhs, preferred_element_type=f32))
        for i in range(count):
            s = part * (seqs // 2) + first + i
            add = adds[i // 2]
            side = i % 2 * states
            for h in range(heads):
                lo, hi = h * head_dim, (h + 1) * head_dim
                new = decay_buf[h, s : s + 1, :] * base_ref[s, lo:hi, :]
                new = new + add[lo:hi, side : side + states]
                base_ref[s, lo:hi, :] = new
                half_ref[s, lo:hi, :] = new.astype(bf16)

    hops = [(s, c) for s in range(1, n) for c in range(SPLITS)]
    done = [0, 0]
    for part in range(2):
        prepare(part)
        for g in range(per_half):
            b = part * per_half + g
            queue[b].wait()
            more = queue[b + AHEAD : b + AHEAD + 1] if b + 1 < blocks else queue[b + AHEAD :]
            for c in more:
                c.start()
            update(part, g * BLOCK, BLOCK)
            for ends, plan in enumerate((HOPS_IN, HOPS_END)):
                goal = len(hops) * plan[b] // 6
                if done[ends] < goal:
                    @pl.when(jnp.logical_not(inside) if ends else inside)
                    def _():
                        for e in range(done[ends], goal):
                            hop(*hops[e])
                    done[ends] = goal
    for w in weights:
        w.wait()
    local.wait()
    for s in range(n - 1):
        for c in range(SPLITS):
            @pl.when((k - s >= 0) & (k < n - 1))
            def _():
                to_right(s, c).wait_send()

            @pl.when((k + s < n) & (k > 0))
            def _():
                to_left(s, c).wait_send()
    for j in range(n):
        for c in range(SPLITS):
            across(j, c).wait_send()
            there = rows_ref.at[j, 1 - t, :, pl.ds(c * span, span)]
            remote(there, there, fs.at[j, c], fr.at[j, c], partner).wait_recv()


kept = pltpu.with_memory_space_constraint


def lead(tokens, norm_gain, acc, last, decay_log, hi, hw, hr, ci, cw, cr, state, weights):
    n = lax.axis_size("kv")
    rows, width = tokens.shape
    props, heads, seqs = last.shape
    cols, states = state.shape[1:]
    taps = ci.shape[0]
    dma = pltpu.SemaphoreType.DMA
    vmem = pl.BlockSpec(memory_space=pltpu.VMEM)
    hbm = pl.BlockSpec(memory_space=pltpu.HBM)
    f32, bf16 = jnp.float32, jnp.bfloat16
    shape = jax.ShapeDtypeStruct
    blocks = seqs // BLOCK
    half_rows = seqs // 2 * props
    small = (tokens, norm_gain, acc, last, decay_log, hi, hw, hr, ci, cw, cr)
    return pl.pallas_call(
        functools.partial(lead_kernel, n),
        out_shape=[
            shape((n, 2, rows, width), bf16),
            pltpu.VMEM(state.shape, f32),
            pltpu.VMEM(state.shape, bf16),
            shape((taps - 1, seqs, cols), f32),
            shape((taps - 1, seqs, states), f32),
            shape((taps - 1, seqs, states), f32),
        ]
        + [pltpu.VMEM(w.shape, w.dtype) for w in weights],
        in_specs=[hbm] * (len(small) + 1 + len(weights)),
        out_specs=[vmem] * (6 + len(weights)),
        scratch_shapes=[
            pltpu.VMEM((rows, width), bf16),
            pltpu.VMEM((heads, seqs, states), f32),
            pltpu.VMEM((props, seqs, cols), f32),
            pltpu.VMEM((2, cols, half_rows), bf16),
            pltpu.VMEM((2, half_rows, states), bf16),
        ]
        + [dma((n - 1, SPLITS))] * 4
        + [dma((n, SPLITS))] * 2
        + [dma, dma((blocks,)), dma((len(small),)), dma((len(weights),))]
        + [pltpu.VMEM(x.shape, x.dtype) for x in small],
        compiler_params=pltpu.CompilerParams(
            collective_id=2, has_side_effects=True, vmem_limit_bytes=8 * 1024 * 1024
        ),
        name="lead",
    )(*[kept(x, pltpu.HBM) for x in small + (state,) + weights])


def carry_over(first, props, half_ref, read_ref, carried_ref):
    rows_of = props * BLOCK
    span = CARRY * rows_of
    asked = jnp.transpose(read_ref[pl.ds(pl.multiple_of(first * rows_of, span), span), :])
    col = lax.broadcasted_iota(jnp.int32, asked.shape, 1)
    seq_of = col // rows_of * BLOCK + col % BLOCK
    total = None
    for s in range(0, CARRY * BLOCK, 2):
        lhs = jnp.concatenate([half_ref[first * BLOCK + s + e] for e in range(2)], axis=1)
        rhs = jnp.concatenate(
            [jnp.where(seq_of == s + e, asked, 0.0).astype(jnp.bfloat16) for e in range(2)], axis=0
        )
        got = jnp.dot(lhs, rhs, preferred_element_type=jnp.float32)
        total = got if total is None else total + got
    carried_ref[...] = jnp.transpose(total)


def mix_rows(first, props, gain, wide_ref, inner_ref, gate_ref, carried_ref, un_ref, put_square):
    rows_of = props * BLOCK
    pairs_of = pairs_up_to(props)
    lane_of = lax.broadcasted_iota(jnp.int32, (BLOCK, 128), 1)

    def one(b):
        r = first + b
        near = pl.multiple_of(b * rows_of, rows_of)
        at_row = pl.multiple_of(r * rows_of, rows_of)

        def at(e):
            return wide_ref[r, e * BLOCK : (e + 1) * BLOCK, :]

        def part(ref, i):
            return ref[pl.ds(at_row + i * BLOCK, BLOCK), :]

        squares = jnp.zeros((BLOCK, 128), jnp.float32)
        outs = []
        for i in range(props):
            y = at(len(pairs_of) + i) * carried_ref[pl.ds(near + i * BLOCK, BLOCK), :]
            for j in range(i + 1):
                y = y + at(pairs_of[(i, j)]) * part(inner_ref, j)
            g = y * silu_of(part(gate_ref, i))
            squares = jnp.where(lane_of == i, jnp.sum(g * g, axis=-1, keepdims=True), squares)
            outs.append(g * gain)
        put_square(b, squares)
        un_ref[pl.ds(near, rows_of), :] = jnp.concatenate(outs, axis=0).astype(jnp.bfloat16)

    each(one, 0, CARRY, 2)


def each(fn, lo, hi, step):
    def run(i, carry):
        for u in range(step):
            fn(lo + i * step + u)
        return carry

    lax.fori_loop(0, (hi - lo) // step, run, 0)


def pairs_up_to(props):
    order = [(i, j) for i in range(props) for j in range(i + 1)]
    return {p: e for e, p in enumerate(order)}


def out_tiles(un_ref, outw_ref, put):
    un = un_ref[...]
    tile = 512
    for lo in range(0, outw_ref.shape[1], tile):
        got = jnp.dot(un, outw_ref[:, lo : lo + tile], preferred_element_type=jnp.float32)
        put(pl.ds(lo, tile), got.astype(jnp.bfloat16))


def core_kernel(
    heads,
    rank_ref,
    rows_ref,
    base_ref,
    half_ref,
    part_inner_ref,
    part_write_ref,
    part_read_ref,
    inner_ref,
    write_ref,
    read_ref,
    step_ref,
    gate_ref,
    outw_ref,
    bias_ref,
    decay_ref,
    skip_ref,
    taps_inner_ref,
    taps_write_ref,
    taps_read_ref,
    gain_ref,
    out_ref,
    sq_ref,
    state_out,
    gate_buf,
    inner_buf,
    read_buf,
    wide_buf,
    write_buf,
    step_buf,
    un_buf,
    carried_buf,
    sems,
):
    f32, bf16 = jnp.float32, jnp.bfloat16
    rank = rank_ref[0]
    seqs, cols, states = base_ref.shape
    blocks = seqs // BLOCK
    props = rows_ref.shape[0] // seqs
    width = taps_inner_ref.shape[0]
    head_count = step_ref.shape[0]

    def flush(b):
        span = pl.ds(b * BLOCK, BLOCK)
        return pltpu.make_async_copy(base_ref.at[span], state_out.at[span], sems.at[b])

    rows = rows_ref[...]
    tile = 256
    for w_ref, buf in ((inner_ref, inner_buf), (gate_ref, gate_buf)):
        for lo in range(0, cols, tile):
            buf[:, lo : lo + tile] = round_of(
                jnp.dot(rows, w_ref[:, lo : lo + tile], preferred_element_type=f32)
            )
    both = jnp.dot(
        rows, jnp.concatenate([write_ref[...], read_ref[...]], axis=1), preferred_element_type=f32
    )
    write_buf[...] = round_of(both[:, :states])
    read_buf[...] = round_of(both[:, states:])
    nt = (((1,), (1,)), ((), ()))
    step_buf[...] = lax.dot_general(rows, step_ref[...], nt, preferred_element_type=f32)
    taps_inner = own_slice(taps_inner_ref, rank * cols, cols)
    taps_write = own_slice(taps_write_ref, rank * states, states)
    taps_read = own_slice(taps_read_ref, rank * states, states)
    gain = own_slice(gain_ref, rank * cols, cols)
    bias = bias_ref[...]
    rate = -jnp.exp(decay_ref[...])
    skip = skip_ref[...]
    lane = lax.broadcasted_iota(jnp.int32, (2 * head_count, cols), 1)
    row = lax.broadcasted_iota(jnp.int32, (2 * head_count, cols), 0)
    expand = jnp.where(
        lane // (cols // heads) + rank * heads == row % head_count, 1.0, 0.0
    ).astype(bf16)

    rows_of = props * BLOCK
    pairs_of = pairs_up_to(props)

    def prepare(r):
        at_row = pl.multiple_of(r * rows_of, rows_of)
        at_seq = pl.multiple_of(r * BLOCK, BLOCK)

        def news(buf, part_ref, taps):
            fresh = [buf[pl.ds(at_row + i * BLOCK, BLOCK), :] for i in range(props)]
            res = []
            for i in range(props):
                total = taps[width - 1 : width] * fresh[i]
                for e in range(1, min(i, width - 1) + 1):
                    total = total + taps[width - 1 - e : width - e] * fresh[i - e]
                if i < width - 1:
                    total = total + part_ref[i, pl.ds(at_seq, BLOCK), :]
                res.append(silu_of(total))
            return res

        inner_new = news(inner_buf, part_inner_ref, taps_inner)
        for i in range(props):
            inner_buf[pl.ds(at_row + i * BLOCK, BLOCK), :] = inner_new[i]
        write_new = [round_of(x) for x in news(write_buf, part_write_ref, taps_write)]
        read_new = [round_of(x) for x in news(read_buf, part_read_ref, taps_read)]
        for i in range(props):
            read_buf[pl.ds(at_row + i * BLOCK, BLOCK), :] = read_new[i]
        steps = step_buf[pl.ds(at_row, rows_of), :] + bias
        steps = jnp.maximum(steps, 0.0) + jnp.log1p(jnp.exp(-jnp.abs(steps)))
        step = [steps[i * BLOCK : (i + 1) * BLOCK] for i in range(props)]
        cums = []
        for i in range(props):
            cums.append(rate * step[i] + (cums[-1] if cums else 0.0))
        coefs = []
        for i, j in pairs_of:
            score = jnp.sum(read_new[i] * write_new[j], axis=-1, keepdims=True)
            c = jnp.exp(cums[i] - cums[j]) * step[j] * score
            coefs.append(c + skip if i == j else c)
        coefs += [jnp.exp(c) for c in cums]
        high, low = split_of(jnp.concatenate(coefs, axis=0))
        wide_buf[r] = jnp.dot(
            jnp.concatenate([high, low], axis=1), expand, preferred_element_type=f32
        )

    for b in range(blocks):
        flush(b).start()
    each(prepare, 0, blocks, 2)
    first = jnp.where(rank < blocks // 2, CARRY, 0)

    def put_square(e, squares):
        sq_ref[e] = squares

    carry_over(first, props, half_ref, read_buf, carried_buf)
    mix_rows(
        first, props, gain, wide_buf, inner_buf, gate_buf, carried_buf, un_buf, put_square
    )

    def put(cut, got):
        out_ref[:, cut] = got

    out_tiles(un_buf, outw_ref, put)
    for b in range(blocks):
        flush(b).wait()


def core(rank, heads, rows, base, half, parts, weights, bias, decay_log, skip, ci, cw, cr, gain):
    seqs, cols, states = base.shape
    tokens = rows.shape[0]
    width = weights[-1].shape[1]
    ranks = seqs // BLOCK
    props = tokens // seqs
    coefs = props * (props + 1) // 2 + props
    f32, bf16 = jnp.float32, jnp.bfloat16
    vmem = pl.BlockSpec(memory_space=pltpu.VMEM)
    shape = jax.ShapeDtypeStruct
    kept_in = pltpu.VMEM
    return pl.pallas_call(
        functools.partial(core_kernel, heads),
        out_shape=[
            kept_in((tokens // 2, width), bf16),
            kept_in((ranks // 2, BLOCK, 128), f32),
            pltpu.HBM(base.shape, f32),
            kept_in((tokens, cols), f32),
            kept_in((tokens, cols), f32),
            kept_in((tokens, states), f32),
            kept_in((ranks, coefs * BLOCK, cols), f32),
        ],
        in_specs=[pl.BlockSpec(memory_space=pltpu.SMEM)] + [vmem] * 19,
        out_specs=[vmem, vmem, pl.BlockSpec(memory_space=pl.ANY)] + [vmem] * 4,
        scratch_shapes=[
            pltpu.VMEM((tokens, states), f32),
            pltpu.VMEM((tokens, weights[3].shape[0]), f32),
            pltpu.VMEM((tokens // 2, cols), bf16),
            pltpu.VMEM((tokens // 2, cols), f32),
            pltpu.SemaphoreType.DMA((ranks,)),
        ],
        compiler_params=pltpu.CompilerParams(vmem_limit_bytes=8 * 1024 * 1024),
        name="core",
    )(rank, rows, kept(base, pltpu.VMEM), kept(half, pltpu.VMEM), *parts, *[kept(w, pltpu.VMEM) for w in weights], bias, decay_log, skip, ci, cw, cr, gain)


def tail_kernel(
    n,
    props,
    channels,
    far,
    far_sq,
    gate,
    inner,
    read,
    wide,
    half,
    outw,
    gain_ref,
    mixed,
    near,
    near_sq,
    carried,
    un,
    out,
    out_sq,
    pbuf,
    rbuf,
    lbuf,
    rout,
    lout,
    psq,
    rsq,
    lsq,
    routq,
    loutq,
    ps,
    pr,
    rs,
    rr,
    ls,
    lr,
):
    f32 = jnp.float32
    k = lax.axis_index("kv")
    t = lax.axis_index("tp")
    rank = k * 2 + t
    mid = n // 2
    right = {"kv": lax.rem(k + 1, n)}
    left = {"kv": lax.rem(k + n - 1, n)}
    partner = {"tp": 1 - t}
    span = far.shape[3] // CHUNKS
    rows = far.shape[2]
    barrier = pltpu.get_barrier_semaphore()

    low = k < mid
    first = jnp.where(low, 0, CARRY)
    inside = (k > 0) & (k < n - 1)
    pl.semaphore_signal(barrier, inc=1, device_id=partner, device_id_type=MESH)

    @pl.when(k < n - 1)
    def _():
        pl.semaphore_signal(barrier, inc=1, device_id=right, device_id_type=MESH)

    @pl.when(k > 0)
    def _():
        pl.semaphore_signal(barrier, inc=1, device_id=left, device_id_type=MESH)

    @pl.when(inside)
    def _():
        pl.semaphore_wait(barrier, 3)

    @pl.when(jnp.logical_not(inside))
    def _():
        pl.semaphore_wait(barrier, 2)

    pieces = range(CHUNKS + 1)

    def piece(data, squares, lead, c):
        if c == CHUNKS:
            return squares.at[lead]
        return data.at[(*lead, slice(None), pl.ds(c * span, span))]

    def across(away, i, c):
        at = jnp.where(low, mid - 1 - i, i)
        j = jnp.where(low, (mid if away else 0) + at, at + (0 if away else mid))
        lead = (at, 1 - t)
        src = piece(far, far_sq, lead, c) if away else piece(near, near_sq, lead, c)
        return remote(src, piece(pbuf, psq, (j,), c), ps.at[j, c], pr.at[j, c], partner)

    def arrived(j, c):
        there = piece(pbuf, psq, (j,), c)
        return remote(there, there, ps.at[j, c], pr.at[j, c], partner)

    def to_right(d, c):
        src, dst = piece(rout, routq, (d,), c), piece(rbuf, rsq, (d,), c)
        return remote(src, dst, rs.at[d, c], rr.at[d, c], right)

    def to_left(d, c):
        src, dst = piece(lout, loutq, (d,), c), piece(lbuf, lsq, (d,), c)
        return remote(src, dst, ls.at[d, c], lr.at[d, c], left)

    for i in range(mid):
        for c in pieces:
            across(True, i, c).start()


    def read_of(data, squares, lead, c):
        return piece(data, squares, lead, c)[...].astype(f32)

    def pair(away, at, j, c):
        arrived(j, c).wait_recv()
        lead = (at, t)
        own = read_of(far, far_sq, lead, c) if away else read_of(near, near_sq, lead, c)
        return own + read_of(pbuf, psq, (j,), c)

    def pair_low(j, c):
        return pair(j >= mid, j % mid, j, c)

    def pair_high(j, c):
        return pair(j < mid, j % mid, j, c)

    def send_right(value, d, c):
        ref = piece(rout, routq, (d,), c)
        ref[...] = value.astype(ref.dtype)
        to_right(d, c).start()

    def send_left(value, d, c):
        ref = piece(lout, loutq, (d,), c)
        ref[...] = value.astype(ref.dtype)
        to_left(d, c).start()

    @pl.when(k == 0)
    def _():
        for d in range(n - 1, mid - 1, -1):
            for c in pieces:
                send_right(pair_low(d, c), d, c)

    @pl.when(k == n - 1)
    def _():
        for d in range(mid):
            for c in pieces:
                send_left(pair_high(d, c), d, c)

    def put_square(e, squares):
        near_sq[lax.div(e, 2), lax.rem(e, 2)] = squares

    carry_over(first, props, half, read, carried)
    gain = own_slice(gain_ref, rank * gate.shape[1], gate.shape[1])
    mix_rows(first, props, gain, wide, inner, gate, carried, un, put_square)
    def put(at, got):
        for j in range(mid):
            for side in range(2):
                lo = (j * 2 + side) * rows
                near[j, side, :, at] = got[lo : lo + rows]

    out_tiles(un, outw, put)
    for i in range(mid):
        for c in pieces:
            across(False, i, c).start()

    def rightward(pair_of, skip):
        for d in range(n - 1, 0, -1):
            for c in pieces:
                if d < skip:
                    @pl.when(k == 0)
                    def _():
                        send_right(pair_of(d, c), d, c)

                @pl.when((k < d) & (k > 0))
                def _():
                    value = pair_of(d, c)
                    to_right(d, c).wait_recv()
                    send_right(value + read_of(rbuf, rsq, (d,), c), d, c)

    def leftward(pair_of, skip):
        for d in range(n - 1):
            for c in pieces:
                if d >= skip:
                    @pl.when(k == n - 1)
                    def _():
                        send_left(pair_of(d, c), d, c)

                @pl.when((k > d) & (k < n - 1))
                def _():
                    value = pair_of(d, c)
                    to_left(d, c).wait_recv()
                    send_left(value + read_of(lbuf, lsq, (d,), c), d, c)

    def total(at, c):
        ref = out_sq if c == CHUNKS else out.at[:, pl.ds(c * span, span)]
        ref[...] = pair(False, at, k, c)

        @pl.when(k > 0)
        def _():
            to_right(k, c).wait_recv()
            ref[...] += read_of(rbuf, rsq, (k,), c)

        @pl.when(k < n - 1)
        def _():
            to_left(k, c).wait_recv()
            ref[...] += read_of(lbuf, lsq, (k,), c)

    @pl.when(low)
    def _():
        rightward(pair_low, mid)
        leftward(pair_low, mid)

    @pl.when(jnp.logical_not(low))
    def _():
        leftward(pair_high, mid)
        rightward(pair_high, mid)

    for c in pieces:
        total(k - jnp.where(low, 0, mid), c)
    scale = lax.rsqrt(out_sq[...] / channels + EPSILON)
    for i in range(props):
        out[i * BLOCK : (i + 1) * BLOCK, :] = (
            out[i * BLOCK : (i + 1) * BLOCK, :] * scale[:, i : i + 1]
        )
    mixed[...] = jnp.dot(
        turn_rows(rows, props, True), out[...].astype(mixed.dtype), preferred_element_type=f32
    ).astype(mixed.dtype)
    for j in range(n):
        for c in pieces:
            arrived(j, c).wait_send()

            @pl.when(k < j)
            def _():
                to_right(j, c).wait_send()

            @pl.when(k > j)
            def _():
                to_left(j, c).wait_send()


def finish(far, squares, near, half, outw, gain, props, channels):
    n = lax.axis_size("kv")
    ranks = n * 2
    tokens, cols = near[0].shape
    rows = tokens // ranks
    width = far.shape[1]
    dma = pltpu.SemaphoreType.DMA
    vmem = pl.BlockSpec(memory_space=pltpu.VMEM)
    kind = far.dtype
    f32 = jnp.float32
    refs = [far.reshape(n // 2, 2, rows, width), squares.reshape(n // 2, 2, BLOCK, 128), *near, half, outw]
    return pl.pallas_call(
        functools.partial(tail_kernel, n, props, channels),
        out_shape=jax.ShapeDtypeStruct((rows, width), kind),
        in_specs=[vmem] * (len(refs) + 1),
        out_specs=vmem,
        scratch_shapes=[
            pltpu.VMEM((n // 2, 2, rows, width), kind),
            pltpu.VMEM((n // 2, 2, BLOCK, 128), f32),
            pltpu.VMEM((tokens // 2, cols), f32),
            pltpu.VMEM((tokens // 2, cols), kind),
            pltpu.VMEM((rows, width), f32),
            pltpu.VMEM((BLOCK, 128), f32),
        ]
        + [pltpu.VMEM((n, rows, width), kind)] * 5
        + [pltpu.VMEM((n, BLOCK, 128), f32)] * 5
        + [dma((n, CHUNKS + 1))] * 6,
        compiler_params=pltpu.CompilerParams(
            collective_id=3, has_side_effects=True, vmem_limit_bytes=12 * 1024 * 1024
        ),
        name="tail",
    )(*[kept(x, pltpu.VMEM) for x in refs], gain)


def whole_groups(tokens, saved_state, last_steps):
    span = lax.axis_size("kv") * lax.axis_size("tp")
    return span == GROUPS and tokens.shape[0] == BLOCK * last_steps.shape[1]


def quick(
    tokens,
    norm_gain,
    gate_proj,
    inner_proj,
    write_proj,
    read_proj,
    step_proj,
    step_bias,
    decay_log,
    skip_gain,
    conv_inner,
    conv_write,
    conv_read,
    out_gain,
    out_proj,
    saved_state,
    inner_history,
    write_history,
    read_history,
    last_steps,
    accepted,
):
    device_rank = lax.axis_index(("kv", "tp"))
    seqs, heads, head_dim, states = saved_state.shape
    slab = lambda x: x.transpose(1, 0, 2)
    row = lambda x: x.reshape(1, -1)
    weights = (inner_proj, write_proj, read_proj, step_proj.T, gate_proj, out_proj)
    got = lead(
        tokens,
        row(norm_gain),
        row(accepted),
        last_steps.transpose(1, 2, 0),
        row(decay_log),
        slab(inner_history),
        slab(write_history),
        slab(read_history),
        conv_inner,
        conv_write,
        conv_read,
        saved_state.reshape(seqs, heads * head_dim, states),
        weights,
    )
    rows, base, half = got[:3]
    far, squares, base_state, *near = core(
        device_rank.reshape(1).astype(jnp.int32),
        heads,
        rows.reshape(-1, rows.shape[-1]),
        base,
        half,
        got[3:6],
        got[6:],
        row(step_bias),
        row(decay_log),
        row(skip_gain),
        conv_inner,
        conv_write,
        conv_read,
        row(out_gain),
    )
    mixed = finish(
        far, squares, near, half, got[-1], row(out_gain), last_steps.shape[1], out_gain.shape[0]
    )
    return (mixed, base_state.reshape(saved_state.shape))


def body(
    tokens,
    norm_gain,
    gate_proj,
    inner_proj,
    write_proj,
    read_proj,
    step_proj,
    step_bias,
    decay_log,
    skip_gain,
    conv_inner,
    conv_write,
    conv_read,
    out_gain,
    out_proj,
    saved_state,
    inner_history,
    write_history,
    read_history,
    last_steps,
    accepted,
):
    if whole_groups(tokens, saved_state, last_steps):
        return quick(
            tokens,
            norm_gain,
            gate_proj,
            inner_proj,
            write_proj,
            read_proj,
            step_proj,
            step_bias,
            decay_log,
            skip_gain,
            conv_inner,
            conv_write,
            conv_read,
            out_gain,
            out_proj,
            saved_state,
            inner_history,
            write_history,
            read_history,
            last_steps,
            accepted,
        )
    device_rank = lax.axis_index(("kv", "tp"))
    seq_count = saved_state.shape[0]
    local_heads = saved_state.shape[1]
    head_dim = saved_state.shape[2]
    proposals = last_steps.shape[1]
    inner_cols = inner_proj.shape[1]
    state_cols = write_proj.shape[1]
    token_count = tokens.shape[0]
    own_rows = tokens.astype(jnp.float32)
    normed_own = (
        own_rows
        * lax.rsqrt(jnp.mean(own_rows * own_rows, axis=-1, keepdims=True) + EPSILON)
        * norm_gain
    ).astype(jnp.bfloat16)
    normed = gathered(normed_own)
    normed = normed.reshape(seq_count, proposals, -1).transpose(1, 0, 2)
    normed = normed.reshape(proposals * seq_count, -1)

    def project(weight):
        out = jnp.dot(normed, weight, preferred_element_type=jnp.float32)
        return out.reshape(proposals, seq_count, -1)

    gate_rows = project(gate_proj).astype(jnp.bfloat16)
    inner_rows = project(inner_proj).astype(jnp.bfloat16)
    first_head = device_rank * local_heads
    state_cols = write_proj.shape[1]
    states = saved_state.shape[3]
    step_local = lax.dynamic_slice_in_dim(step_proj, first_head, local_heads, 1)
    step_local = jnp.pad(step_local, ((0, 0), (0, states - local_heads)))
    small = project(jnp.concatenate([write_proj, read_proj, step_local], axis=1))
    par = lax.dynamic_slice_in_dim(
        jnp.stack([step_bias, decay_log, skip_gain]), first_head, local_heads, 1
    )
    slab = lambda x: x.transpose(1, 0, 2)
    hist_inner, hist_write, hist_read = slab(inner_history), slab(write_history), slab(read_history)
    group_span = lax.axis_size("kv") * lax.axis_size("tp") // GROUPS
    if group_span >= 2:
        write_rows = small[:, :, :state_cols].astype(jnp.bfloat16)
        read_rows = small[:, :, state_cols : 2 * state_cols].astype(jnp.bfloat16)
        pieces = (write_rows, read_rows, hist_write, hist_read)
        pieces = tuple(lax.all_gather(x, "tp", axis=2, tiled=True) for x in pieces)
        kv_rank = lax.axis_index("kv")
        bit_count = (group_span // lax.axis_size("tp")).bit_length() - 1
        for bit in range(bit_count):
            partner = swapped(pieces, "kv", bit)
            lower = jnp.bitwise_and(jnp.right_shift(kv_rank, bit), 1) == 0
            pieces = tuple(
                jnp.where(
                    lower,
                    jnp.concatenate([mine, theirs], axis=2),
                    jnp.concatenate([theirs, mine], axis=2),
                )
                for mine, theirs in zip(pieces, partner)
            )
        write_rows, read_rows, hist_write, hist_read = pieces
        small = jnp.concatenate(
            [
                write_rows.astype(jnp.float32),
                read_rows.astype(jnp.float32),
                small[:, :, 2 * state_cols :],
            ],
            axis=2,
        )
    unscaled, squares, base_state = mix(
        device_rank,
        device_rank // group_span,
        accepted[:, None],
        slab(last_steps),
        par,
        gate_rows,
        inner_rows,
        small,
        hist_inner,
        hist_write,
        hist_read,
        conv_inner,
        conv_write,
        conv_read,
        out_gain[None, :],
        saved_state.reshape(seq_count, local_heads * head_dim, -1),
    )
    base_state = base_state.reshape(saved_state.shape)
    unscaled = unscaled.transpose(1, 0, 2).reshape(seq_count * proposals, inner_cols)
    partial_value = jnp.dot(unscaled, out_proj, preferred_element_type=jnp.float32)
    squares = squares[:, :, 0].T.reshape(-1)
    summed, square_own = scattered(partial_value.astype(jnp.bfloat16), squares)
    mixed = (summed * lax.rsqrt(square_own / out_gain.shape[0] + EPSILON)[:, None]).astype(jnp.bfloat16)
    return (mixed, base_state)


def solution(mesh):
    placed = (
        P(("dp", "kv", "tp"), None),
        P(),
        P(None, ("kv", "tp")),
        P(None, ("kv", "tp")),
        P(None, ("kv", "tp")),
        P(None, ("kv", "tp")),
        P(),
        P(),
        P(),
        P(),
        P(),
        P(),
        P(),
        P(),
        P(("kv", "tp"), None),
        P("dp", ("kv", "tp"), None, None),
        P("dp", None, ("kv", "tp")),
        P("dp", None, ("kv", "tp")),
        P("dp", None, ("kv", "tp")),
        P("dp", None, ("kv", "tp")),
        P("dp"),
    )
    return jax.shard_map(
        body,
        mesh=mesh,
        in_specs=placed,
        out_specs=(P(("dp", "kv", "tp"), None), P("dp", ("kv", "tp"), None, None)),
        check_vma=False,
    )
```
